32 devices in a mesh: sp: 8 (over z, x), tp: 4 (over y, core).
Axes of the slice: x: 2, y: 2, z: 4, core: 2. Of those that a mesh axis runs over, the one named last changes fastest.
Arguments:
- tokens: bfloat16 [1024, 2048], P('sp', 'tp'), may hold values from -6 to 6
- conv_value_weight: bfloat16 [2048, 1024], P('sp', 'tp'), may hold values from -0.125 to 0.125
- conv_gate_weight: bfloat16 [2048, 1024], P('sp', 'tp'), may hold values from -0.125 to 0.125
- conv_kernel: bfloat16 [31, 1024], P(None, 'tp'), may hold values from -16 to 16
- conv_norm_gain: float32 [1024], P('tp'), may hold values from 0.1 to 1.9
- query_weight: bfloat16 [2048, 2048], P('sp', 'tp'), may hold values from -0.125 to 0.125
- key_weight: bfloat16 [2048, 2048], P('sp', 'tp'), may hold values from -0.125 to 0.125
- value_weight: bfloat16 [2048, 2048], P('sp', 'tp'), may hold values from -0.125 to 0.125
- input_gate_weight: bfloat16 [2048, 8], P(None, 'tp'), may hold values from -0.125 to 0.125
- forget_gate_weight: bfloat16 [2048, 8], P(None, 'tp'), may hold values from -0.125 to 0.125
- input_offset: float32 [1024, 8], P('sp', 'tp'), may hold values from -4 to 210
- forget_offset: float32 [1024, 8], P('sp', 'tp'), may hold values from 0 to 30
- memory_norm_gain: float32 [2048], P('tp'), may hold values from 0.1 to 1.9
- conv_out_weight: bfloat16 [1024, 2048], P('tp', 'sp'), may hold values from -0.3125 to 0.3125
- memory_out_weight: bfloat16 [2048, 2048], P('tp', 'sp'), may hold values from -0.125 to 0.125
Outputs:
- mixed: bfloat16 [1024, 2048], P('sp', 'tp')
The draws below stay inside these ranges and needn't reach their ends.
All inputs are finite; a program needn't handle non-finite values.
Results may differ from the reference program's by a relative error of at most 0.03.
Values may be sent and summed in bfloat16 or wider, within the bound.
A program may use at most 128 MiB of HBM per device.

```python
import jax
import jax.numpy as jnp
from jax import lax

D = 2048
CONV = 1024
MEMORY_HEADS = 8
HEAD_DIM = 256
KERNEL = 31
BLOCK = 64
TOK_DEV = 128
SEQUENCE_TOKENS = 1024
GROUPS = 4


def draw_conv_kernel(key, part):
    key_rows = jax.random.split(jax.random.fold_in(key, 101), 2)
    channel = jnp.arange(CONV, dtype=jnp.float32) / CONV
    entries = jnp.clip(jax.random.normal(key_rows[0], (KERNEL, CONV), jnp.float32), -4.0, 4.0)
    rise = jnp.power(10.0, channel)
    factor = jnp.exp(jax.random.uniform(key_rows[1], (CONV,), jnp.float32, -0.35, 0.35))
    return (entries * rise * factor / jnp.sqrt(jnp.float32(KERNEL))).astype(jnp.bfloat16)


def draw_input_offset(key, part):
    key_rows = jax.random.split(jax.random.fold_in(key, 202), 1)
    position_offset = jnp.clip(jax.random.normal(key_rows[0], (SEQUENCE_TOKENS, MEMORY_HEADS), jnp.float32), -4.0, 4.0)
    return position_offset.astype(jnp.float32)


def draw_forget_offset(key, part):
    key_rows = jax.random.split(jax.random.fold_in(key, 303), 6)
    slow_head = jax.random.uniform(key_rows[0], (MEMORY_HEADS,)) < 0.5
    slow_level = jnp.log(jnp.float32(SEQUENCE_TOKENS)) + 3.0
    fast_level = jax.random.uniform(key_rows[1], (MEMORY_HEADS,), jnp.float32, 3.4, 4.6)
    level = jnp.where(slow_head, slow_level, fast_level)
    devices = SEQUENCE_TOKENS // TOK_DEV
    device_shift = jax.random.uniform(key_rows[2], (devices, 1, MEMORY_HEADS), jnp.float32, -0.7, 0.7)
    rough = 0.3 * jnp.clip(jax.random.normal(key_rows[3], (devices, TOK_DEV, MEMORY_HEADS), jnp.float32), -4.0, 4.0)
    position_offset = (level + device_shift + rough).reshape(SEQUENCE_TOKENS, MEMORY_HEADS)
    group_rows = jax.random.randint(key_rows[4], (3,), 0, SEQUENCE_TOKENS)
    token_positions = jnp.arange(SEQUENCE_TOKENS)
    token_group = jnp.any(token_positions[:, None] == group_rows[None, :], axis=1)
    group_level = jax.random.uniform(key_rows[5], (SEQUENCE_TOKENS, MEMORY_HEADS), jnp.float32, 0.9, 1.6)
    return jnp.where(token_group[:, None], group_level, position_offset).astype(jnp.float32)


def block_levels(key, dims, cuts, least, largest):
    level, own = 1.0, jax.random.fold_in(key, 6)
    for position, parts in cuts:
        draws = jnp.exp(jax.random.uniform(jax.random.fold_in(own, position), (parts,), jnp.float32, least / len(cuts), largest / len(cuts)))
        level = level * jnp.repeat(draws, dims[position] // parts).reshape([-1 if axis == position else 1 for axis in range(len(dims))])
    return level


def centred(stream_key, dims, width, limit, cuts=(), kind=jnp.bfloat16):
    drawn = width * jax.random.normal(stream_key, dims, jnp.float32)
    if cuts:
        drawn = drawn * block_levels(stream_key, dims, cuts, -0.22, 0.18)
    return jnp.clip(drawn, -limit, limit).astype(kind)


def setup_inputs(seed: int = 0) -> dict:
    keys = jax.random.split(jax.random.key(seed), 16)
    tokens = centred(keys[0], (SEQUENCE_TOKENS, D), 1.0, 6.0, ((0, 8), (1, 4)))
    conv_value_weight = centred(keys[1], (D, CONV), D ** -0.5, 0.125, ((0, 8), (1, 4)))
    conv_gate_weight = centred(keys[2], (D, CONV), D ** -0.5, 0.125, ((0, 8), (1, 4)))
    conv_kernel = draw_conv_kernel(jax.random.fold_in(keys[15], 71), 0)
    conv_norm_gain = jnp.clip(1.0 + 0.18 * jax.random.normal(keys[4], (CONV,), jnp.float32), 0.1, 1.9)
    query_weight = centred(keys[5], (D, MEMORY_HEADS * HEAD_DIM), D ** -0.5, 0.125, ((0, 8), (1, 4)))
    key_weight = centred(keys[6], (D, MEMORY_HEADS * HEAD_DIM), D ** -0.5, 0.125, ((0, 8), (1, 4)))
    value_weight = centred(keys[7], (D, MEMORY_HEADS * HEAD_DIM), D ** -0.5, 0.125, ((0, 8), (1, 4)))
    input_gate_weight = centred(keys[8], (D, MEMORY_HEADS), D ** -0.5, 0.125, ((1, 4),))
    forget_gate_weight = centred(keys[9], (D, MEMORY_HEADS), D ** -0.5, 0.125, ((1, 4),))
    input_offset = draw_input_offset(jax.random.fold_in(keys[15], 71), 0)
    forget_offset = draw_forget_offset(jax.random.fold_in(keys[15], 71), 0)
    memory_norm_gain = jnp.clip(1.0 + 0.18 * jax.random.normal(keys[12], (MEMORY_HEADS * HEAD_DIM,), jnp.float32), 0.1, 1.9)
    conv_out_weight = centred(keys[13], (CONV, D), (CONV // 3) ** -0.5, 0.3125, ((0, 4), (1, 8)))
    memory_out_weight = centred(keys[14], (MEMORY_HEADS * HEAD_DIM, D), (MEMORY_HEADS * HEAD_DIM) ** -0.5, 0.125, ((0, 4), (1, 8)))
    return {"tokens": tokens, "conv_value_weight": conv_value_weight, "conv_gate_weight": conv_gate_weight, "conv_kernel": conv_kernel, "conv_norm_gain": conv_norm_gain, "query_weight": query_weight, "key_weight": key_weight, "value_weight": value_weight, "input_gate_weight": input_gate_weight, "forget_gate_weight": forget_gate_weight, "input_offset": input_offset, "forget_offset": forget_offset, "memory_norm_gain": memory_norm_gain, "conv_out_weight": conv_out_weight, "memory_out_weight": memory_out_weight}


EPS = 1e-06

def block_step(carry, inputs):
    state, normal, level = carry
    query, key, value, gate_in, forget_log = inputs
    length = gate_in.shape[-1]
    scale = query.shape[-1] ** (-0.5)
    causal = jnp.tril(jnp.ones((length, length), dtype=bool))
    within = jnp.cumsum(forget_log, axis=-1)
    log_weight = within[:, :, None] - within[:, None, :] + gate_in[:, None, :]
    log_weight = jnp.where(causal, log_weight, -jnp.inf)
    carried = within + level[:, None]
    top = jnp.maximum(carried, lax.optimization_barrier(jnp.max(log_weight, axis=-1)))
    weight = jnp.exp(log_weight - top[:, :, None])
    carried_weight = jnp.exp(carried - top) * scale
    scores = jnp.einsum('htd,hsd->hts', query, key, preferred_element_type=jnp.float32) * (scale * weight)
    numer = jnp.einsum('hts,hse->hte', scores.astype(jnp.bfloat16), value, preferred_element_type=jnp.float32)
    numer = numer + carried_weight[:, :, None] * jnp.einsum('hed,htd->hte', state.astype(jnp.bfloat16), query, preferred_element_type=jnp.float32)
    denom = lax.optimization_barrier(jnp.sum(scores, axis=-1)) + carried_weight * jnp.einsum('hd,htd->ht', normal.astype(jnp.bfloat16), query, preferred_element_type=jnp.float32)
    result = numer / jnp.maximum(jnp.abs(denom), 1.0)[:, :, None]
    last = within[:, -1]
    end_log = last[:, None] - within + gate_in
    new_level = jnp.maximum(last + level, lax.optimization_barrier(jnp.max(end_log, axis=-1)))
    keep = jnp.exp(last + level - new_level)
    fresh = jnp.exp(end_log - new_level[:, None])
    scaled_key = (fresh[:, :, None] * key).astype(jnp.bfloat16)
    new_state = keep[:, None, None] * state + jnp.einsum('hse,hsd->hed', value, scaled_key, preferred_element_type=jnp.float32)
    new_normal = keep[:, None] * normal + lax.optimization_barrier(jnp.sum(scaled_key.astype(jnp.float32), axis=1))
    return ((new_state, new_normal, new_level), result)

def depthwise(extended, kernel):
    taps = kernel.shape[0]
    length = extended.shape[0] - taps + 1
    total = extended[0:length] * kernel[0]
    for index in range(1, taps):
        total = total + extended[index:index + length] * kernel[index]
    return total

def reference(tokens, conv_value_weight, conv_gate_weight, conv_kernel, conv_norm_gain, query_weight, key_weight, value_weight, input_gate_weight, forget_gate_weight, input_offset, forget_offset, memory_norm_gain, conv_out_weight, memory_out_weight):

    def project(weight):
        return jnp.dot(tokens, weight, preferred_element_type=jnp.float32)
    glu = (project(conv_value_weight) * jax.nn.sigmoid(project(conv_gate_weight))).astype(jnp.bfloat16)
    extended = jnp.concatenate([jnp.zeros((KERNEL - 1, CONV), jnp.float32), glu.astype(jnp.float32)], axis=0)
    conv = depthwise(extended, conv_kernel.astype(jnp.float32))
    mean = lax.optimization_barrier(jnp.mean(conv, axis=1, keepdims=True))
    variance = lax.optimization_barrier(jnp.mean(conv * conv, axis=1, keepdims=True)) - mean * mean
    conv_branch = jax.nn.silu((conv - mean) * lax.rsqrt(variance + EPS) * conv_norm_gain).astype(jnp.bfloat16)

    def to_heads(weight):
        return project(weight).astype(jnp.bfloat16).reshape(SEQUENCE_TOKENS, MEMORY_HEADS, HEAD_DIM).transpose(1, 0, 2)
    query = to_heads(query_weight)
    key = to_heads(key_weight)
    value = to_heads(value_weight)
    gate_in = (project(input_gate_weight) + input_offset).T
    forget_log = jax.nn.log_sigmoid(project(forget_gate_weight) + forget_offset).T
    blocks = SEQUENCE_TOKENS // BLOCK

    def split(array):
        return jnp.moveaxis(array.reshape((MEMORY_HEADS, blocks, BLOCK) + array.shape[2:]), 1, 0)
    start_state = (jnp.zeros((MEMORY_HEADS, HEAD_DIM, HEAD_DIM), jnp.float32), jnp.zeros((MEMORY_HEADS, HEAD_DIM), jnp.float32), jnp.full((MEMORY_HEADS,), -1e+30, jnp.float32))
    _, hidden = lax.scan(block_step, start_state, (split(query), split(key), split(value), split(gate_in), split(forget_log)))
    hidden = jnp.moveaxis(hidden, 0, 1).reshape(MEMORY_HEADS, SEQUENCE_TOKENS, HEAD_DIM)
    hidden = hidden * lax.rsqrt(lax.optimization_barrier(jnp.mean(hidden * hidden, axis=(0, 2), keepdims=True)) + EPS)
    hidden = hidden * memory_norm_gain.reshape(MEMORY_HEADS, 1, HEAD_DIM)
    memory_branch = hidden.transpose(1, 0, 2).reshape(SEQUENCE_TOKENS, MEMORY_HEADS * HEAD_DIM).astype(jnp.bfloat16)
    conv_share = CONV // GROUPS
    memory_share = MEMORY_HEADS * HEAD_DIM // GROUPS
    mixed = jnp.zeros((SEQUENCE_TOKENS, D), jnp.float32)
    for group in range(GROUPS):
        conv_rows = slice(group * conv_share, (group + 1) * conv_share)
        memory_rows = slice(group * memory_share, (group + 1) * memory_share)
        partial_value = jnp.dot(conv_branch[:, conv_rows], conv_out_weight[conv_rows], preferred_element_type=jnp.float32)
        partial_value = partial_value + jnp.dot(memory_branch[:, memory_rows], memory_out_weight[memory_rows], preferred_element_type=jnp.float32)
        rounded = lax.optimization_barrier(partial_value.astype(jnp.bfloat16))
        mixed = mixed + rounded.astype(jnp.float32)
    return mixed.astype(jnp.bfloat16)
```

```python
import jax
import jax.numpy as jnp
from jax import lax
from jax.experimental import pallas as pl
from jax.experimental.pallas import tpu as pltpu
from jax.sharding import PartitionSpec as P

BLOCK = 64


EPS = 1e-06
LOWEST_LEVEL = -1e30


def shifted_2(value, axis, steps):
    count = lax.axis_size(axis)
    leading, last = (max(0, -steps), min(count, count - steps))
    return lax.ppermute(value, axis, [(source, source + steps) for source in range(leading, last)])


def carried_in(shard, axis, join, neutral):
    place = lax.axis_index(axis)
    gathered = jax.tree.map(
        lambda a, kind: lax.all_gather(a.astype(kind), axis),
        shard,
        (jnp.bfloat16, jnp.bfloat16, jnp.bfloat16, jnp.bfloat16),
    )
    state = jax.tree.map(lambda a, e: jnp.zeros_like(a) + jnp.asarray(e, a.dtype), shard, neutral)

    def one(step, state):
        return join(
            state,
            jax.tree.map(
                lambda a, own: lax.dynamic_index_in_dim(a, step, 0, False).astype(own.dtype),
                gathered,
                shard,
            ),
        )

    return lax.fori_loop(0, place, one, state)


def block_step(carry, inputs):
    state, normal, level = carry
    query, key, value, gate_in, forget_log = inputs
    length = gate_in.shape[-1]
    scale = query.shape[-1] ** (-0.5)
    causal = jnp.tril(jnp.ones((length, length), dtype=bool))
    within = jnp.cumsum(forget_log, axis=-1)
    log_weight = within[:, :, None] - within[:, None, :] + gate_in[:, None, :]
    log_weight = jnp.where(causal, log_weight, -jnp.inf)
    carried = within + level[:, None]
    top = jnp.maximum(carried, jnp.max(log_weight, axis=-1))
    weight = jnp.exp(log_weight - top[:, :, None])
    carried_weight = jnp.exp(carried - top) * scale
    scores = jnp.einsum("htd,hsd->hts", query, key, preferred_element_type=jnp.float32) * (
        scale * weight
    )
    numer = jnp.einsum(
        "hts,hse->hte", scores.astype(jnp.bfloat16), value, preferred_element_type=jnp.float32
    )
    numer = numer + carried_weight[:, :, None] * jnp.einsum(
        "hed,htd->hte", state.astype(jnp.bfloat16), query, preferred_element_type=jnp.float32
    )
    denom = jnp.sum(scores, axis=-1) + carried_weight * jnp.einsum(
        "hd,htd->ht", normal.astype(jnp.bfloat16), query, preferred_element_type=jnp.float32
    )
    result = numer / jnp.maximum(jnp.abs(denom), 1.0)[:, :, None]
    last = within[:, -1]
    end_log = last[:, None] - within + gate_in
    new_level = jnp.maximum(last + level, jnp.max(end_log, axis=-1))
    keep = jnp.exp(last + level - new_level)
    fresh = jnp.exp(end_log - new_level[:, None])
    scaled_key = (fresh[:, :, None] * key).astype(jnp.bfloat16)
    new_state = keep[:, None, None] * state + jnp.einsum(
        "hse,hsd->hed", value, scaled_key, preferred_element_type=jnp.float32
    )
    new_normal = keep[:, None] * normal + jnp.sum(scaled_key.astype(jnp.float32), axis=1)
    return ((new_state, new_normal, new_level), result)


def depthwise(extended, kernel):
    taps = kernel.shape[0]
    length = extended.shape[0] - taps + 1
    total = extended[0:length] * kernel[0]
    for index in range(1, taps):
        total = total + extended[index : index + length] * kernel[index]
    return total


def merge_states(first, second):
    first_state, first_normal, first_level, first_total = first
    second_state, second_normal, second_level, second_total = second
    shifted = first_level + second_total
    level = jnp.maximum(shifted, second_level)
    older = jnp.exp(shifted - level)
    newer = jnp.exp(second_level - level)
    state = older[:, None, None] * first_state + newer[:, None, None] * second_state
    normal = older[:, None] * first_normal + newer[:, None] * second_normal
    return (state, normal, level, first_total + second_total)


def on_device_by_position(
    tokens,
    conv_value_weight,
    conv_gate_weight,
    conv_kernel,
    conv_norm_gain,
    query_weight,
    key_weight,
    value_weight,
    input_gate_weight,
    forget_gate_weight,
    input_offset,
    forget_offset,
    memory_norm_gain,
    conv_out_weight,
    memory_out_weight,
):
    length = tokens.shape[0]
    heads_here = input_gate_weight.shape[1]
    whole = lax.all_gather(tokens, "tp", axis=1, tiled=True)
    pieces = (
        lax.all_gather(conv_value_weight, "sp", axis=0, tiled=True),
        lax.all_gather(conv_gate_weight, "sp", axis=0, tiled=True),
        lax.all_gather(query_weight, "sp", axis=0, tiled=True),
        lax.all_gather(key_weight, "sp", axis=0, tiled=True),
        lax.all_gather(value_weight, "sp", axis=0, tiled=True),
    )
    folded = tuple((jnp.dot(whole, piece, preferred_element_type=jnp.float32) for piece in pieces))
    conv_value, conv_gate, query_flat, key_flat, value_flat = folded
    gate_pre = jnp.dot(whole, input_gate_weight, preferred_element_type=jnp.float32)
    forget_pre = jnp.dot(whole, forget_gate_weight, preferred_element_type=jnp.float32)
    glu = (conv_value * jax.nn.sigmoid(conv_gate)).astype(jnp.bfloat16)
    taps = conv_kernel.shape[0]
    head_dim = query_flat.shape[1] // heads_here

    def to_heads(flat):
        return flat.astype(jnp.bfloat16).reshape(length, heads_here, head_dim).transpose(1, 0, 2)

    query = to_heads(query_flat)
    key = to_heads(key_flat)
    value = to_heads(value_flat)
    gate_in = (gate_pre + input_offset).T
    forget_log = jax.nn.log_sigmoid(forget_pre + forget_offset).T
    within = jnp.cumsum(forget_log, axis=1)
    total = within[:, -1]
    end_log = total[:, None] - within + gate_in
    local_level = jnp.max(end_log, axis=1)
    fresh = jnp.exp(end_log - local_level[:, None])
    scaled_key = (fresh[:, :, None] * key).astype(jnp.bfloat16)
    local_state = jnp.einsum("hse,hsd->hed", value, scaled_key, preferred_element_type=jnp.float32)
    local_normal = jnp.sum(scaled_key.astype(jnp.float32), axis=1)
    blank_state = (
        jnp.zeros_like(local_state),
        jnp.zeros_like(local_normal),
        jnp.full_like(local_level, LOWEST_LEVEL),
        jnp.zeros_like(total),
    )
    prior = shifted_2(glu[length - (taps - 1) :], "sp", 1)
    incoming = carried_in(
        (local_state, local_normal, local_level, total), "sp", merge_states, blank_state
    )
    extended = jnp.concatenate([prior, glu], axis=0).astype(jnp.float32)
    conv = depthwise(extended, conv_kernel.astype(jnp.float32))
    blocks = length // BLOCK

    def split(array):
        return jnp.moveaxis(array.reshape((heads_here, blocks, BLOCK) + array.shape[2:]), 1, 0)

    _, hidden = lax.scan(
        block_step,
        tuple(incoming[:3]),
        (split(query), split(key), split(value), split(gate_in), split(forget_log)),
    )
    hidden = jnp.moveaxis(hidden, 0, 1).reshape(heads_here, length, head_dim)
    hidden_squares = jnp.sum(hidden * hidden, axis=(0, 2))
    channel_sum, channel_squares, memory_squares = lax.psum(
        (jnp.sum(conv, axis=1), jnp.sum(conv * conv, axis=1), hidden_squares), "tp"
    )
    channels = conv.shape[1] * lax.axis_size("tp")
    mean = (channel_sum / channels)[:, None]
    variance = (channel_squares / channels)[:, None] - mean * mean
    conv_branch = jax.nn.silu((conv - mean) * lax.rsqrt(variance + EPS) * conv_norm_gain).astype(
        jnp.bfloat16
    )
    entries = heads_here * head_dim * lax.axis_size("tp")
    memory_scale = lax.rsqrt(memory_squares / entries + EPS)
    hidden = hidden * memory_scale[None, :, None]
    hidden = hidden * memory_norm_gain.reshape(heads_here, 1, head_dim)
    memory_branch = (
        hidden.transpose(1, 0, 2).reshape(length, heads_here * head_dim).astype(jnp.bfloat16)
    )
    conv_columns, memory_columns = (
        lax.all_gather(conv_out_weight, "sp", axis=1, tiled=True),
        lax.all_gather(memory_out_weight, "sp", axis=1, tiled=True),
    )
    contract = (((0,), (1,)), ((), ()))
    summed = lax.psum_scatter(
        (
            lax.dot_general(conv_columns, conv_branch, contract, preferred_element_type=jnp.float32)
            + lax.dot_general(
                memory_columns, memory_branch, contract, preferred_element_type=jnp.float32
            )
        ).astype(jnp.bfloat16),
        "tp",
        scatter_dimension=0,
        tiled=True,
    ).astype(jnp.float32)
    return summed.T.astype(jnp.bfloat16)


MESH = pl.DeviceIdType.MESH
IN_VMEM = pl.BlockSpec(memory_space=pltpu.VMEM)
SENDS = 224
ROW_TILE = 8
LANES = 128
NT = (((1,), (1,)), ((), ()))


def when(conditions, action):
    if not conditions:
        action()
        return
    every = conditions[0]
    for condition in conditions[1:]:
        every = jnp.logical_and(every, condition)
    pl.when(every)(action)


class Sends:
    def __init__(self, semaphores):
        self.semaphores = semaphores
        self.started = []

    def start(self, source, target, arrival, device, *conditions):
        copy = pltpu.make_async_remote_copy(
            src_ref=source,
            dst_ref=target,
            send_sem=self.semaphores.at[len(self.started)],
            recv_sem=arrival,
            device_id=device,
            device_id_type=MESH,
        )
        self.started.append((copy, conditions))
        when(conditions, copy.start)

    def finish(self):
        for copy, conditions in self.started:
            when(conditions, copy.wait_send)


def arrived(block, semaphore, *conditions):
    copy = pltpu.make_async_remote_copy(
        src_ref=block,
        dst_ref=block,
        send_sem=semaphore,
        recv_sem=semaphore,
        device_id=(lax.axis_index("sp"), lax.axis_index("tp")),
        device_id_type=MESH,
    )
    when(conditions, copy.wait_recv)


def line_order(here, count):
    order = []
    for distance in range(1, count):
        order.append((here - distance, here >= distance, here + 1, here + 1 < count))
        order.append((here + distance, here + distance < count, here - 1, here > 0))
    return order


def pick(index, first, second):
    return jnp.where(jnp.full(first.shape, index, jnp.int32) == 1, second, first)


def stacked(rows, length):
    place = lax.broadcasted_iota(jnp.int32, (ROW_TILE, length), 0)
    result = jnp.zeros((ROW_TILE, length), jnp.float32)
    for index, row in enumerate(rows):
        result = jnp.where(place == index, row, result)
    return result


def as_columns(rows):
    length = rows.shape[1]
    rest = jnp.zeros((LANES - ROW_TILE, length), jnp.float32)
    return jnp.concatenate([rows, rest], axis=0).T


def as_rows(columns):
    length = columns[0].shape[0]
    place = lax.broadcasted_iota(jnp.int32, (length, LANES), 1)
    result = jnp.zeros((length, LANES), jnp.float32)
    for index, column in enumerate(columns):
        result = jnp.where(place == index, column, result)
    return result.T[:ROW_TILE]


def prefix_sums(rows):
    before = lax.broadcasted_iota(jnp.int32, (LANES, LANES), 0)
    after = lax.broadcasted_iota(jnp.int32, (LANES, LANES), 1)
    upper = (before <= after).astype(jnp.float32)
    carry = jnp.zeros((ROW_TILE, 1), jnp.float32)
    parts = []
    for start in range(0, rows.shape[1], LANES):
        part = carry + jnp.dot(
            rows[:, start : start + LANES],
            upper,
            precision=lax.Precision.HIGHEST,
            preferred_element_type=jnp.float32,
        )
        carry = part[:, LANES - 1 :]
        parts.append(part)
    return jnp.concatenate(parts, axis=1)


def layer_kernel(
    count,
    columns,
    tokens,
    wq,
    wk,
    wv,
    wcv,
    wcg,
    own_taps,
    own_conv_gain,
    own_memory_gain,
    own_input_gates,
    own_forget_gates,
    own_input_offsets,
    own_forget_offsets,
    own_memory_out,
    own_conv_out,
    slots,
    lines,
    weights,
    product,
    taps,
    conv_gain,
    memory_gain,
    input_gates,
    forget_gates,
    offsets,
    gate_rows,
    level_before,
    level_here,
    keys,
    values,
    queries,
    weight_near,
    weight_far,
    memory_done,
    squares_done,
    squares_in,
    extended,
    conv,
    sums_done,
    sums_in,
    conv_done,
    memory_in,
    conv_in,
    memory_out,
    conv_out,
    partial,
    send_sem,
    token_sem,
    weight_sem,
    own_sem,
    offset_sem,
    level_sem,
    pair_sem,
    query_sem,
    halo_sem,
    sums_sem,
    squares_sem,
    memory_sem,
    conv_sem,
    memory_out_sem,
    conv_out_sem,
    slot_sem,
):
    f32, bf16 = jnp.float32, jnp.bfloat16
    me, tp = lax.axis_index("sp"), lax.axis_index("tp")
    layers = count // 2
    z, x, y, core = me // 2, lax.rem(me, 2), tp // 2, lax.rem(tp, 2)
    side, odd = z // 2, lax.rem(z, 2)
    length, features = tokens.shape
    depth, head_dim = wq.shape[0], wq.shape[1] // 2
    channels = wcv.shape[1] // 2
    rows = 4 * length
    near, far = core == side, core != side
    first, second = x == 0, x == 1
    peer = (me, y * 2 + 1 - core)
    below, above = (me - 2, tp), (me + 2, tp)
    x_side = (z * 2 + 1 - x, tp)
    y_side = (me, (1 - y) * 2 + core)
    has_below, has_above = z > 0, z + 1 < layers
    sends = Sends(send_sem)

    barrier = pltpu.get_barrier_semaphore()
    devices = count * columns
    rank = me * columns + tp
    for step in range(1, devices):
        other = lax.rem(rank + step, devices)
        pl.semaphore_signal(
            barrier,
            inc=1,
            device_id=(other // columns, lax.rem(other, columns)),
            device_id_type=MESH,
        )

    def block(i, j):
        return lines.at[
            pl.ds(pl.multiple_of(i * length, length), length),
            pl.ds(pl.multiple_of(j * features, features), features),
        ]

    place = odd * 2 + x

    @pl.when(near)
    def _():
        lines[
            pl.ds(pl.multiple_of(place * length, length), length),
            pl.ds(pl.multiple_of(tp * features, features), features),
        ] = tokens[...]

    pl.semaphore_wait(barrier, devices - 1)

    goal = y * 2 + side
    mine, mine_sem = block(place, tp), token_sem.at[place, tp]
    sends.start(tokens, mine, mine_sem, (me - 2, goal), has_below)
    sends.start(tokens, mine, mine_sem, (me + 2, goal), has_above)
    sends.start(tokens, mine, mine_sem, (z * 2 + 1 - x, goal))
    sends.start(tokens, mine, mine_sem, (me, (1 - y) * 2 + side))
    sends.start(tokens, mine, mine_sem, peer, far)

    def piece(unit, i):
        return weights.at[
            pl.ds(pl.multiple_of(i * depth, depth), depth),
            unit * head_dim : (unit + 1) * head_dim,
        ]

    def shares(k, x_goal):
        whole = slice(k * head_dim, (k + 1) * head_dim)
        part = slice(k * channels, (k + 1) * channels)
        if x_goal == 0:
            return ((wk.at[:, whole], 0, 0), (wv.at[:, whole], 1, head_dim))
        return (
            (wq.at[:, whole], 0, 0),
            (wcv.at[:, part], 1, head_dim),
            (wcg.at[:, part], 1, head_dim + channels),
        )

    own_rows = pl.ds(pl.multiple_of(me * depth, depth), depth)

    def send_weights(k, x_goal, to_peer, *conditions):
        for source, unit, start in shares(k, x_goal):
            goal = peer if to_peer else ((core * 2 + k) * 2 + x_goal, y * 2 + unit)
            target = weights.at[own_rows, start : start + source.shape[1]]
            sends.start(source, target, weight_sem.at[unit, me], goal, *conditions)

    for k in (1, 0):
        for x_goal in range(2):
            send_weights(k, x_goal, False, core * 2 + k != z)
    for k in range(2):
        for x_goal in range(2):
            home = (core * 2 + k == z, x == x_goal)
            send_weights(k, x_goal, True, *home)

            def keep():
                for source, _, start in shares(k, x_goal):
                    weights[own_rows, start : start + source.shape[1]] = source[...]

            when(home, keep)

    for index, (source, target) in enumerate(
        (
            (own_taps, taps),
            (own_conv_gain, conv_gain),
            (own_memory_gain, memory_gain),
            (own_input_gates, input_gates),
            (own_forget_gates, forget_gates),
        )
    ):
        sends.start(source, target, own_sem.at[index], peer, near)

        @pl.when(near)
        def _():
            target[...] = source[...]

    for k in range(2):
        goal = ((core * 2 + k) * 2, y * 2 + side)
        here = jnp.logical_and(near, jnp.logical_and(first, core * 2 + k == z))
        for kind, source in enumerate((own_input_offsets, own_forget_offsets)):
            target = offsets.at[place, kind]
            sends.start(source, target, offset_sem.at[place], goal, jnp.logical_not(here))

            @pl.when(here)
            def _():
                target[...] = source[...]

    k_near = jnp.where(near, odd, 1 - core)
    groups = []
    for k in (k_near, 1 - k_near):
        source = core * 2 + k
        groups.append((source, k * 2 + x, k * 2 + 1 - x))
    for source, i, _ in groups:
        away, up = source != z, source < z
        for j in (y * 2, y * 2 + 1):
            spot, sem = block(i, j), token_sem.at[i, j]
            arrived(spot, sem, jnp.logical_or(away, j != tp))
            sends.start(spot, spot, sem, above, away, up, has_above)
            sends.start(spot, spot, sem, below, away, jnp.logical_not(up), has_below)
            sends.start(spot, spot, sem, x_side, away)
            sends.start(spot, spot, sem, y_side, away)
    for k in range(2):
        for x_goal in range(2):
            send_weights(k, x_goal, False, core * 2 + k == z, x != x_goal)
    for _, _, i in groups:
        for j in (y * 2, y * 2 + 1):
            spot, sem = block(i, j), token_sem.at[i, j]
            arrived(spot, sem)
            sends.start(spot, spot, sem, y_side)

    def both_units(i, *conditions):
        part = weights.at[pl.ds(pl.multiple_of(i * depth, depth), depth), :]
        for unit in range(2):
            conditional = (core == unit,) + conditions
            arrived(piece(unit, i), weight_sem.at[unit, i], *conditional)
            sends.start(piece(unit, i), piece(unit, i), weight_sem.at[unit, i], peer, *conditional)

    def other_unit(i, *conditions):
        for unit in range(2):
            arrived(piece(unit, i), weight_sem.at[unit, i], core != unit, *conditions)

    z_mate = side * 2 + 1 - odd
    near_sources = (z * 2 + 1 - x, z_mate * 2 + x, z_mate * 2 + 1 - x)
    for i in near_sources:
        both_units(i)
    for i in range(4):
        for j in ((1 - y) * 2, (1 - y) * 2 + 1):
            arrived(block(i, j), token_sem.at[i, j])
    for i in near_sources:
        other_unit(i)
    for unit in range(2):
        arrived(piece(unit, me), weight_sem.at[unit, me], far)

    def multiply(start, size):
        part = pl.ds(pl.multiple_of(start, size), size)
        return jnp.dot(lines[:, part], weights[part, :], preferred_element_type=f32)

    half = count // 2 * depth
    product[...] = multiply(side * half, half)

    for index, target in enumerate((taps, conv_gain, memory_gain, input_gates, forget_gates)):
        arrived(target, own_sem.at[index], far)
    for i in range(4):
        here = jnp.logical_and(near, place == i)
        arrived(offsets.at[i], offset_sem.at[i], first, jnp.logical_not(here))

    @pl.when(first)
    def _():
        gate_rows[...] = jnp.zeros_like(gate_rows)
        gate_rows[0:2, :] = input_gates[...].astype(f32)
        gate_rows[2:4, :] = forget_gates[...].astype(f32)
        gates = lax.dot_general(
            lines[...], gate_rows[...].astype(bf16), NT, preferred_element_type=f32
        ).T
        shift = [jnp.concatenate([offsets[i, kind] for i in range(4)], 1) for kind in range(2)]
        gate_in = pick(odd, gates[0:1] + shift[0][0:1], gates[1:2] + shift[0][1:2])
        forget = pick(odd, gates[2:3] + shift[1][0:1], gates[3:4] + shift[1][1:2])
        forget_log = jnp.minimum(forget, 0.0) - jnp.log1p(jnp.exp(-jnp.abs(forget)))
        coarse = jnp.round(forget_log * 8.0) * 0.125
        within = prefix_sums(stacked((coarse, forget_log - coarse), rows))
        which = lax.broadcasted_iota(jnp.int32, (ROW_TILE, rows), 0)
        level_here[...] = jnp.where(which == 2, gate_in, within)

    first_core, second_core = core == 0, core == 1
    sends.start(level_here, level_before, level_sem.at[0], peer, first, first_core)
    arrived(level_before, level_sem.at[0], first, second_core)

    @pl.when(jnp.logical_and(first, first_core))
    def _():
        level_before[...] = jnp.zeros_like(level_before)
        keys[:rows, :] = jnp.zeros_like(keys[:rows, :])
        values[:rows, :] = jnp.zeros_like(values[:rows, :])

    span = rows // 2
    scale = head_dim ** (-0.5)
    reach = (rows + span, 2 * rows)
    stores = (weight_near, weight_far)

    @pl.when(first)
    def _():
        before = level_before[...]
        which = lax.broadcasted_iota(jnp.int32, (ROW_TILE, rows), 0)
        here = level_here[...] + jnp.where(which < 2, before[:, rows - 1 :], 0.0)
        from_rows = jnp.concatenate([before, here], axis=1)
        to_columns = as_columns(here)
        tile = 64
        for start in range(0, rows, tile):
            index = start // span
            width = reach[index]
            to = to_columns[start : start + tile]
            log_weight = (
                (to[:, 0:1] - from_rows[0:1, :width])
                + (to[:, 1:2] - from_rows[1:2, :width])
                + from_rows[2:3, :width]
            )
            at = lax.broadcasted_iota(jnp.int32, (tile, width), 1)
            until = lax.broadcasted_iota(jnp.int32, (tile, width), 0) + (start + rows)
            seen = jnp.logical_and(at <= until, at >= rows * (1 - core))
            log_weight = jnp.where(seen, log_weight, -jnp.inf)
            weight = jnp.exp(log_weight - jnp.max(log_weight, axis=1, keepdims=True)) * scale
            stores[index][start - index * span : start - index * span + tile, :] = weight

    own_part = x * 2 + core

    def send_out(*conditions):
        for device in (peer, x_side):
            sends.start(
                own_memory_out,
                memory_out.at[own_part],
                memory_out_sem.at[own_part],
                device,
                *conditions,
            )
            sends.start(
                own_conv_out, conv_out.at[own_part], conv_out_sem.at[own_part], device, *conditions
            )

    send_out(first)
    memory_out[own_part] = own_memory_out[...]
    conv_out[own_part] = own_conv_out[...]

    far_pairs = (
        jnp.where(side == 0, 2, 1),
        jnp.where(side == 0, 3, 0),
    )
    for pair in far_pairs:
        both_units(pair * 2 + x)
        both_units(pair * 2 + 1 - x)
    for pair in far_pairs:
        other_unit(pair * 2)
        other_unit(pair * 2 + 1)
        product[...] += multiply(pair * 2 * depth, 2 * depth)

    @pl.when(second)
    def _():
        queries[...] = product[:, :head_dim].astype(bf16)

    for index in range(2):
        part = queries.at[index * span : (index + 1) * span, :]
        sends.start(part, part, query_sem.at[index], x_side, second)
    send_out(second)

    @pl.when(first)
    def _():
        keys[rows:, :] = product[:, :head_dim].astype(bf16)
        values[rows:, :] = product[:, head_dim:].astype(bf16)

    for index, array in enumerate((keys, values)):
        target = array.at[:rows, :]
        sends.start(array.at[rows:, :], target, pair_sem.at[index], peer, first, first_core)

    halo = extended.shape[0] - rows

    @pl.when(second)
    def _():
        gated = product[:, head_dim : head_dim + channels] * jax.nn.sigmoid(
            product[:, head_dim + channels :]
        )
        extended[halo:, :] = gated.astype(bf16).astype(f32)

    sends.start(
        extended.at[rows:, :], extended.at[:halo, :], halo_sem.at[0], peer, second, first_core
    )

    @pl.when(jnp.logical_and(second, first_core))
    def _():
        extended[:halo, :] = jnp.zeros((halo, channels), f32)

    arrived(extended.at[:halo, :], halo_sem.at[0], second, second_core)
    source_index = y * layers + z

    @pl.when(second)
    def _():
        number = taps.shape[0]
        kernel = taps[...].astype(f32)
        kernel = pick(odd, kernel[:, :channels], kernel[:, channels:])
        for start in range(0, rows, length):
            base = start + halo - (number - 1)
            total = extended[base : base + length, :] * kernel[0:1]
            for index in range(1, number):
                total = total + (
                    extended[base + index : base + index + length, :] * kernel[index : index + 1]
                )
            conv[start : start + length, :] = total
        all_rows = conv[...]
        sums_done[...] = as_rows(
            (
                jnp.sum(all_rows, axis=1, keepdims=True),
                jnp.sum(all_rows * all_rows, axis=1, keepdims=True),
            )
        )
        sums_in[source_index] = sums_done[...]

    sources = [(z_other, y_other) for z_other in range(layers) for y_other in range(2)]
    for z_other, y_other in sources:
        away = jnp.logical_or(z != z_other, y != y_other)
        sends.start(
            sums_done,
            sums_in.at[source_index],
            sums_sem.at[source_index],
            (z_other * 2 + 1, y_other * 2 + core),
            second,
            away,
        )
    for z_other, y_other in sources:
        away = jnp.logical_or(z != z_other, y != y_other)
        index = y_other * layers + z_other
        arrived(sums_in.at[index], sums_sem.at[index], second, away)

    @pl.when(second)
    def _():
        total = sums_in[0]
        for index in range(1, 2 * layers):
            total = total + sums_in[index]
        total = total * (1.0 / (2 * layers * channels))
        mean = total[0:1]
        inverse = lax.rsqrt(total[1:2] - mean * mean + EPS)
        across = as_columns(stacked((mean, inverse), rows))
        gain = conv_gain[...]
        gain = pick(odd, gain[:, :channels], gain[:, channels:])
        normed = (conv[...] - across[:, 0:1]) * across[:, 1:2] * gain
        conv_done[...] = (normed * jax.nn.sigmoid(normed)).astype(bf16)

    def spread(done, inside, semaphores, home, index):
        here, away = x == home, x != home
        kept = done.at[(2 * index + home) * length : (2 * index + home + 1) * length, :]
        given = done.at[(2 * index + 1 - home) * length : (2 * index + 2 - home) * length, :]
        part = slice(index * length, (index + 1) * length)
        target, sem = inside.at[z, part, :], semaphores.at[z, index]
        sends.start(kept, target, sem, below, here, has_below)
        sends.start(kept, target, sem, above, here, has_above)
        sends.start(given, target, sem, x_side, here)

        @pl.when(here)
        def _():
            inside[z, part, :] = kept[...]

    for index in range(2):
        spread(conv_done, conv_in, conv_sem, 1, index)

    for index, array in enumerate((keys, values)):
        arrived(array.at[:rows, :], pair_sem.at[index], first, second_core)
    squares_index = source_index
    for index in range(2):
        arrived(
            queries.at[index * span : (index + 1) * span, :], query_sem.at[index], first
        )

        @pl.when(first)
        def _():
            width = reach[index]
            gain = memory_gain[...]
            gain = pick(odd, gain[:, :head_dim], gain[:, head_dim:])
            squares = []
            for inner in range(2):
                start = index * span + inner * length
                scores = lax.dot_general(
                    queries[start : start + length, :],
                    keys[:width, :],
                    NT,
                    preferred_element_type=f32,
                )
                scores = scores * stores[index][inner * length : (inner + 1) * length, :]
                numer = jnp.dot(
                    scores.astype(bf16), values[:width, :], preferred_element_type=f32
                )
                denom = jnp.sum(scores, axis=1, keepdims=True)
                cell = numer / jnp.maximum(jnp.abs(denom), 1.0)
                memory_done[start : start + length, :] = (cell * gain).astype(bf16)
                squares.append(jnp.sum(cell * cell, axis=1, keepdims=True))
            squares_done[index] = as_rows((jnp.concatenate(squares, axis=0),))
            squares_in[squares_index, index] = squares_done[index]

        spread(memory_done, memory_in, memory_sem, 0, index)
        for z_other, y_other in sources:
            for x_other in range(2):
                away = jnp.logical_or(
                    jnp.logical_or(z != z_other, y != y_other), x != x_other
                )
                sends.start(
                    squares_done.at[index],
                    squares_in.at[squares_index, index],
                    squares_sem.at[squares_index, index],
                    (z_other * 2 + x_other, y_other * 2 + core),
                    first,
                    away,
                )

    across = (1 - x) * 2 + core
    arrived(memory_out.at[across], memory_out_sem.at[across])
    sends.start(memory_out.at[across], memory_out.at[across], memory_out_sem.at[across], peer)
    arrived(conv_out.at[across], conv_out_sem.at[across])
    sends.start(conv_out.at[across], conv_out.at[across], conv_out_sem.at[across], peer)

    order = line_order(z, layers)
    kinds = ((conv_in, conv_sem, 1), (memory_in, memory_sem, 0))
    entries = layers * 2 * head_dim
    for index in range(2):
        part = slice(index * length, (index + 1) * length)
        for inside, semaphores, home in kinds:
            away = x != home
            spot, sem = inside.at[z, part, :], semaphores.at[z, index]
            arrived(spot, sem, away)
            sends.start(spot, spot, sem, below, away, has_below)
            sends.start(spot, spot, sem, above, away, has_above)
        for source, there, onward, further in order:
            for inside, semaphores, _ in kinds:
                spot, sem = inside.at[source, part, :], semaphores.at[source, index]
                arrived(spot, sem, there)
                sends.start(spot, spot, sem, (onward * 2 + x, tp), there, further)
        for z_other, y_other in sources:
            own = jnp.logical_and(first, jnp.logical_and(z == z_other, y == y_other))
            slot = y_other * layers + z_other
            arrived(
                squares_in.at[slot, index], squares_sem.at[slot, index], jnp.logical_not(own)
            )
        if index == 0:
            for group in range(2):
                part_out = group * 2 + 1 - core
                arrived(memory_out.at[part_out], memory_out_sem.at[part_out])
                arrived(conv_out.at[part_out], conv_out_sem.at[part_out])
        total = squares_in[0, index]
        for slot in range(1, 2 * layers):
            total = total + squares_in[slot, index]
        total = pick(x, total[:, :length], total[:, length:])
        row_scale = as_columns(lax.rsqrt(total * (1.0 / entries) + EPS))[:, 0:1]
        for group in range(2):
            from_memory, from_conv = None, None
            for head in range(layers):
                where = group * 2 + head // 2
                inner = head % 2
                memory_term = jnp.dot(
                    memory_in[head, part, :],
                    memory_out[where, inner * head_dim : (inner + 1) * head_dim, :],
                    preferred_element_type=f32,
                )
                conv_term = jnp.dot(
                    conv_in[head, part, :],
                    conv_out[where, inner * channels : (inner + 1) * channels, :],
                    preferred_element_type=f32,
                )
                from_memory = memory_term if head == 0 else from_memory + memory_term
                from_conv = conv_term if head == 0 else from_conv + conv_term
            width = from_memory.shape[1]
            partial[index, :, group * width : (group + 1) * width] = (
                from_conv + row_scale * from_memory
            ).astype(bf16)
        goal = ((core * 2 + index) * 2 + x, z)
        away = jnp.logical_or(core * 2 + index != z, tp != z)
        sends.start(partial.at[index], slots.at[y], slot_sem.at[y], goal, away)

        @pl.when(jnp.logical_not(away))
        def _():
            slots[y] = partial[index]

    for y_other in range(2):
        own = jnp.logical_and(tp == z, jnp.logical_and(y == y_other, core == side))
        arrived(slots.at[y_other], slot_sem.at[y_other], jnp.logical_not(own))
    sends.finish()


def layer(arrays):
    count, columns = lax.axis_size("sp"), lax.axis_size("tp")
    (
        tokens,
        conv_value_weight,
        conv_gate_weight,
        conv_kernel,
        conv_norm_gain,
        query_weight,
        key_weight,
        value_weight,
        input_gate_weight,
        forget_gate_weight,
        input_offset,
        forget_offset,
        memory_norm_gain,
        conv_out_weight,
        memory_out_weight,
    ) = arrays
    length, features = tokens.shape
    depth, head_dim = query_weight.shape[0], query_weight.shape[1] // 2
    channels = conv_value_weight.shape[1] // 2
    wide = features * columns
    rows = length * count // 2
    layers = count // 2
    taps = conv_kernel.shape[0]
    halo = -(-(taps - 1) // ROW_TILE) * ROW_TILE
    width = memory_out_weight.shape[1]
    f32, bf16 = jnp.float32, jnp.bfloat16
    DMA = pltpu.SemaphoreType.DMA
    V = pltpu.VMEM
    return pl.pallas_call(
        lambda *refs: layer_kernel(count, columns, *refs),
        out_shape=jax.ShapeDtypeStruct((2, length, features), bf16),
        in_specs=[IN_VMEM] * 15,
        out_specs=IN_VMEM,
        scratch_shapes=[
            V((rows, wide), bf16),
            V((wide, 2 * head_dim), bf16),
            V((rows, 2 * head_dim), f32),
            V(conv_kernel.shape, bf16),
            V((1, 2 * channels), f32),
            V((1, 2 * head_dim), f32),
            V((2, wide), bf16),
            V((2, wide), bf16),
            V((4, 2, 2, length), f32),
            V((LANES, wide), f32),
            V((ROW_TILE, rows), f32),
            V((ROW_TILE, rows), f32),
            V((2 * rows, head_dim), bf16),
            V((2 * rows, head_dim), bf16),
            V((rows, head_dim), bf16),
            V((rows // 2, rows + rows // 2), f32),
            V((rows // 2, 2 * rows), f32),
            V((rows, head_dim), bf16),
            V((2, ROW_TILE, rows // 2), f32),
            V((count, 2, ROW_TILE, rows // 2), f32),
            V((halo + rows, channels), f32),
            V((rows, channels), f32),
            V((ROW_TILE, rows), f32),
            V((count, ROW_TILE, rows), f32),
            V((rows, channels), bf16),
            V((layers, rows // 2, head_dim), bf16),
            V((layers, rows // 2, channels), bf16),
            V((4, 2 * head_dim, width), bf16),
            V((4, 2 * channels, width), bf16),
            V((2, length, features), bf16),
            DMA((SENDS,)),
            DMA((4, columns)),
            DMA((2, count)),
            DMA((5,)),
            DMA((4,)),
            DMA((1,)),
            DMA((2,)),
            DMA((2,)),
            DMA((1,)),
            DMA((count,)),
            DMA((count, 2)),
            DMA((layers, 2)),
            DMA((layers, 2)),
            DMA((4,)),
            DMA((4,)),
            DMA((2,)),
        ],
        compiler_params=pltpu.CompilerParams(collective_id=0, has_side_effects=True),
    )(
        tokens,
        query_weight,
        key_weight,
        value_weight,
        conv_value_weight,
        conv_gate_weight,
        conv_kernel,
        conv_norm_gain.reshape(1, -1),
        memory_norm_gain.reshape(1, -1),
        input_gate_weight.T,
        forget_gate_weight.T,
        input_offset.T,
        forget_offset.T,
        memory_out_weight,
        conv_out_weight,
    )


def on_device_by_column(*arrays):
    slots = layer(arrays)
    return jnp.sum(slots.astype(jnp.float32), axis=0).astype(jnp.bfloat16)


def splits_by_column(mesh, tokens, query_weight, conv_value_weight, conv_kernel, input_gate_weight):
    count, columns = mesh.shape["sp"], mesh.shape["tp"]
    heads = input_gate_weight.shape[1]
    head_dim = query_weight.shape[1] // heads
    length = tokens.shape[0] // count
    return (
        count == 8
        and columns == 4
        and heads == count
        and length % LANES == 0
        and tokens.size * 2 <= 4 * 2**20
        and conv_value_weight.shape[1] * 2 == head_dim * heads
        and head_dim == 256
        and conv_kernel.shape[0] - 1 <= length
    )


def solution(mesh):
    in_specs = (
        P("sp", "tp"),
        P("sp", "tp"),
        P("sp", "tp"),
        P(None, "tp"),
        P("tp"),
        P("sp", "tp"),
        P("sp", "tp"),
        P("sp", "tp"),
        P(None, "tp"),
        P(None, "tp"),
        P("sp", "tp"),
        P("sp", "tp"),
        P("tp"),
        P("tp", "sp"),
        P("tp", "sp"),
    )
    out_specs = P("sp", "tp")

    def run(*arrays):
        by_column = splits_by_column(
            mesh, arrays[0], arrays[5], arrays[1], arrays[3], arrays[8]
        )
        on_device = on_device_by_column if by_column else on_device_by_position
        return jax.shard_map(
            on_device, mesh=mesh, in_specs=in_specs, out_specs=out_specs, check_vma=False
        )(*arrays)

    return run
```

```python
import jax
import jax.numpy as jnp
from jax import lax
from jax.experimental import pallas as pl
from jax.experimental.pallas import tpu as pltpu
from jax.sharding import PartitionSpec as P

BLOCK = 64


EPS = 1e-06
LOWEST_LEVEL = -1e30


def shifted_2(value, axis, steps):
    count = lax.axis_size(axis)
    leading, last = (max(0, -steps), min(count, count - steps))
    return lax.ppermute(value, axis, [(source, source + steps) for source in range(leading, last)])


def carried_in(shard, axis, join, neutral):
    place = lax.axis_index(axis)
    gathered = jax.tree.map(
        lambda a, kind: lax.all_gather(a.astype(kind), axis),
        shard,
        (jnp.bfloat16, jnp.bfloat16, jnp.bfloat16, jnp.bfloat16),
    )
    state = jax.tree.map(lambda a, e: jnp.zeros_like(a) + jnp.asarray(e, a.dtype), shard, neutral)

    def one(step, state):
        return join(
            state,
            jax.tree.map(
                lambda a, own: lax.dynamic_index_in_dim(a, step, 0, False).astype(own.dtype),
                gathered,
                shard,
            ),
        )

    return lax.fori_loop(0, place, one, state)


def block_step(carry, inputs):
    state, normal, level = carry
    query, key, value, gate_in, forget_log = inputs
    length = gate_in.shape[-1]
    scale = query.shape[-1] ** (-0.5)
    causal = jnp.tril(jnp.ones((length, length), dtype=bool))
    within = jnp.cumsum(forget_log, axis=-1)
    log_weight = within[:, :, None] - within[:, None, :] + gate_in[:, None, :]
    log_weight = jnp.where(causal, log_weight, -jnp.inf)
    carried = within + level[:, None]
    top = jnp.maximum(carried, jnp.max(log_weight, axis=-1))
    weight = jnp.exp(log_weight - top[:, :, None])
    carried_weight = jnp.exp(carried - top) * scale
    scores = jnp.einsum("htd,hsd->hts", query, key, preferred_element_type=jnp.float32) * (
        scale * weight
    )
    numer = jnp.einsum(
        "hts,hse->hte", scores.astype(jnp.bfloat16), value, preferred_element_type=jnp.float32
    )
    numer = numer + carried_weight[:, :, None] * jnp.einsum(
        "hed,htd->hte", state.astype(jnp.bfloat16), query, preferred_element_type=jnp.float32
    )
    denom = jnp.sum(scores, axis=-1) + carried_weight * jnp.einsum(
        "hd,htd->ht", normal.astype(jnp.bfloat16), query, preferred_element_type=jnp.float32
    )
    result = numer / jnp.maximum(jnp.abs(denom), 1.0)[:, :, None]
    last = within[:, -1]
    end_log = last[:, None] - within + gate_in
    new_level = jnp.maximum(last + level, jnp.max(end_log, axis=-1))
    keep = jnp.exp(last + level - new_level)
    fresh = jnp.exp(end_log - new_level[:, None])
    scaled_key = (fresh[:, :, None] * key).astype(jnp.bfloat16)
    new_state = keep[:, None, None] * state + jnp.einsum(
        "hse,hsd->hed", value, scaled_key, preferred_element_type=jnp.float32
    )
    new_normal = keep[:, None] * normal + jnp.sum(scaled_key.astype(jnp.float32), axis=1)
    return ((new_state, new_normal, new_level), result)


def depthwise(extended, kernel):
    taps = kernel.shape[0]
    length = extended.shape[0] - taps + 1
    total = extended[0:length] * kernel[0]
    for index in range(1, taps):
        total = total + extended[index : index + length] * kernel[index]
    return total


def merge_states(first, second):
    first_state, first_normal, first_level, first_total = first
    second_state, second_normal, second_level, second_total = second
    shifted = first_level + second_total
    level = jnp.maximum(shifted, second_level)
    older = jnp.exp(shifted - level)
    newer = jnp.exp(second_level - level)
    state = older[:, None, None] * first_state + newer[:, None, None] * second_state
    normal = older[:, None] * first_normal + newer[:, None] * second_normal
    return (state, normal, level, first_total + second_total)


def on_device_by_position(
    tokens,
    conv_value_weight,
    conv_gate_weight,
    conv_kernel,
    conv_norm_gain,
    query_weight,
    key_weight,
    value_weight,
    input_gate_weight,
    forget_gate_weight,
    input_offset,
    forget_offset,
    memory_norm_gain,
    conv_out_weight,
    memory_out_weight,
):
    length = tokens.shape[0]
    heads_here = input_gate_weight.shape[1]
    whole = lax.all_gather(tokens, "tp", axis=1, tiled=True)
    pieces = (
        lax.all_gather(conv_value_weight, "sp", axis=0, tiled=True),
        lax.all_gather(conv_gate_weight, "sp", axis=0, tiled=True),
        lax.all_gather(query_weight, "sp", axis=0, tiled=True),
        lax.all_gather(key_weight, "sp", axis=0, tiled=True),
        lax.all_gather(value_weight, "sp", axis=0, tiled=True),
    )
    folded = tuple((jnp.dot(whole, piece, preferred_element_type=jnp.float32) for piece in pieces))
    conv_value, conv_gate, query_flat, key_flat, value_flat = folded
    gate_pre = jnp.dot(whole, input_gate_weight, preferred_element_type=jnp.float32)
    forget_pre = jnp.dot(whole, forget_gate_weight, preferred_element_type=jnp.float32)
    glu = (conv_value * jax.nn.sigmoid(conv_gate)).astype(jnp.bfloat16)
    taps = conv_kernel.shape[0]
    head_dim = query_flat.shape[1] // heads_here

    def to_heads(flat):
        return flat.astype(jnp.bfloat16).reshape(length, heads_here, head_dim).transpose(1, 0, 2)

    query = to_heads(query_flat)
    key = to_heads(key_flat)
    value = to_heads(value_flat)
    gate_in = (gate_pre + input_offset).T
    forget_log = jax.nn.log_sigmoid(forget_pre + forget_offset).T
    within = jnp.cumsum(forget_log, axis=1)
    total = within[:, -1]
    end_log = total[:, None] - within + gate_in
    local_level = jnp.max(end_log, axis=1)
    fresh = jnp.exp(end_log - local_level[:, None])
    scaled_key = (fresh[:, :, None] * key).astype(jnp.bfloat16)
    local_state = jnp.einsum("hse,hsd->hed", value, scaled_key, preferred_element_type=jnp.float32)
    local_normal = jnp.sum(scaled_key.astype(jnp.float32), axis=1)
    blank_state = (
        jnp.zeros_like(local_state),
        jnp.zeros_like(local_normal),
        jnp.full_like(local_level, LOWEST_LEVEL),
        jnp.zeros_like(total),
    )
    prior = shifted_2(glu[length - (taps - 1) :], "sp", 1)
    incoming = carried_in(
        (local_state, local_normal, local_level, total), "sp", merge_states, blank_state
    )
    extended = jnp.concatenate([prior, glu], axis=0).astype(jnp.float32)
    conv = depthwise(extended, conv_kernel.astype(jnp.float32))
    blocks = length // BLOCK

    def split(array):
        return jnp.moveaxis(array.reshape((heads_here, blocks, BLOCK) + array.shape[2:]), 1, 0)

    _, hidden = lax.scan(
        block_step,
        tuple(incoming[:3]),
        (split(query), split(key), split(value), split(gate_in), split(forget_log)),
    )
    hidden = jnp.moveaxis(hidden, 0, 1).reshape(heads_here, length, head_dim)
    hidden_squares = jnp.sum(hidden * hidden, axis=(0, 2))
    channel_sum, channel_squares, memory_squares = lax.psum(
        (jnp.sum(conv, axis=1), jnp.sum(conv * conv, axis=1), hidden_squares), "tp"
    )
    channels = conv.shape[1] * lax.axis_size("tp")
    mean = (channel_sum / channels)[:, None]
    variance = (channel_squares / channels)[:, None] - mean * mean
    conv_branch = jax.nn.silu((conv - mean) * lax.rsqrt(variance + EPS) * conv_norm_gain).astype(
        jnp.bfloat16
    )
    entries = heads_here * head_dim * lax.axis_size("tp")
    memory_scale = lax.rsqrt(memory_squares / entries + EPS)
    hidden = hidden * memory_scale[None, :, None]
    hidden = hidden * memory_norm_gain.reshape(heads_here, 1, head_dim)
    memory_branch = (
        hidden.transpose(1, 0, 2).reshape(length, heads_here * head_dim).astype(jnp.bfloat16)
    )
    conv_columns, memory_columns = (
        lax.all_gather(conv_out_weight, "sp", axis=1, tiled=True),
        lax.all_gather(memory_out_weight, "sp", axis=1, tiled=True),
    )
    contract = (((0,), (1,)), ((), ()))
    summed = lax.psum_scatter(
        (
            lax.dot_general(conv_columns, conv_branch, contract, preferred_element_type=jnp.float32)
            + lax.dot_general(
                memory_columns, memory_branch, contract, preferred_element_type=jnp.float32
            )
        ).astype(jnp.bfloat16),
        "tp",
        scatter_dimension=0,
        tiled=True,
    ).astype(jnp.float32)
    return summed.T.astype(jnp.bfloat16)


MESH = pl.DeviceIdType.MESH
IN_VMEM = pl.BlockSpec(memory_space=pltpu.VMEM)
SENDS = 224
ROW_TILE = 8
LANES = 128
NT = (((1,), (1,)), ((), ()))


def when(conditions, action):
    if not conditions:
        action()
        return
    every = conditions[0]
    for condition in conditions[1:]:
        every = jnp.logical_and(every, condition)
    pl.when(every)(action)


class Sends:
    def __init__(self, semaphores):
        self.semaphores = semaphores
        self.started = []

    def start(self, source, target, arrival, device, *conditions):
        copy = pltpu.make_async_remote_copy(
            src_ref=source,
            dst_ref=target,
            send_sem=self.semaphores.at[len(self.started)],
            recv_sem=arrival,
            device_id=device,
            device_id_type=MESH,
        )
        self.started.append((copy, conditions))
        when(conditions, copy.start)

    def finish(self):
        for copy, conditions in self.started:
            when(conditions, copy.wait_send)


def arrived(block, semaphore, *conditions):
    copy = pltpu.make_async_remote_copy(
        src_ref=block,
        dst_ref=block,
        send_sem=semaphore,
        recv_sem=semaphore,
        device_id=(lax.axis_index("sp"), lax.axis_index("tp")),
        device_id_type=MESH,
    )
    when(conditions, copy.wait_recv)


def line_order(here, count):
    order = []
    for distance in range(1, count):
        order.append((here - distance, here >= distance, here + 1, here + 1 < count))
        order.append((here + distance, here + distance < count, here - 1, here > 0))
    return order


def pick(index, first, second):
    return jnp.where(jnp.full(first.shape, index, jnp.int32) == 1, second, first)


def stacked(rows, length):
    place = lax.broadcasted_iota(jnp.int32, (ROW_TILE, length), 0)
    result = jnp.zeros((ROW_TILE, length), jnp.float32)
    for index, row in enumerate(rows):
        result = jnp.where(place == index, row, result)
    return result


def as_columns(rows):
    length = rows.shape[1]
    rest = jnp.zeros((LANES - ROW_TILE, length), jnp.float32)
    return jnp.concatenate([rows, rest], axis=0).T


def as_rows(columns):
    length = columns[0].shape[0]
    place = lax.broadcasted_iota(jnp.int32, (length, LANES), 1)
    result = jnp.zeros((length, LANES), jnp.float32)
    for index, column in enumerate(columns):
        result = jnp.where(place == index, column, result)
    return result.T[:ROW_TILE]


def prefix_sums(rows):
    before = lax.broadcasted_iota(jnp.int32, (LANES, LANES), 0)
    after = lax.broadcasted_iota(jnp.int32, (LANES, LANES), 1)
    upper = (before <= after).astype(jnp.float32)
    carry = jnp.zeros((ROW_TILE, 1), jnp.float32)
    parts = []
    for start in range(0, rows.shape[1], LANES):
        part = carry + jnp.dot(
            rows[:, start : start + LANES],
            upper,
            precision=lax.Precision.HIGHEST,
            preferred_element_type=jnp.float32,
        )
        carry = part[:, LANES - 1 :]
        parts.append(part)
    return jnp.concatenate(parts, axis=1)


def layer_kernel(
    count,
    columns,
    tokens,
    wq,
    wk,
    wv,
    wcv,
    wcg,
    own_taps,
    own_conv_gain,
    own_memory_gain,
    own_input_gates,
    own_forget_gates,
    own_input_offsets,
    own_forget_offsets,
    own_memory_out,
    own_conv_out,
    slots,
    lines,
    weights,
    product,
    taps,
    conv_gain,
    memory_gain,
    input_gates,
    forget_gates,
    offsets,
    gate_rows,
    level_before,
    level_here,
    keys,
    values,
    queries,
    weight_near,
    weight_far,
    memory_done,
    squares_done,
    squares_in,
    extended,
    conv,
    sums_done,
    sums_in,
    conv_done,
    memory_in,
    conv_in,
    memory_out,
    conv_out,
    partial,
    send_sem,
    token_sem,
    weight_sem,
    own_sem,
    offset_sem,
    level_sem,
    pair_sem,
    query_sem,
    halo_sem,
    sums_sem,
    squares_sem,
    memory_sem,
    conv_sem,
    out_sem,
    slot_sem,
):
    f32, bf16 = jnp.float32, jnp.bfloat16
    me, tp = lax.axis_index("sp"), lax.axis_index("tp")
    layers = count // 2
    z, x, y, core = me // 2, lax.rem(me, 2), tp // 2, lax.rem(tp, 2)
    side, odd = z // 2, lax.rem(z, 2)
    length, features = tokens.shape
    depth, head_dim = wq.shape[0], wq.shape[1] // 2
    channels = wcv.shape[1] // 2
    rows = 4 * length
    near, far = core == side, core != side
    first, second = x == 0, x == 1
    peer = (me, y * 2 + 1 - core)
    below, above = (me - 2, tp), (me + 2, tp)
    x_side = (z * 2 + 1 - x, tp)
    y_side = (me, (1 - y) * 2 + core)
    has_below, has_above = z > 0, z + 1 < layers
    sends = Sends(send_sem)

    barrier = pltpu.get_barrier_semaphore()
    devices = count * columns
    rank = me * columns + tp
    for step in range(1, devices):
        other = lax.rem(rank + step, devices)
        pl.semaphore_signal(
            barrier,
            inc=1,
            device_id=(other // columns, lax.rem(other, columns)),
            device_id_type=MESH,
        )

    def block(i, j):
        return lines.at[
            pl.ds(pl.multiple_of(i * length, length), length),
            pl.ds(pl.multiple_of(j * features, features), features),
        ]

    place = odd * 2 + x

    @pl.when(near)
    def _():
        lines[
            pl.ds(pl.multiple_of(place * length, length), length),
            pl.ds(pl.multiple_of(tp * features, features), features),
        ] = tokens[...]

    pl.semaphore_wait(barrier, devices - 1)

    goal = y * 2 + side
    mine, mine_sem = block(place, tp), token_sem.at[place, tp]
    sends.start(tokens, mine, mine_sem, (me - 2, goal), has_below)
    sends.start(tokens, mine, mine_sem, (me + 2, goal), has_above)
    sends.start(tokens, mine, mine_sem, (z * 2 + 1 - x, goal))
    sends.start(tokens, mine, mine_sem, (me, (1 - y) * 2 + side))
    sends.start(tokens, mine, mine_sem, peer, far)

    def piece(unit, i):
        return weights.at[
            pl.ds(pl.multiple_of(i * depth, depth), depth),
            unit * head_dim : (unit + 1) * head_dim,
        ]

    def shares(k, x_goal):
        whole = pl.ds(pl.multiple_of(k * head_dim, head_dim), head_dim)
        part = pl.ds(pl.multiple_of(k * channels, channels), channels)
        if x_goal == 0:
            return (
                (wk.at[:, whole], 0, 0, head_dim),
                (wv.at[:, whole], 1, head_dim, head_dim),
            )
        return (
            (wq.at[:, whole], 0, 0, head_dim),
            (wcv.at[:, part], 1, head_dim, channels),
            (wcg.at[:, part], 1, head_dim + channels, channels),
        )

    own_rows = pl.ds(pl.multiple_of(me * depth, depth), depth)
    z_first = (1 - core) * 2

    def send_weights(k, x_goal, to_peer, *conditions):
        for source, unit, start, size in shares(k, x_goal):
            goal = peer if to_peer else ((z_first + k) * 2 + x_goal, y * 2 + unit)
            target = weights.at[own_rows, start : start + size]
            sends.start(source, target, weight_sem.at[unit, me], goal, *conditions)

    for x_goal in range(2):
        home = (far, x == x_goal)
        send_weights(odd, x_goal, True, *home)

        def keep():
            for source, _, start, size in shares(odd, x_goal):
                weights[own_rows, start : start + size] = source[...]

        when(home, keep)

    for index, (source, target) in enumerate(
        (
            (own_taps, taps),
            (own_conv_gain, conv_gain),
            (own_memory_gain, memory_gain),
            (own_input_gates, input_gates),
            (own_forget_gates, forget_gates),
        )
    ):
        sends.start(source, target, own_sem.at[index], peer, far)

        @pl.when(far)
        def _():
            target[...] = source[...]

    for k in range(2):
        goal = ((z_first + k) * 2, y * 2 + side)
        for kind, source in enumerate((own_input_offsets, own_forget_offsets)):
            sends.start(source, offsets.at[place, kind], offset_sem.at[place], goal)

    own_part = x * 2 + core
    half_rows = own_memory_out.shape[0] // 2

    def out_piece(part, number):
        if number == 1:
            return conv_out.at[part], out_sem.at[part, number]
        start = half_rows * (number // 2)
        return memory_out.at[part, start : start + half_rows, :], out_sem.at[part, number]

    def send_out(number, *conditions):
        if number == 1:
            source = own_conv_out
        else:
            start = half_rows * (number // 2)
            source = own_memory_out.at[start : start + half_rows, :]
        target, sem = out_piece(own_part, number)
        for device in (x_side, peer):
            sends.start(source, target, sem, device, *conditions)

    for x_goal in range(2):
        send_weights(1 - odd, x_goal, False, far, x == x_goal)
    send_out(0)
    memory_out[own_part] = own_memory_out[...]
    conv_out[own_part] = own_conv_out[...]

    k_near = jnp.where(near, odd, 1 - core)
    groups = []
    for k in (k_near, 1 - k_near):
        source = core * 2 + k
        groups.append((source, k * 2 + x, k * 2 + 1 - x))
    for source, i, _ in groups:
        away, up = source != z, source < z
        for j in (y * 2, y * 2 + 1):
            spot, sem = block(i, j), token_sem.at[i, j]
            arrived(spot, sem, jnp.logical_or(away, j != tp))
            sends.start(spot, spot, sem, above, away, up, has_above)
            sends.start(spot, spot, sem, below, away, jnp.logical_not(up), has_below)
            sends.start(spot, spot, sem, x_side, away)
            sends.start(spot, spot, sem, y_side, away)
    send_out(1)
    middle = jnp.logical_or(z == 1, z == 2)
    for x_goal in range(2):
        send_weights(side, x_goal, False, near, middle, x == x_goal)
    for _, _, i in groups:
        for j in (y * 2, y * 2 + 1):
            spot, sem = block(i, j), token_sem.at[i, j]
            arrived(spot, sem)
            sends.start(spot, spot, sem, y_side)

    for x_goal in range(2):
        send_weights(side, x_goal, False, near, jnp.logical_not(middle), x == x_goal)
    for x_goal in range(2):
        send_weights(1 - side, x_goal, False, near, x == x_goal)
    for k in (jnp.where(near, side, 1 - odd), jnp.where(near, 1 - side, odd)):
        for x_goal in range(2):
            send_weights(k, x_goal, False, x != x_goal)

    def both_units(i, *conditions):
        part = weights.at[pl.ds(pl.multiple_of(i * depth, depth), depth), :]
        for unit in range(2):
            conditional = (core == unit,) + conditions
            arrived(piece(unit, i), weight_sem.at[unit, i], *conditional)
            sends.start(piece(unit, i), piece(unit, i), weight_sem.at[unit, i], peer, *conditional)

    def other_unit(i, *conditions):
        for unit in range(2):
            arrived(piece(unit, i), weight_sem.at[unit, i], core != unit, *conditions)

    z_mate = side * 2 + 1 - odd
    near_sources = (z_mate * 2 + x, z * 2 + 1 - x, z_mate * 2 + 1 - x)
    for i in near_sources:
        both_units(i)
    for i in range(4):
        for j in ((1 - y) * 2, (1 - y) * 2 + 1):
            arrived(block(i, j), token_sem.at[i, j])
    for i in near_sources:
        other_unit(i)
    for unit in range(2):
        arrived(piece(unit, me), weight_sem.at[unit, me], near)

    def multiply(start, size):
        part = pl.ds(pl.multiple_of(start, size), size)
        return jnp.dot(lines[:, part], weights[part, :], preferred_element_type=f32)

    half = count // 2 * depth
    product[...] = multiply(side * half, half)

    for index, target in enumerate((taps, conv_gain, memory_gain, input_gates, forget_gates)):
        arrived(target, own_sem.at[index], near)
    for i in range(4):
        arrived(offsets.at[i], offset_sem.at[i], first)

    @pl.when(first)
    def _():
        gate_rows[...] = jnp.zeros_like(gate_rows)
        gate_rows[0:2, :] = input_gates[...].astype(f32)
        gate_rows[2:4, :] = forget_gates[...].astype(f32)
        gates = lax.dot_general(
            lines[...], gate_rows[...].astype(bf16), NT, preferred_element_type=f32
        ).T
        shift = [jnp.concatenate([offsets[i, kind] for i in range(4)], 1) for kind in range(2)]
        gate_in = pick(odd, gates[0:1] + shift[0][0:1], gates[1:2] + shift[0][1:2])
        forget = pick(odd, gates[2:3] + shift[1][0:1], gates[3:4] + shift[1][1:2])
        forget_log = jnp.minimum(forget, 0.0) - jnp.log1p(jnp.exp(-jnp.abs(forget)))
        coarse = jnp.round(forget_log * 8.0) * 0.125
        within = prefix_sums(stacked((coarse, forget_log - coarse), rows))
        which = lax.broadcasted_iota(jnp.int32, (ROW_TILE, rows), 0)
        level_here[...] = jnp.where(which == 2, gate_in, within)

    first_core, second_core = core == 0, core == 1
    sends.start(level_here, level_before, level_sem.at[0], peer, first, first_core)
    arrived(level_before, level_sem.at[0], first, second_core)

    @pl.when(jnp.logical_and(first, first_core))
    def _():
        level_before[...] = jnp.zeros_like(level_before)
        keys[:rows, :] = jnp.zeros_like(keys[:rows, :])
        values[:rows, :] = jnp.zeros_like(values[:rows, :])

    span = rows // 2
    scale = head_dim ** (-0.5)
    reach = (rows + span, 2 * rows)
    stores = (weight_near, weight_far)

    @pl.when(first)
    def _():
        before = level_before[...]
        which = lax.broadcasted_iota(jnp.int32, (ROW_TILE, rows), 0)
        here = level_here[...] + jnp.where(which < 2, before[:, rows - 1 :], 0.0)
        from_rows = jnp.concatenate([before, here], axis=1)
        to_columns = as_columns(here)
        tile = 64
        for start in range(0, rows, tile):
            index = start // span
            width = reach[index]
            to = to_columns[start : start + tile]
            log_weight = (
                (to[:, 0:1] - from_rows[0:1, :width])
                + (to[:, 1:2] - from_rows[1:2, :width])
                + from_rows[2:3, :width]
            )
            at = lax.broadcasted_iota(jnp.int32, (tile, width), 1)
            until = lax.broadcasted_iota(jnp.int32, (tile, width), 0) + (start + rows)
            seen = jnp.logical_and(at <= until, at >= rows * (1 - core))
            log_weight = jnp.where(seen, log_weight, -jnp.inf)
            weight = jnp.exp(log_weight - jnp.max(log_weight, axis=1, keepdims=True)) * scale
            stores[index][start - index * span : start - index * span + tile, :] = weight

    send_out(2, first)

    far_pairs = (
        jnp.where(side == 0, 2, 1),
        jnp.where(side == 0, 3, 0),
    )
    for pair in far_pairs:
        both_units(pair * 2 + x)
        both_units(pair * 2 + 1 - x)
    for pair in far_pairs:
        other_unit(pair * 2)
        other_unit(pair * 2 + 1)
        product[...] += multiply(pair * 2 * depth, 2 * depth)

    @pl.when(second)
    def _():
        queries[...] = product[:, :head_dim].astype(bf16)

    for index in range(2):
        part = queries.at[index * span : (index + 1) * span, :]
        sends.start(part, part, query_sem.at[index], x_side, second)
    send_out(2, second)

    @pl.when(first)
    def _():
        keys[rows:, :] = product[:, :head_dim].astype(bf16)
        values[rows:, :] = product[:, head_dim:].astype(bf16)

    for index, array in enumerate((keys, values)):
        target = array.at[:rows, :]
        sends.start(array.at[rows:, :], target, pair_sem.at[index], peer, first, first_core)

    halo = extended.shape[0] - rows

    @pl.when(second)
    def _():
        gated = product[:, head_dim : head_dim + channels] * jax.nn.sigmoid(
            product[:, head_dim + channels :]
        )
        extended[halo:, :] = gated.astype(bf16).astype(f32)

    sends.start(
        extended.at[rows:, :], extended.at[:halo, :], halo_sem.at[0], peer, second, first_core
    )

    @pl.when(jnp.logical_and(second, first_core))
    def _():
        extended[:halo, :] = jnp.zeros((halo, channels), f32)

    arrived(extended.at[:halo, :], halo_sem.at[0], second, second_core)
    source_index = y * layers + z

    @pl.when(second)
    def _():
        number = taps.shape[0]
        kernel = taps[...].astype(f32)
        kernel = pick(odd, kernel[:, :channels], kernel[:, channels:])
        for start in range(0, rows, length):
            base = start + halo - (number - 1)
            total = extended[base : base + length, :] * kernel[0:1]
            for index in range(1, number):
                total = total + (
                    extended[base + index : base + index + length, :] * kernel[index : index + 1]
                )
            conv[start : start + length, :] = total
        all_rows = conv[...]
        sums_done[...] = as_rows(
            (
                jnp.sum(all_rows, axis=1, keepdims=True),
                jnp.sum(all_rows * all_rows, axis=1, keepdims=True),
            )
        )
        sums_in[source_index] = sums_done[...]

    sources = [(z_other, y_other) for z_other in range(layers) for y_other in range(2)]
    for z_other, y_other in sources:
        away = jnp.logical_or(z != z_other, y != y_other)
        sends.start(
            sums_done,
            sums_in.at[source_index],
            sums_sem.at[source_index],
            (z_other * 2 + 1, y_other * 2 + core),
            second,
            away,
        )
    for z_other, y_other in sources:
        away = jnp.logical_or(z != z_other, y != y_other)
        index = y_other * layers + z_other
        arrived(sums_in.at[index], sums_sem.at[index], second, away)

    @pl.when(second)
    def _():
        total = sums_in[0]
        for index in range(1, 2 * layers):
            total = total + sums_in[index]
        total = total * (1.0 / (2 * layers * channels))
        mean = total[0:1]
        inverse = lax.rsqrt(total[1:2] - mean * mean + EPS)
        across = as_columns(stacked((mean, inverse), rows))
        gain = conv_gain[...]
        gain = pick(odd, gain[:, :channels], gain[:, channels:])
        normed = (conv[...] - across[:, 0:1]) * across[:, 1:2] * gain
        conv_done[...] = (normed * jax.nn.sigmoid(normed)).astype(bf16)

    def spread(done, inside, semaphores, home, index):
        here, away = x == home, x != home
        kept = done.at[(2 * index + home) * length : (2 * index + home + 1) * length, :]
        given = done.at[(2 * index + 1 - home) * length : (2 * index + 2 - home) * length, :]
        part = slice(index * length, (index + 1) * length)
        target, sem = inside.at[z, part, :], semaphores.at[z, index]
        sends.start(kept, target, sem, below, here, has_below)
        sends.start(kept, target, sem, above, here, has_above)
        sends.start(given, target, sem, x_side, here)

        @pl.when(here)
        def _():
            inside[z, part, :] = kept[...]

    for index in range(2):
        spread(conv_done, conv_in, conv_sem, 1, index)

    for index, array in enumerate((keys, values)):
        arrived(array.at[:rows, :], pair_sem.at[index], first, second_core)
    squares_index = source_index
    for index in range(2):
        arrived(
            queries.at[index * span : (index + 1) * span, :], query_sem.at[index], first
        )

        @pl.when(first)
        def _():
            width = reach[index]
            gain = memory_gain[...]
            gain = pick(odd, gain[:, :head_dim], gain[:, head_dim:])
            squares = []
            for inner in range(2):
                start = index * span + inner * length
                scores = lax.dot_general(
                    queries[start : start + length, :],
                    keys[:width, :],
                    NT,
                    preferred_element_type=f32,
                )
                scores = scores * stores[index][inner * length : (inner + 1) * length, :]
                numer = jnp.dot(
                    scores.astype(bf16), values[:width, :], preferred_element_type=f32
                )
                denom = jnp.sum(scores, axis=1, keepdims=True)
                cell = numer / jnp.maximum(jnp.abs(denom), 1.0)
                memory_done[start : start + length, :] = (cell * gain).astype(bf16)
                squares.append(jnp.sum(cell * cell, axis=1, keepdims=True))
            squares_done[index] = as_rows((jnp.concatenate(squares, axis=0),))
            squares_in[squares_index, index] = squares_done[index]

        spread(memory_done, memory_in, memory_sem, 0, index)
        for z_other, y_other in sources:
            for x_other in range(2):
                away = jnp.logical_or(
                    jnp.logical_or(z != z_other, y != y_other), x != x_other
                )
                sends.start(
                    squares_done.at[index],
                    squares_in.at[squares_index, index],
                    squares_sem.at[squares_index, index],
                    (z_other * 2 + x_other, y_other * 2 + core),
                    first,
                    away,
                )

    order = line_order(z, layers)

    kinds = [(conv_in, conv_sem, 1, index) for index in range(2)]
    kinds += [(memory_in, memory_sem, 0, index) for index in range(2)]
    for inside, semaphores, home, index in kinds:
        part = slice(index * length, (index + 1) * length)
        away = x != home
        spot, sem = inside.at[z, part, :], semaphores.at[z, index]
        arrived(spot, sem, away)
        sends.start(spot, spot, sem, below, away, has_below)
        sends.start(spot, spot, sem, above, away, has_above)
    across = (1 - x) * 2 + core
    for distance in range(1, layers):
        for inside, semaphores, _, index in kinds:
            part = slice(index * length, (index + 1) * length)
            for source, there, onward, further in order[2 * distance - 2 : 2 * distance]:
                spot, sem = inside.at[source, part, :], semaphores.at[source, index]
                arrived(spot, sem, there)
                sends.start(spot, spot, sem, (onward * 2 + x, tp), there, further)
        if distance == 1:
            for number in range(3):
                spot, sem = out_piece(across, number)
                arrived(spot, sem)
                sends.start(spot, spot, sem, peer)
    entries = layers * 2 * head_dim
    for index in range(2):
        part = slice(index * length, (index + 1) * length)
        for z_other, y_other in sources:
            own = jnp.logical_and(first, jnp.logical_and(z == z_other, y == y_other))
            slot = y_other * layers + z_other
            arrived(
                squares_in.at[slot, index], squares_sem.at[slot, index], jnp.logical_not(own)
            )
        if index == 0:
            for group in range(2):
                part_out = group * 2 + 1 - core
                for number in range(3):
                    arrived(*out_piece(part_out, number))
        total = squares_in[0, index]
        for slot in range(1, 2 * layers):
            total = total + squares_in[slot, index]
        total = pick(x, total[:, :length], total[:, length:])
        row_scale = as_columns(lax.rsqrt(total * (1.0 / entries) + EPS))[:, 0:1]
        for group in range(2):
            from_memory, from_conv = None, None
            for head in range(layers):
                where = group * 2 + 1 - head // 2
                inner = head % 2
                memory_term = jnp.dot(
                    memory_in[head, part, :],
                    memory_out[where, inner * head_dim : (inner + 1) * head_dim, :],
                    preferred_element_type=f32,
                )
                conv_term = jnp.dot(
                    conv_in[head, part, :],
                    conv_out[where, inner * channels : (inner + 1) * channels, :],
                    preferred_element_type=f32,
                )
                from_memory = memory_term if head == 0 else from_memory + memory_term
                from_conv = conv_term if head == 0 else from_conv + conv_term
            width = from_memory.shape[1]
            partial[index, :, group * width : (group + 1) * width] = (
                from_conv + row_scale * from_memory
            ).astype(bf16)
        goal = ((core * 2 + index) * 2 + x, z)
        away = jnp.logical_or(core * 2 + index != z, tp != z)
        sends.start(partial.at[index], slots.at[y], slot_sem.at[y], goal, away)

        @pl.when(jnp.logical_not(away))
        def _():
            slots[y] = partial[index]

    for y_other in range(2):
        own = jnp.logical_and(tp == z, jnp.logical_and(y == y_other, core == side))
        arrived(slots.at[y_other], slot_sem.at[y_other], jnp.logical_not(own))
    sends.finish()


def layer(arrays):
    count, columns = lax.axis_size("sp"), lax.axis_size("tp")
    (
        tokens,
        conv_value_weight,
        conv_gate_weight,
        conv_kernel,
        conv_norm_gain,
        query_weight,
        key_weight,
        value_weight,
        input_gate_weight,
        forget_gate_weight,
        input_offset,
        forget_offset,
        memory_norm_gain,
        conv_out_weight,
        memory_out_weight,
    ) = arrays
    length, features = tokens.shape
    depth, head_dim = query_weight.shape[0], query_weight.shape[1] // 2
    channels = conv_value_weight.shape[1] // 2
    wide = features * columns
    rows = length * count // 2
    layers = count // 2
    taps = conv_kernel.shape[0]
    halo = -(-(taps - 1) // ROW_TILE) * ROW_TILE
    width = memory_out_weight.shape[1]
    f32, bf16 = jnp.float32, jnp.bfloat16
    DMA = pltpu.SemaphoreType.DMA
    V = pltpu.VMEM
    return pl.pallas_call(
        lambda *refs: layer_kernel(count, columns, *refs),
        out_shape=jax.ShapeDtypeStruct((2, length, features), bf16),
        in_specs=[IN_VMEM] * 15,
        out_specs=IN_VMEM,
        scratch_shapes=[
            V((rows, wide), bf16),
            V((wide, 2 * head_dim), bf16),
            V((rows, 2 * head_dim), f32),
            V(conv_kernel.shape, bf16),
            V((1, 2 * channels), f32),
            V((1, 2 * head_dim), f32),
            V((2, wide), bf16),
            V((2, wide), bf16),
            V((4, 2, 2, length), f32),
            V((LANES, wide), f32),
            V((ROW_TILE, rows), f32),
            V((ROW_TILE, rows), f32),
            V((2 * rows, head_dim), bf16),
            V((2 * rows, head_dim), bf16),
            V((rows, head_dim), bf16),
            V((rows // 2, rows + rows // 2), f32),
            V((rows // 2, 2 * rows), f32),
            V((rows, head_dim), bf16),
            V((2, ROW_TILE, rows // 2), f32),
            V((count, 2, ROW_TILE, rows // 2), f32),
            V((halo + rows, channels), f32),
            V((rows, channels), f32),
            V((ROW_TILE, rows), f32),
            V((count, ROW_TILE, rows), f32),
            V((rows, channels), bf16),
            V((layers, rows // 2, head_dim), bf16),
            V((layers, rows // 2, channels), bf16),
            V((4, 2 * head_dim, width), bf16),
            V((4, 2 * channels, width), bf16),
            V((2, length, features), bf16),
            DMA((SENDS,)),
            DMA((4, columns)),
            DMA((2, count)),
            DMA((5,)),
            DMA((4,)),
            DMA((1,)),
            DMA((2,)),
            DMA((2,)),
            DMA((1,)),
            DMA((count,)),
            DMA((count, 2)),
            DMA((layers, 2)),
            DMA((layers, 2)),
            DMA((4, 3)),
            DMA((2,)),
        ],
        compiler_params=pltpu.CompilerParams(collective_id=0, has_side_effects=True),
    )(
        tokens,
        query_weight,
        key_weight,
        value_weight,
        conv_value_weight,
        conv_gate_weight,
        conv_kernel,
        conv_norm_gain.reshape(1, -1),
        memory_norm_gain.reshape(1, -1),
        input_gate_weight.T,
        forget_gate_weight.T,
        input_offset.T,
        forget_offset.T,
        memory_out_weight,
        conv_out_weight,
    )


def on_device_by_column(*arrays):
    slots = layer(arrays)
    return jnp.sum(slots.astype(jnp.float32), axis=0).astype(jnp.bfloat16)


def splits_by_column(mesh, tokens, query_weight, conv_value_weight, conv_kernel, input_gate_weight):
    count, columns = mesh.shape["sp"], mesh.shape["tp"]
    heads = input_gate_weight.shape[1]
    head_dim = query_weight.shape[1] // heads
    length = tokens.shape[0] // count
    return (
        count == 8
        and columns == 4
        and heads == count
        and length % LANES == 0
        and tokens.size * 2 <= 4 * 2**20
        and conv_value_weight.shape[1] * 2 == head_dim * heads
        and head_dim == 256
        and conv_kernel.shape[0] - 1 <= length
    )


def solution(mesh):
    in_specs = (
        P("sp", "tp"),
        P("sp", "tp"),
        P("sp", "tp"),
        P(None, "tp"),
        P("tp"),
        P("sp", "tp"),
        P("sp", "tp"),
        P("sp", "tp"),
        P(None, "tp"),
        P(None, "tp"),
        P("sp", "tp"),
        P("sp", "tp"),
        P("tp"),
        P("tp", "sp"),
        P("tp", "sp"),
    )
    out_specs = P("sp", "tp")

    def run(*arrays):
        by_column = splits_by_column(
            mesh, arrays[0], arrays[5], arrays[1], arrays[3], arrays[8]
        )
        on_device = on_device_by_column if by_column else on_device_by_position
        return jax.shard_map(
            on_device, mesh=mesh, in_specs=in_specs, out_specs=out_specs, check_vma=False
        )(*arrays)

    return run
```

```python
import jax
import jax.numpy as jnp
from jax import lax
from jax.experimental import pallas as pl
from jax.experimental.pallas import tpu as pltpu
from jax.sharding import PartitionSpec as P

BLOCK = 64


EPS = 1e-06
LOWEST_LEVEL = -1e30


def shifted_2(value, axis, steps):
    count = lax.axis_size(axis)
    leading, last = (max(0, -steps), min(count, count - steps))
    return lax.ppermute(value, axis, [(source, source + steps) for source in range(leading, last)])


def carried_in(shard, axis, join, neutral):
    place = lax.axis_index(axis)
    gathered = jax.tree.map(
        lambda a, kind: lax.all_gather(a.astype(kind), axis),
        shard,
        (jnp.bfloat16, jnp.bfloat16, jnp.bfloat16, jnp.bfloat16),
    )
    state = jax.tree.map(lambda a, e: jnp.zeros_like(a) + jnp.asarray(e, a.dtype), shard, neutral)

    def one(step, state):
        return join(
            state,
            jax.tree.map(
                lambda a, own: lax.dynamic_index_in_dim(a, step, 0, False).astype(own.dtype),
                gathered,
                shard,
            ),
        )

    return lax.fori_loop(0, place, one, state)


def block_step(carry, inputs):
    state, normal, level = carry
    query, key, value, gate_in, forget_log = inputs
    length = gate_in.shape[-1]
    scale = query.shape[-1] ** (-0.5)
    causal = jnp.tril(jnp.ones((length, length), dtype=bool))
    within = jnp.cumsum(forget_log, axis=-1)
    log_weight = within[:, :, None] - within[:, None, :] + gate_in[:, None, :]
    log_weight = jnp.where(causal, log_weight, -jnp.inf)
    carried = within + level[:, None]
    top = jnp.maximum(carried, jnp.max(log_weight, axis=-1))
    weight = jnp.exp(log_weight - top[:, :, None])
    carried_weight = jnp.exp(carried - top) * scale
    scores = jnp.einsum("htd,hsd->hts", query, key, preferred_element_type=jnp.float32) * (
        scale * weight
    )
    numer = jnp.einsum(
        "hts,hse->hte", scores.astype(jnp.bfloat16), value, preferred_element_type=jnp.float32
    )
    numer = numer + carried_weight[:, :, None] * jnp.einsum(
        "hed,htd->hte", state.astype(jnp.bfloat16), query, preferred_element_type=jnp.float32
    )
    denom = jnp.sum(scores, axis=-1) + carried_weight * jnp.einsum(
        "hd,htd->ht", normal.astype(jnp.bfloat16), query, preferred_element_type=jnp.float32
    )
    result = numer / jnp.maximum(jnp.abs(denom), 1.0)[:, :, None]
    last = within[:, -1]
    end_log = last[:, None] - within + gate_in
    new_level = jnp.maximum(last + level, jnp.max(end_log, axis=-1))
    keep = jnp.exp(last + level - new_level)
    fresh = jnp.exp(end_log - new_level[:, None])
    scaled_key = (fresh[:, :, None] * key).astype(jnp.bfloat16)
    new_state = keep[:, None, None] * state + jnp.einsum(
        "hse,hsd->hed", value, scaled_key, preferred_element_type=jnp.float32
    )
    new_normal = keep[:, None] * normal + jnp.sum(scaled_key.astype(jnp.float32), axis=1)
    return ((new_state, new_normal, new_level), result)


def depthwise(extended, kernel):
    taps = kernel.shape[0]
    length = extended.shape[0] - taps + 1
    total = extended[0:length] * kernel[0]
    for index in range(1, taps):
        total = total + extended[index : index + length] * kernel[index]
    return total


def merge_states(first, second):
    first_state, first_normal, first_level, first_total = first
    second_state, second_normal, second_level, second_total = second
    shifted = first_level + second_total
    level = jnp.maximum(shifted, second_level)
    older = jnp.exp(shifted - level)
    newer = jnp.exp(second_level - level)
    state = older[:, None, None] * first_state + newer[:, None, None] * second_state
    normal = older[:, None] * first_normal + newer[:, None] * second_normal
    return (state, normal, level, first_total + second_total)


def on_device_by_position(
    tokens,
    conv_value_weight,
    conv_gate_weight,
    conv_kernel,
    conv_norm_gain,
    query_weight,
    key_weight,
    value_weight,
    input_gate_weight,
    forget_gate_weight,
    input_offset,
    forget_offset,
    memory_norm_gain,
    conv_out_weight,
    memory_out_weight,
):
    length = tokens.shape[0]
    heads_here = input_gate_weight.shape[1]
    whole = lax.all_gather(tokens, "tp", axis=1, tiled=True)
    pieces = (
        lax.all_gather(conv_value_weight, "sp", axis=0, tiled=True),
        lax.all_gather(conv_gate_weight, "sp", axis=0, tiled=True),
        lax.all_gather(query_weight, "sp", axis=0, tiled=True),
        lax.all_gather(key_weight, "sp", axis=0, tiled=True),
        lax.all_gather(value_weight, "sp", axis=0, tiled=True),
    )
    folded = tuple((jnp.dot(whole, piece, preferred_element_type=jnp.float32) for piece in pieces))
    conv_value, conv_gate, query_flat, key_flat, value_flat = folded
    gate_pre = jnp.dot(whole, input_gate_weight, preferred_element_type=jnp.float32)
    forget_pre = jnp.dot(whole, forget_gate_weight, preferred_element_type=jnp.float32)
    glu = (conv_value * jax.nn.sigmoid(conv_gate)).astype(jnp.bfloat16)
    taps = conv_kernel.shape[0]
    head_dim = query_flat.shape[1] // heads_here

    def to_heads(flat):
        return flat.astype(jnp.bfloat16).reshape(length, heads_here, head_dim).transpose(1, 0, 2)

    query = to_heads(query_flat)
    key = to_heads(key_flat)
    value = to_heads(value_flat)
    gate_in = (gate_pre + input_offset).T
    forget_log = jax.nn.log_sigmoid(forget_pre + forget_offset).T
    within = jnp.cumsum(forget_log, axis=1)
    total = within[:, -1]
    end_log = total[:, None] - within + gate_in
    local_level = jnp.max(end_log, axis=1)
    fresh = jnp.exp(end_log - local_level[:, None])
    scaled_key = (fresh[:, :, None] * key).astype(jnp.bfloat16)
    local_state = jnp.einsum("hse,hsd->hed", value, scaled_key, preferred_element_type=jnp.float32)
    local_normal = jnp.sum(scaled_key.astype(jnp.float32), axis=1)
    blank_state = (
        jnp.zeros_like(local_state),
        jnp.zeros_like(local_normal),
        jnp.full_like(local_level, LOWEST_LEVEL),
        jnp.zeros_like(total),
    )
    prior = shifted_2(glu[length - (taps - 1) :], "sp", 1)
    incoming = carried_in(
        (local_state, local_normal, local_level, total), "sp", merge_states, blank_state
    )
    extended = jnp.concatenate([prior, glu], axis=0).astype(jnp.float32)
    conv = depthwise(extended, conv_kernel.astype(jnp.float32))
    blocks = length // BLOCK

    def split(array):
        return jnp.moveaxis(array.reshape((heads_here, blocks, BLOCK) + array.shape[2:]), 1, 0)

    _, hidden = lax.scan(
        block_step,
        tuple(incoming[:3]),
        (split(query), split(key), split(value), split(gate_in), split(forget_log)),
    )
    hidden = jnp.moveaxis(hidden, 0, 1).reshape(heads_here, length, head_dim)
    hidden_squares = jnp.sum(hidden * hidden, axis=(0, 2))
    channel_sum, channel_squares, memory_squares = lax.psum(
        (jnp.sum(conv, axis=1), jnp.sum(conv * conv, axis=1), hidden_squares), "tp"
    )
    channels = conv.shape[1] * lax.axis_size("tp")
    mean = (channel_sum / channels)[:, None]
    variance = (channel_squares / channels)[:, None] - mean * mean
    conv_branch = jax.nn.silu((conv - mean) * lax.rsqrt(variance + EPS) * conv_norm_gain).astype(
        jnp.bfloat16
    )
    entries = heads_here * head_dim * lax.axis_size("tp")
    memory_scale = lax.rsqrt(memory_squares / entries + EPS)
    hidden = hidden * memory_scale[None, :, None]
    hidden = hidden * memory_norm_gain.reshape(heads_here, 1, head_dim)
    memory_branch = (
        hidden.transpose(1, 0, 2).reshape(length, heads_here * head_dim).astype(jnp.bfloat16)
    )
    conv_columns, memory_columns = (
        lax.all_gather(conv_out_weight, "sp", axis=1, tiled=True),
        lax.all_gather(memory_out_weight, "sp", axis=1, tiled=True),
    )
    contract = (((0,), (1,)), ((), ()))
    summed = lax.psum_scatter(
        (
            lax.dot_general(conv_columns, conv_branch, contract, preferred_element_type=jnp.float32)
            + lax.dot_general(
                memory_columns, memory_branch, contract, preferred_element_type=jnp.float32
            )
        ).astype(jnp.bfloat16),
        "tp",
        scatter_dimension=0,
        tiled=True,
    ).astype(jnp.float32)
    return summed.T.astype(jnp.bfloat16)


MESH = pl.DeviceIdType.MESH
IN_VMEM = pl.BlockSpec(memory_space=pltpu.VMEM)
SENDS = 30
ROW_TILE = 8
LANES = 128
NT = (((1,), (1,)), ((), ()))


def when(conditions, action):
    if not conditions:
        action()
        return
    every = conditions[0]
    for condition in conditions[1:]:
        every = jnp.logical_and(every, condition)
    pl.when(every)(action)


class Sends:
    def __init__(self, semaphores):
        self.semaphores = semaphores
        self.waits = []
        self.used = 0

    def shared(self, *waits):
        semaphore = self.semaphores.at[self.used]
        self.used += 1
        for whole, *conditions in waits:
            self.waits.append((whole, semaphore, conditions))
        return semaphore

    def start(self, source, target, arrival, device, *conditions, leaving=None):
        if leaving is None:
            leaving = self.shared((source, *conditions))
        copy = pltpu.make_async_remote_copy(
            src_ref=source,
            dst_ref=target,
            send_sem=leaving,
            recv_sem=arrival,
            device_id=device,
            device_id_type=MESH,
        )
        when(conditions, copy.start)

    def finish(self):
        for whole, semaphore, conditions in self.waits:
            when(conditions, waiting(whole, semaphore).wait_send)


def waiting(block, semaphore):
    return pltpu.make_async_remote_copy(
        src_ref=block,
        dst_ref=block,
        send_sem=semaphore,
        recv_sem=semaphore,
        device_id=(lax.axis_index("sp"), lax.axis_index("tp")),
        device_id_type=MESH,
    )


def arrived(block, semaphore, *conditions):
    copy = waiting(block, semaphore)
    when(conditions, copy.wait_recv)


def line_order(here, count):
    order = []
    for distance in range(1, count):
        order.append((here - distance, here >= distance, here + 1, here + 1 < count))
        order.append((here + distance, here + distance < count, here - 1, here > 0))
    return order


def pick(index, first, second):
    return jnp.where(jnp.full(first.shape, index, jnp.int32) == 1, second, first)


def stacked(rows, length):
    place = lax.broadcasted_iota(jnp.int32, (ROW_TILE, length), 0)
    result = jnp.zeros((ROW_TILE, length), jnp.float32)
    for index, row in enumerate(rows):
        result = jnp.where(place == index, row, result)
    return result


def as_columns(rows):
    length = rows.shape[1]
    rest = jnp.zeros((LANES - ROW_TILE, length), jnp.float32)
    return jnp.concatenate([rows, rest], axis=0).T


def as_rows(columns):
    length = columns[0].shape[0]
    place = lax.broadcasted_iota(jnp.int32, (length, LANES), 1)
    result = jnp.zeros((length, LANES), jnp.float32)
    for index, column in enumerate(columns):
        result = jnp.where(place == index, column, result)
    return result.T[:ROW_TILE]


def prefix_sums(rows):
    before = lax.broadcasted_iota(jnp.int32, (LANES, LANES), 0)
    after = lax.broadcasted_iota(jnp.int32, (LANES, LANES), 1)
    upper = (before <= after).astype(jnp.float32)
    carry = jnp.zeros((ROW_TILE, 1), jnp.float32)
    parts = []
    for start in range(0, rows.shape[1], LANES):
        part = carry + jnp.dot(
            rows[:, start : start + LANES],
            upper,
            precision=lax.Precision.HIGHEST,
            preferred_element_type=jnp.float32,
        )
        carry = part[:, LANES - 1 :]
        parts.append(part)
    return jnp.concatenate(parts, axis=1)


def layer_kernel(
    count,
    columns,
    all_tokens,
    all_wq,
    all_wk,
    all_wv,
    all_wcv,
    all_wcg,
    own_taps,
    own_conv_gain,
    own_memory_gain,
    own_input_gates,
    own_forget_gates,
    own_input_offsets,
    own_forget_offsets,
    own_memory_out,
    own_conv_out,
    slots,
    tokens,
    wq,
    wk,
    wv,
    wcv,
    wcg,
    shifts,
    lines,
    weights,
    product,
    taps,
    conv_gain,
    memory_gain,
    gate_weights,
    offsets,
    gate_rows,
    level_before,
    level_here,
    keys,
    values,
    queries,
    weight_near,
    weight_far,
    memory_done,
    squares_done,
    squares_in,
    extended,
    conv,
    sums_done,
    sums_in,
    conv_done,
    memory_in,
    conv_in,
    memory_out,
    conv_out,
    partial,
    load_sem,
    send_sem,
    token_sem,
    y_sem,
    weight_sem,
    own_sem,
    offset_sem,
    level_sem,
    pair_sem,
    query_sem,
    halo_sem,
    sums_sem,
    squares_sem,
    memory_sem,
    conv_sem,
    out_sem,
    slot_sem,
):
    f32, bf16 = jnp.float32, jnp.bfloat16
    me, tp = lax.axis_index("sp"), lax.axis_index("tp")
    layers = count // 2
    z, x, y, core = me // 2, lax.rem(me, 2), tp // 2, lax.rem(tp, 2)
    side, odd = z // 2, lax.rem(z, 2)
    length, features = tokens.shape
    depth, head_dim = wq.shape[0], wq.shape[1] // 2
    channels = wcv.shape[1] // 2
    rows = 4 * length
    span = rows // 2
    near, far = core == side, core != side
    first, second = x == 0, x == 1
    middle = jnp.logical_or(z == 1, z == 2)
    ends = jnp.logical_not(middle)
    peer = (me, y * 2 + 1 - core)
    below, above = (me - 2, tp), (me + 2, tp)
    x_side = (z * 2 + 1 - x, tp)
    y_side = (me, (1 - y) * 2 + core)
    has_below, has_above = z > 0, z + 1 < layers
    sends = Sends(send_sem)

    barrier = pltpu.get_barrier_semaphore()
    devices = count * columns
    rank = me * columns + tp
    for step in range(1, devices):
        other = lax.rem(rank + step, devices)
        pl.semaphore_signal(
            barrier,
            inc=1,
            device_id=(other // columns, lax.rem(other, columns)),
            device_id_type=MESH,
        )

    def block(i, j):
        return lines.at[
            pl.ds(pl.multiple_of(i * length, length), length),
            pl.ds(pl.multiple_of(j * features, features), features),
        ]

    def blocks(number):
        return lines.at[: number * length // columns, :]

    place = odd * 2 + x
    own_part = x * 2 + core
    loads = []
    for source, target, *conditions in (
        (all_tokens, tokens),
        (all_tokens, block(place, tp), near),
        (all_wq, wq),
        (all_wk, wk),
        (all_wv, wv),
        (all_wcv, wcv),
        (all_wcg, wcg),
        (own_input_offsets, shifts.at[0]),
        (own_forget_offsets, shifts.at[1]),
        (own_taps, taps, far),
        (own_conv_gain, conv_gain, far),
        (own_memory_gain, memory_gain, far),
        (own_input_gates, gate_weights.at[0], far),
        (own_forget_gates, gate_weights.at[1], far),
        (own_memory_out, memory_out.at[own_part]),
        (own_conv_out, conv_out.at[own_part]),
    ):
        copy = pltpu.make_async_copy(source, target, load_sem.at[len(loads)])
        loads.append((copy, conditions))
        when(conditions, copy.start)

    def loaded(first_load, last_load):
        for copy, conditions in loads[first_load:last_load]:
            when(conditions, copy.wait)

    loaded(0, 2)
    pl.semaphore_wait(barrier, devices - 1)

    goal = y * 2 + side
    mine, mine_sem = block(place, tp), token_sem.at[place, core]
    z_leaving = sends.shared(
        (blocks(1), ends), (blocks(4), middle, near), (blocks(6), middle, far)
    )
    x_leaving = sends.shared((blocks(3), near), (blocks(5), far))
    y_leaving = sends.shared((blocks(7), near), (blocks(9), far))
    sends.start(tokens, mine, mine_sem, (me - 2, goal), has_below, leaving=z_leaving)
    sends.start(tokens, mine, mine_sem, (me + 2, goal), has_above, leaving=z_leaving)
    sends.start(tokens, mine, mine_sem, (z * 2 + 1 - x, goal), leaving=x_leaving)
    sends.start(tokens, mine, y_sem.at[0], (me, (1 - y) * 2 + side), leaving=y_leaving)
    sends.start(tokens, mine, mine_sem, peer, far)

    def piece(unit, i):
        return weights.at[
            pl.ds(pl.multiple_of(i * depth, depth), depth),
            unit * head_dim : (unit + 1) * head_dim,
        ]

    def shares(k, x_goal):
        whole = pl.ds(pl.multiple_of(k * head_dim, head_dim), head_dim)
        part = pl.ds(pl.multiple_of(k * channels, channels), channels)
        if x_goal == 0:
            return (
                (wk.at[:, whole], 0, 0, head_dim),
                (wv.at[:, whole], 1, head_dim, head_dim),
            )
        return (
            (wq.at[:, whole], 0, 0, head_dim),
            (wcv.at[:, part], 1, head_dim, channels),
            (wcg.at[:, part], 1, head_dim + channels, channels),
        )

    own_rows = pl.ds(pl.multiple_of(me * depth, depth), depth)
    z_first = (1 - core) * 2
    share = weights.at[:depth, :]

    def send_weights(k, cross, leaving, *conditions, to_peer=False):
        for x_goal in range(2):
            chosen = conditions + ((x != x_goal) if cross else (x == x_goal),)
            for source, unit, start, size in shares(k, x_goal):
                device = peer if to_peer else ((z_first + k) * 2 + x_goal, y * 2 + unit)
                target = weights.at[own_rows, start : start + size]
                sends.start(
                    source, target, weight_sem.at[unit, me], device, *chosen, leaving=leaving
                )

    loaded(2, len(loads))
    mate_leaving, other_leaving = sends.shared((share,)), sends.shared((share,))
    send_weights(odd, False, other_leaving, far, to_peer=True)
    send_weights(1 - odd, False, mate_leaving, far)
    for x_goal in range(2):

        def keep():
            for source, _, start, size in shares(odd, x_goal):
                weights[own_rows, start : start + size] = source[...]

        when((far, x == x_goal), keep)

    own_arrays = (taps, conv_gain, memory_gain, gate_weights)
    for index, array in enumerate(own_arrays):
        sends.start(array, array, own_sem.at[index], peer, far)
    leaving = sends.shared((offsets.at[:2],))
    for k in range(2):
        device = ((z_first + k) * 2, y * 2 + side)
        sends.start(shifts, offsets.at[place], offset_sem.at[0], device, leaving=leaving)

    half_rows = memory_out.shape[1] // 2
    out_width = memory_out.shape[2]
    three_pieces = weights.at[: 3 * half_rows * out_width // (2 * head_dim), :]

    def out_piece(part, number):
        if number == 1:
            return conv_out.at[part]
        start = half_rows * (number // 2)
        return memory_out.at[part, start : start + half_rows, :]

    out_leaving = [sends.shared((three_pieces,)) for _ in range(2)]

    def send_out(number, *conditions):
        spot = out_piece(own_part, number)
        for device, leaving in zip((x_side, peer), out_leaving):
            sends.start(spot, spot, out_sem.at[own_part], device, *conditions, leaving=leaving)

    k_near = jnp.where(near, odd, 1 - core)
    groups = []
    for k in (k_near, 1 - k_near):
        source = core * 2 + k
        groups.append((source, k * 2 + x, k * 2 + 1 - x))
    for source, i, _ in groups:
        away, up = source != z, source < z
        onward = (jnp.where(up, z + 1, z - 1) * 2 + x, tp)
        for j in range(2):
            spot, sem = block(i, y * 2 + j), token_sem.at[i, j]
            arrived(spot, sem, jnp.logical_or(away, j != core))
            sends.start(spot, spot, sem, onward, away, middle, leaving=z_leaving)
            sends.start(spot, spot, sem, x_side, away, leaving=x_leaving)
            sends.start(spot, spot, y_sem.at[0], y_side, away, leaving=y_leaving)
    send_weights(side, False, mate_leaving, near, middle)
    for _, _, i in groups:
        for j in range(2):
            spot, sem = block(i, y * 2 + j), token_sem.at[i, j]
            arrived(spot, sem)
            sends.start(spot, spot, y_sem.at[0], y_side, leaving=y_leaving)

    send_weights(side, False, mate_leaving, near, ends)
    send_weights(1 - side, False, other_leaving, near)
    for k in (jnp.where(near, 1 - side, 1 - odd), jnp.where(near, side, odd)):
        send_weights(k, True, sends.shared((share,)))
    for number in range(3):
        send_out(number, first)
    for number in range(2):
        send_out(number, second, near)

    arrived(blocks(8), y_sem.at[0])
    for index, array in enumerate(own_arrays):
        arrived(array, own_sem.at[index], near)
    arrived(offsets, offset_sem.at[0], first)

    @pl.when(first)
    def _():
        gate_rows[...] = jnp.zeros_like(gate_rows)
        gate_rows[0:2, :] = gate_weights[0].astype(f32)
        gate_rows[2:4, :] = gate_weights[1].astype(f32)
        gates = lax.dot_general(
            lines[...], gate_rows[...].astype(bf16), NT, preferred_element_type=f32
        ).T
        shift = [jnp.concatenate([offsets[i, kind] for i in range(4)], 1) for kind in range(2)]
        gate_in = pick(odd, gates[0:1] + shift[0][0:1], gates[1:2] + shift[0][1:2])
        forget = pick(odd, gates[2:3] + shift[1][0:1], gates[3:4] + shift[1][1:2])
        forget_log = jnp.minimum(forget, 0.0) - jnp.log1p(jnp.exp(-jnp.abs(forget)))
        coarse = jnp.round(forget_log * 8.0) * 0.125
        within = prefix_sums(stacked((coarse, forget_log - coarse), rows))
        which = lax.broadcasted_iota(jnp.int32, (ROW_TILE, rows), 0)
        level_here[...] = jnp.where(which == 2, gate_in, within)

    first_core, second_core = core == 0, core == 1
    sends.start(level_here, level_before, level_sem.at[0], peer, first, first_core)

    @pl.when(jnp.logical_and(first, first_core))
    def _():
        level_before[...] = jnp.zeros_like(level_before)
        keys[:rows, :] = jnp.zeros_like(keys[:rows, :])
        values[:rows, :] = jnp.zeros_like(values[:rows, :])

    scale = head_dim ** (-0.5)
    reach = (rows + span, 2 * rows)
    stores = (weight_near, weight_far)

    def position_weights():
        before = level_before[...]
        which = lax.broadcasted_iota(jnp.int32, (ROW_TILE, rows), 0)
        here = level_here[...] + jnp.where(which < 2, before[:, rows - 1 :], 0.0)
        from_rows = jnp.concatenate([before, here], axis=1)
        to_columns = as_columns(here)
        tile = 64
        for start in range(0, rows, tile):
            index = start // span
            width = reach[index]
            to = to_columns[start : start + tile]
            log_weight = (
                (to[:, 0:1] - from_rows[0:1, :width])
                + (to[:, 1:2] - from_rows[1:2, :width])
                + from_rows[2:3, :width]
            )
            at = lax.broadcasted_iota(jnp.int32, (tile, width), 1)
            until = lax.broadcasted_iota(jnp.int32, (tile, width), 0) + (start + rows)
            seen = jnp.logical_and(at <= until, at >= rows * (1 - core))
            log_weight = jnp.where(seen, log_weight, -jnp.inf)
            weight = jnp.exp(log_weight - jnp.max(log_weight, axis=1, keepdims=True)) * scale
            stores[index][start - index * span : start - index * span + tile, :] = weight

    forward_leaving = sends.shared((weights.at[: 7 * depth // 2, :],))

    def own_unit(i):
        for unit in range(2):
            spot, sem = piece(unit, i), weight_sem.at[unit, i]
            arrived(spot, sem, core == unit)
            sends.start(spot, spot, sem, peer, core == unit, leaving=forward_leaving)

    def other_unit(i):
        for unit in range(2):
            arrived(piece(unit, i), weight_sem.at[unit, i], core != unit)

    def multiply(start, size):
        part = pl.ds(pl.multiple_of(start, size), size)
        return jnp.dot(lines[:, part], weights[part, :], preferred_element_type=f32)

    z_mate = side * 2 + 1 - odd
    z_far = (jnp.where(side == 0, 3, 0), jnp.where(side == 0, 2, 1))
    own_unit(z_mate * 2 + x)
    own_unit(z_far[0] * 2 + x)
    arrived(level_before, level_sem.at[0], first, second_core)
    when((first,), position_weights)
    for i in (z * 2 + 1 - x, z_mate * 2 + 1 - x):
        own_unit(i)
    for i in (z_mate * 2 + x, z * 2 + 1 - x, z_mate * 2 + 1 - x):
        other_unit(i)
    for unit in range(2):
        arrived(piece(unit, me), weight_sem.at[unit, me], near)
    half = count // 2 * depth
    product[...] = multiply(side * half, half)
    own_unit(z_far[0] * 2 + 1 - x)
    own_unit(z_far[1] * 2 + x)
    own_unit(z_far[1] * 2 + 1 - x)
    for pair in z_far:
        other_unit(pair * 2)
        other_unit(pair * 2 + 1)
        product[...] += multiply(pair * 2 * depth, 2 * depth)

    @pl.when(second)
    def _():
        queries[...] = product[:, :head_dim].astype(bf16)

    leaving = sends.shared((queries, second))
    for index in range(2):
        part = queries.at[index * span : (index + 1) * span, :]
        sends.start(part, part, query_sem.at[index], x_side, second, leaving=leaving)

    @pl.when(first)
    def _():
        keys[rows:, :] = product[:, :head_dim].astype(bf16)
        values[rows:, :] = product[:, head_dim:].astype(bf16)

    leaving = sends.shared((keys, first, first_core))
    for array in (keys, values):
        sends.start(
            array.at[rows:, :],
            array.at[:rows, :],
            pair_sem.at[0],
            peer,
            first,
            first_core,
            leaving=leaving,
        )

    halo = extended.shape[0] - rows

    @pl.when(second)
    def _():
        gated = product[:, head_dim : head_dim + channels] * jax.nn.sigmoid(
            product[:, head_dim + channels :]
        )
        extended[halo:, :] = gated.astype(bf16).astype(f32)

    sends.start(
        extended.at[rows:, :], extended.at[:halo, :], halo_sem.at[0], peer, second, first_core
    )

    @pl.when(jnp.logical_and(second, first_core))
    def _():
        extended[:halo, :] = jnp.zeros((halo, channels), f32)

    arrived(extended.at[:halo, :], halo_sem.at[0], second, second_core)
    source_index = y * layers + z

    @pl.when(second)
    def _():
        number = taps.shape[0]
        kernel = taps[...].astype(f32)
        kernel = pick(odd, kernel[:, :channels], kernel[:, channels:])
        for start in range(0, rows, length):
            base = start + halo - (number - 1)
            total = extended[base : base + length, :] * kernel[0:1]
            for index in range(1, number):
                total = total + (
                    extended[base + index : base + index + length, :] * kernel[index : index + 1]
                )
            conv[start : start + length, :] = total
        all_rows = conv[...]
        both = as_rows(
            (
                jnp.sum(all_rows, axis=1, keepdims=True),
                jnp.sum(all_rows * all_rows, axis=1, keepdims=True),
            )
        )
        sums_done[...] = jnp.concatenate(
            [both[:2, start : start + LANES] for start in range(0, rows, LANES)], axis=0
        )
        sums_in[source_index] = sums_done[...]

    sources = [(z_other, y_other) for z_other in range(layers) for y_other in range(2)]
    others = sums_in.at[: count - 1]
    leaving = sends.shared((others, second))
    for z_other, y_other in sources:
        away = jnp.logical_or(z != z_other, y != y_other)
        device = (z_other * 2 + 1, y_other * 2 + core)
        sends.start(
            sums_done,
            sums_in.at[source_index],
            sums_sem.at[0],
            device,
            second,
            away,
            leaving=leaving,
        )
    arrived(others, sums_sem.at[0], second)

    @pl.when(second)
    def _():
        total = sums_in[0]
        for index in range(1, 2 * layers):
            total = total + sums_in[index]
        total = total * (1.0 / (2 * layers * channels))
        total = jnp.concatenate([total[at : at + 2] for at in range(0, ROW_TILE, 2)], axis=1)
        mean = total[0:1]
        inverse = lax.rsqrt(total[1:2] - mean * mean + EPS)
        across = as_columns(stacked((mean, inverse), rows))
        gain = conv_gain[...]
        gain = pick(odd, gain[:, :channels], gain[:, channels:])
        normed = (conv[...] - across[:, 0:1]) * across[:, 1:2] * gain
        conv_done[...] = (normed * jax.nn.sigmoid(normed)).astype(bf16)

    piece_rows = span * (head_dim + channels) // (2 * head_dim)

    def so_many(number):
        return weights.at[: number * piece_rows, :]

    up_leaving = sends.shared(*((so_many(at + 1), z == at) for at in range(layers - 1)))
    down_leaving = sends.shared(*((so_many(layers - at), z == at) for at in range(1, layers)))
    given_leaving = sends.shared((memory_in.at[0], first), (conv_in.at[0], second))

    def spread(done, inside, semaphores, home, index):
        here = x == home
        kept = done.at[(2 * index + home) * length : (2 * index + home + 1) * length, :]
        given = done.at[(2 * index + 1 - home) * length : (2 * index + 2 - home) * length, :]
        part = slice(index * length, (index + 1) * length)
        target, sem = inside.at[z, part, :], semaphores.at[z, index]
        sends.start(given, target, sem, x_side, here, leaving=given_leaving)
        sends.start(kept, target, sem, below, here, has_below, leaving=down_leaving)
        sends.start(kept, target, sem, above, here, has_above, leaving=up_leaving)

        @pl.when(here)
        def _():
            inside[z, part, :] = kept[...]

    for index in range(2):
        spread(conv_done, conv_in, conv_sem, 1, index)
    for number in range(2):
        send_out(number, second, far)
    send_out(2, second)

    for array in (keys,):
        arrived(array, pair_sem.at[0], first, second_core)
    for index in range(2):
        arrived(
            queries.at[index * span : (index + 1) * span, :], query_sem.at[index], first
        )

        @pl.when(first)
        def _():
            width = reach[index]
            gain = memory_gain[...]
            gain = pick(odd, gain[:, :head_dim], gain[:, head_dim:])
            for inner in range(2):
                start = index * span + inner * length
                scores = lax.dot_general(
                    queries[start : start + length, :],
                    keys[:width, :],
                    NT,
                    preferred_element_type=f32,
                )
                scores = scores * stores[index][inner * length : (inner + 1) * length, :]
                numer = jnp.dot(
                    scores.astype(bf16), values[:width, :], preferred_element_type=f32
                )
                denom = jnp.sum(scores, axis=1, keepdims=True)
                cell = numer / jnp.maximum(jnp.abs(denom), 1.0)
                memory_done[start : start + length, :] = (cell * gain).astype(bf16)
                square = as_rows((jnp.sum(cell * cell, axis=1, keepdims=True),))
                squares_done[index, inner] = square[0:1]
            squares_in[index * count + source_index] = squares_done[index, 0]

        spread(memory_done, memory_in, memory_sem, 0, index)
        squares_leaving = sends.shared((squares_in.at[: 2 * count - 1], first))
        for z_other, y_other in sources:
            for x_other in range(2):
                away = jnp.logical_or(
                    jnp.logical_or(z != z_other, y != y_other), x != x_other
                )
                sends.start(
                    squares_done.at[index, x_other],
                    squares_in.at[index * count + source_index],
                    squares_sem.at[index],
                    (z_other * 2 + x_other, y_other * 2 + core),
                    first,
                    away,
                    leaving=squares_leaving,
                )

    order = line_order(z, layers)
    across = (1 - x) * 2 + core
    across_leaving = sends.shared((three_pieces,))

    def pass_on(distance, kind, index, *conditions):
        inside, semaphores, home = kind
        part = slice(index * length, (index + 1) * length)
        if distance == 0:
            away = x != home
            spot, sem = inside.at[z, part, :], semaphores.at[z, index]
            arrived(spot, sem, away, *conditions)
            for device, further, leaving in (
                (below, has_below, down_leaving),
                (above, has_above, up_leaving),
            ):
                sends.start(spot, spot, sem, device, away, further, *conditions, leaving=leaving)
            return
        down, up = order[2 * distance - 2 : 2 * distance]
        for (source, there, onward, further), leaving in ((down, up_leaving), (up, down_leaving)):
            spot, sem = inside.at[source, part, :], semaphores.at[source, index]
            arrived(spot, sem, there, *conditions)
            device = (onward * 2 + x, tp)
            sends.start(spot, spot, sem, device, there, further, *conditions, leaving=leaving)

    def share_out(*conditions):
        arrived(three_pieces, out_sem.at[across], *conditions)
        for spot in (memory_out.at[across], conv_out.at[across]):
            sends.start(spot, spot, out_sem.at[across], peer, *conditions, leaving=across_leaving)

    convs, memories = (conv_in, conv_sem, 1), (memory_in, memory_sem, 0)
    pass_on(0, convs, 0, first)
    pass_on(0, convs, 1, first)
    for distance in range(1, layers):
        for kind in (memories, convs):
            for index in range(2):
                if distance + 1 < layers or index == 0:
                    pass_on(distance, kind, index, first)
        if distance == layers - 2:
            share_out(first)
    share_out(second)
    for distance in range(1, layers + 2):
        if distance < layers:
            pass_on(distance, convs, 0, second)
            pass_on(distance, convs, 1, second)
        if 0 <= distance - 1 < layers:
            pass_on(distance - 1, memories, 0, second)
        if 0 <= distance - 2 < layers - 1:
            pass_on(distance - 2, memories, 1, second)
    entries = layers * 2 * head_dim
    for index in range(2):
        part = slice(index * length, (index + 1) * length)
        if index == 1:
            pass_on(layers - 1, memories, 1)
            pass_on(layers - 1, convs, 1, first)
        at = index * count
        arrived(squares_in.at[at : at + count - 1], squares_sem.at[index], first)
        arrived(squares_in.at[at : at + count], squares_sem.at[index], second)
        if index == 0:
            for group in range(2):
                arrived(three_pieces, out_sem.at[group * 2 + 1 - core])
        total = squares_in[at]
        for slot in range(1, 2 * layers):
            total = total + squares_in[at + slot]
        row_scale = stacked((lax.rsqrt(total * (1.0 / entries) + EPS),), length)
        row_scale = as_columns(row_scale)[:, 0:1]
        for group in range(2):
            from_memory, from_conv = None, None
            for head in range(layers):
                where = group * 2 + 1 - head // 2
                inner = head % 2
                memory_term = jnp.dot(
                    memory_in[head, part, :],
                    memory_out[where, inner * head_dim : (inner + 1) * head_dim, :],
                    preferred_element_type=f32,
                )
                conv_term = jnp.dot(
                    conv_in[head, part, :],
                    conv_out[where, inner * channels : (inner + 1) * channels, :],
                    preferred_element_type=f32,
                )
                from_memory = memory_term if head == 0 else from_memory + memory_term
                from_conv = conv_term if head == 0 else from_conv + conv_term
            width = from_memory.shape[1]
            partial[index, :, group * width : (group + 1) * width] = (
                from_conv + row_scale * from_memory
            ).astype(bf16)
        device = ((core * 2 + index) * 2 + x, z)
        away = jnp.logical_or(core * 2 + index != z, tp != z)
        sends.start(partial.at[index], slots.at[y], slot_sem.at[y], device, away)

        @pl.when(jnp.logical_not(away))
        def _():
            slots[y] = partial[index]

    for y_other in range(2):
        own = jnp.logical_and(tp == z, jnp.logical_and(y == y_other, core == side))
        arrived(slots.at[y_other], slot_sem.at[y_other], jnp.logical_not(own))
    sends.finish()


def layer(arrays):
    count, columns = lax.axis_size("sp"), lax.axis_size("tp")
    (
        tokens,
        conv_value_weight,
        conv_gate_weight,
        conv_kernel,
        conv_norm_gain,
        query_weight,
        key_weight,
        value_weight,
        input_gate_weight,
        forget_gate_weight,
        input_offset,
        forget_offset,
        memory_norm_gain,
        conv_out_weight,
        memory_out_weight,
    ) = arrays
    length, features = tokens.shape
    depth, head_dim = query_weight.shape[0], query_weight.shape[1] // 2
    channels = conv_value_weight.shape[1] // 2
    wide = features * columns
    rows = length * count // 2
    span = rows // 2
    layers = count // 2
    halo = -(-(conv_kernel.shape[0] - 1) // ROW_TILE) * ROW_TILE
    width = memory_out_weight.shape[1]
    f32, bf16 = jnp.float32, jnp.bfloat16
    DMA = pltpu.SemaphoreType.DMA
    V = pltpu.VMEM
    return pl.pallas_call(
        lambda *refs: layer_kernel(count, columns, *refs),
        out_shape=jax.ShapeDtypeStruct((2, length, features), bf16),
        in_specs=[pl.BlockSpec(memory_space=pltpu.HBM)] * 15,
        out_specs=IN_VMEM,
        scratch_shapes=[
            V(tokens.shape, bf16),
            V(query_weight.shape, bf16),
            V(key_weight.shape, bf16),
            V(value_weight.shape, bf16),
            V(conv_value_weight.shape, bf16),
            V(conv_gate_weight.shape, bf16),
            V((2, 2, length), f32),
            V((rows, wide), bf16),
            V((wide, 2 * head_dim), bf16),
            V((rows, 2 * head_dim), f32),
            V(conv_kernel.shape, bf16),
            V((1, 2 * channels), f32),
            V((1, 2 * head_dim), f32),
            V((2, 2, wide), bf16),
            V((4, 2, 2, length), f32),
            V((LANES, wide), f32),
            V((ROW_TILE, rows), f32),
            V((ROW_TILE, rows), f32),
            V((2 * rows, head_dim), bf16),
            V((2 * rows, head_dim), bf16),
            V((rows, head_dim), bf16),
            V((span, rows + span), f32),
            V((span, 2 * rows), f32),
            V((rows, head_dim), bf16),
            V((2, 2, 1, length), f32),
            V((2 * count, 1, length), f32),
            V((halo + rows, channels), f32),
            V((rows, channels), f32),
            V((ROW_TILE, LANES), f32),
            V((count, ROW_TILE, LANES), f32),
            V((rows, channels), bf16),
            V((layers, span, head_dim), bf16),
            V((layers, span, channels), bf16),
            V((4, 2 * head_dim, width), bf16),
            V((4, 2 * channels, width), bf16),
            V((2, length, features), bf16),
            DMA((16,)),
            DMA((SENDS,)),
            DMA((4, 2)),
            DMA((1,)),
            DMA((2, count)),
            DMA((4,)),
            DMA((1,)),
            DMA((1,)),
            DMA((1,)),
            DMA((2,)),
            DMA((1,)),
            DMA((1,)),
            DMA((2,)),
            DMA((layers, 2)),
            DMA((layers, 2)),
            DMA((4,)),
            DMA((2,)),
        ],
        compiler_params=pltpu.CompilerParams(
            collective_id=0, has_side_effects=True
        ),
    )(
        tokens,
        query_weight,
        key_weight,
        value_weight,
        conv_value_weight,
        conv_gate_weight,
        conv_kernel,
        conv_norm_gain.reshape(1, -1),
        memory_norm_gain.reshape(1, -1),
        input_gate_weight.T,
        forget_gate_weight.T,
        input_offset.T,
        forget_offset.T,
        memory_out_weight,
        conv_out_weight,
    )


def on_device_by_column(*arrays):
    slots = layer(arrays)
    return jnp.sum(slots.astype(jnp.float32), axis=0).astype(jnp.bfloat16)


def splits_by_column(mesh, tokens, query_weight, conv_value_weight, conv_kernel, input_gate_weight):
    count, columns = mesh.shape["sp"], mesh.shape["tp"]
    heads = input_gate_weight.shape[1]
    head_dim = query_weight.shape[1] // heads
    length = tokens.shape[0] // count
    return (
        count == 8
        and columns == 4
        and heads == count
        and length == LANES
        and tokens.size * 2 <= 4 * 2**20
        and conv_value_weight.shape[1] * 2 == head_dim * heads
        and head_dim == 256
        and conv_kernel.shape[0] - 1 <= length
    )


def solution(mesh):
    in_specs = (
        P("sp", "tp"),
        P("sp", "tp"),
        P("sp", "tp"),
        P(None, "tp"),
        P("tp"),
        P("sp", "tp"),
        P("sp", "tp"),
        P("sp", "tp"),
        P(None, "tp"),
        P(None, "tp"),
        P("sp", "tp"),
        P("sp", "tp"),
        P("tp"),
        P("tp", "sp"),
        P("tp", "sp"),
    )
    out_specs = P("sp", "tp")

    def run(*arrays):
        by_column = splits_by_column(
            mesh, arrays[0], arrays[5], arrays[1], arrays[3], arrays[8]
        )
        on_device = on_device_by_column if by_column else on_device_by_position
        return jax.shard_map(
            on_device, mesh=mesh, in_specs=in_specs, out_specs=out_specs, check_vma=False
        )(*arrays)

    return run
```

```python
import jax
import jax.numpy as jnp
from jax import lax
from jax.experimental import pallas as pl
from jax.experimental.pallas import tpu as pltpu
from jax.sharding import PartitionSpec as P

BLOCK = 64


EPS = 1e-06
LOWEST_LEVEL = -1e30


def shifted_2(value, axis, steps):
    count = lax.axis_size(axis)
    leading, last = (max(0, -steps), min(count, count - steps))
    return lax.ppermute(value, axis, [(source, source + steps) for source in range(leading, last)])


def carried_in(shard, axis, join, neutral):
    place = lax.axis_index(axis)
    gathered = jax.tree.map(
        lambda a, kind: lax.all_gather(a.astype(kind), axis),
        shard,
        (jnp.bfloat16, jnp.bfloat16, jnp.bfloat16, jnp.bfloat16),
    )
    state = jax.tree.map(lambda a, e: jnp.zeros_like(a) + jnp.asarray(e, a.dtype), shard, neutral)

    def one(step, state):
        return join(
            state,
            jax.tree.map(
                lambda a, own: lax.dynamic_index_in_dim(a, step, 0, False).astype(own.dtype),
                gathered,
                shard,
            ),
        )

    return lax.fori_loop(0, place, one, state)


def block_step(carry, inputs):
    state, normal, level = carry
    query, key, value, gate_in, forget_log = inputs
    length = gate_in.shape[-1]
    scale = query.shape[-1] ** (-0.5)
    causal = jnp.tril(jnp.ones((length, length), dtype=bool))
    within = jnp.cumsum(forget_log, axis=-1)
    log_weight = within[:, :, None] - within[:, None, :] + gate_in[:, None, :]
    log_weight = jnp.where(causal, log_weight, -jnp.inf)
    carried = within + level[:, None]
    top = jnp.maximum(carried, jnp.max(log_weight, axis=-1))
    weight = jnp.exp(log_weight - top[:, :, None])
    carried_weight = jnp.exp(carried - top) * scale
    scores = jnp.einsum("htd,hsd->hts", query, key, preferred_element_type=jnp.float32) * (
        scale * weight
    )
    numer = jnp.einsum(
        "hts,hse->hte", scores.astype(jnp.bfloat16), value, preferred_element_type=jnp.float32
    )
    numer = numer + carried_weight[:, :, None] * jnp.einsum(
        "hed,htd->hte", state.astype(jnp.bfloat16), query, preferred_element_type=jnp.float32
    )
    denom = jnp.sum(scores, axis=-1) + carried_weight * jnp.einsum(
        "hd,htd->ht", normal.astype(jnp.bfloat16), query, preferred_element_type=jnp.float32
    )
    result = numer / jnp.maximum(jnp.abs(denom), 1.0)[:, :, None]
    last = within[:, -1]
    end_log = last[:, None] - within + gate_in
    new_level = jnp.maximum(last + level, jnp.max(end_log, axis=-1))
    keep = jnp.exp(last + level - new_level)
    fresh = jnp.exp(end_log - new_level[:, None])
    scaled_key = (fresh[:, :, None] * key).astype(jnp.bfloat16)
    new_state = keep[:, None, None] * state + jnp.einsum(
        "hse,hsd->hed", value, scaled_key, preferred_element_type=jnp.float32
    )
    new_normal = keep[:, None] * normal + jnp.sum(scaled_key.astype(jnp.float32), axis=1)
    return ((new_state, new_normal, new_level), result)


def depthwise(extended, kernel):
    taps = kernel.shape[0]
    length = extended.shape[0] - taps + 1
    total = extended[0:length] * kernel[0]
    for index in range(1, taps):
        total = total + extended[index : index + length] * kernel[index]
    return total


def merge_states(first, second):
    first_state, first_normal, first_level, first_total = first
    second_state, second_normal, second_level, second_total = second
    shifted = first_level + second_total
    level = jnp.maximum(shifted, second_level)
    older = jnp.exp(shifted - level)
    newer = jnp.exp(second_level - level)
    state = older[:, None, None] * first_state + newer[:, None, None] * second_state
    normal = older[:, None] * first_normal + newer[:, None] * second_normal
    return (state, normal, level, first_total + second_total)


def on_device_by_position(
    tokens,
    conv_value_weight,
    conv_gate_weight,
    conv_kernel,
    conv_norm_gain,
    query_weight,
    key_weight,
    value_weight,
    input_gate_weight,
    forget_gate_weight,
    input_offset,
    forget_offset,
    memory_norm_gain,
    conv_out_weight,
    memory_out_weight,
):
    length = tokens.shape[0]
    heads_here = input_gate_weight.shape[1]
    whole = lax.all_gather(tokens, "tp", axis=1, tiled=True)
    pieces = (
        lax.all_gather(conv_value_weight, "sp", axis=0, tiled=True),
        lax.all_gather(conv_gate_weight, "sp", axis=0, tiled=True),
        lax.all_gather(query_weight, "sp", axis=0, tiled=True),
        lax.all_gather(key_weight, "sp", axis=0, tiled=True),
        lax.all_gather(value_weight, "sp", axis=0, tiled=True),
    )
    folded = tuple((jnp.dot(whole, piece, preferred_element_type=jnp.float32) for piece in pieces))
    conv_value, conv_gate, query_flat, key_flat, value_flat = folded
    gate_pre = jnp.dot(whole, input_gate_weight, preferred_element_type=jnp.float32)
    forget_pre = jnp.dot(whole, forget_gate_weight, preferred_element_type=jnp.float32)
    glu = (conv_value * jax.nn.sigmoid(conv_gate)).astype(jnp.bfloat16)
    taps = conv_kernel.shape[0]
    head_dim = query_flat.shape[1] // heads_here

    def to_heads(flat):
        return flat.astype(jnp.bfloat16).reshape(length, heads_here, head_dim).transpose(1, 0, 2)

    query = to_heads(query_flat)
    key = to_heads(key_flat)
    value = to_heads(value_flat)
    gate_in = (gate_pre + input_offset).T
    forget_log = jax.nn.log_sigmoid(forget_pre + forget_offset).T
    within = jnp.cumsum(forget_log, axis=1)
    total = within[:, -1]
    end_log = total[:, None] - within + gate_in
    local_level = jnp.max(end_log, axis=1)
    fresh = jnp.exp(end_log - local_level[:, None])
    scaled_key = (fresh[:, :, None] * key).astype(jnp.bfloat16)
    local_state = jnp.einsum("hse,hsd->hed", value, scaled_key, preferred_element_type=jnp.float32)
    local_normal = jnp.sum(scaled_key.astype(jnp.float32), axis=1)
    blank_state = (
        jnp.zeros_like(local_state),
        jnp.zeros_like(local_normal),
        jnp.full_like(local_level, LOWEST_LEVEL),
        jnp.zeros_like(total),
    )
    prior = shifted_2(glu[length - (taps - 1) :], "sp", 1)
    incoming = carried_in(
        (local_state, local_normal, local_level, total), "sp", merge_states, blank_state
    )
    extended = jnp.concatenate([prior, glu], axis=0).astype(jnp.float32)
    conv = depthwise(extended, conv_kernel.astype(jnp.float32))
    blocks = length // BLOCK

    def split(array):
        return jnp.moveaxis(array.reshape((heads_here, blocks, BLOCK) + array.shape[2:]), 1, 0)

    _, hidden = lax.scan(
        block_step,
        tuple(incoming[:3]),
        (split(query), split(key), split(value), split(gate_in), split(forget_log)),
    )
    hidden = jnp.moveaxis(hidden, 0, 1).reshape(heads_here, length, head_dim)
    hidden_squares = jnp.sum(hidden * hidden, axis=(0, 2))
    channel_sum, channel_squares, memory_squares = lax.psum(
        (jnp.sum(conv, axis=1), jnp.sum(conv * conv, axis=1), hidden_squares), "tp"
    )
    channels = conv.shape[1] * lax.axis_size("tp")
    mean = (channel_sum / channels)[:, None]
    variance = (channel_squares / channels)[:, None] - mean * mean
    conv_branch = jax.nn.silu((conv - mean) * lax.rsqrt(variance + EPS) * conv_norm_gain).astype(
        jnp.bfloat16
    )
    entries = heads_here * head_dim * lax.axis_size("tp")
    memory_scale = lax.rsqrt(memory_squares / entries + EPS)
    hidden = hidden * memory_scale[None, :, None]
    hidden = hidden * memory_norm_gain.reshape(heads_here, 1, head_dim)
    memory_branch = (
        hidden.transpose(1, 0, 2).reshape(length, heads_here * head_dim).astype(jnp.bfloat16)
    )
    conv_columns, memory_columns = (
        lax.all_gather(conv_out_weight, "sp", axis=1, tiled=True),
        lax.all_gather(memory_out_weight, "sp", axis=1, tiled=True),
    )
    contract = (((0,), (1,)), ((), ()))
    summed = lax.psum_scatter(
        (
            lax.dot_general(conv_columns, conv_branch, contract, preferred_element_type=jnp.float32)
            + lax.dot_general(
                memory_columns, memory_branch, contract, preferred_element_type=jnp.float32
            )
        ).astype(jnp.bfloat16),
        "tp",
        scatter_dimension=0,
        tiled=True,
    ).astype(jnp.float32)
    return summed.T.astype(jnp.bfloat16)


MESH = pl.DeviceIdType.MESH
IN_VMEM = pl.BlockSpec(memory_space=pltpu.VMEM)
SENDS = 30
ROW_TILE = 8
LANES = 128
NT = (((1,), (1,)), ((), ()))


def when(conditions, action):
    if not conditions:
        action()
        return
    every = conditions[0]
    for condition in conditions[1:]:
        every = jnp.logical_and(every, condition)
    pl.when(every)(action)


class Sends:
    def __init__(self, semaphores):
        self.semaphores = semaphores
        self.waits = []
        self.used = 0

    def shared(self, *waits):
        semaphore = self.semaphores.at[self.used]
        self.used += 1
        for whole, *conditions in waits:
            self.waits.append((whole, semaphore, conditions))
        return semaphore

    def start(self, source, target, arrival, device, *conditions, leaving=None):
        if leaving is None:
            leaving = self.shared((source, *conditions))
        copy = pltpu.make_async_remote_copy(
            src_ref=source,
            dst_ref=target,
            send_sem=leaving,
            recv_sem=arrival,
            device_id=device,
            device_id_type=MESH,
        )
        when(conditions, copy.start)

    def finish(self):
        for whole, semaphore, conditions in self.waits:
            when(conditions, waiting(whole, semaphore).wait_send)


def waiting(block, semaphore):
    return pltpu.make_async_remote_copy(
        src_ref=block,
        dst_ref=block,
        send_sem=semaphore,
        recv_sem=semaphore,
        device_id=(lax.axis_index("sp"), lax.axis_index("tp")),
        device_id_type=MESH,
    )


def arrived(block, semaphore, *conditions):
    copy = waiting(block, semaphore)
    when(conditions, copy.wait_recv)


def line_order(here, count):
    order = []
    for distance in range(1, count):
        order.append((here - distance, here >= distance, here + 1, here + 1 < count))
        order.append((here + distance, here + distance < count, here - 1, here > 0))
    return order


def pick(index, first, second):
    return jnp.where(jnp.full(first.shape, index, jnp.int32) == 1, second, first)


def stacked(rows, length):
    place = lax.broadcasted_iota(jnp.int32, (ROW_TILE, length), 0)
    result = jnp.zeros((ROW_TILE, length), jnp.float32)
    for index, row in enumerate(rows):
        result = jnp.where(place == index, row, result)
    return result


def as_columns(rows):
    length = rows.shape[1]
    rest = jnp.zeros((LANES - ROW_TILE, length), jnp.float32)
    return jnp.concatenate([rows, rest], axis=0).T


def as_rows(columns):
    length = columns[0].shape[0]
    place = lax.broadcasted_iota(jnp.int32, (length, LANES), 1)
    result = jnp.zeros((length, LANES), jnp.float32)
    for index, column in enumerate(columns):
        result = jnp.where(place == index, column, result)
    return result.T[:ROW_TILE]


def prefix_sums(rows):
    before = lax.broadcasted_iota(jnp.int32, (LANES, LANES), 0)
    after = lax.broadcasted_iota(jnp.int32, (LANES, LANES), 1)
    upper = (before <= after).astype(jnp.float32)
    carry = jnp.zeros((ROW_TILE, 1), jnp.float32)
    parts = []
    for start in range(0, rows.shape[1], LANES):
        part = carry + jnp.dot(
            rows[:, start : start + LANES],
            upper,
            precision=lax.Precision.HIGHEST,
            preferred_element_type=jnp.float32,
        )
        carry = part[:, LANES - 1 :]
        parts.append(part)
    return jnp.concatenate(parts, axis=1)


def layer_kernel(
    count,
    columns,
    all_tokens,
    all_wq,
    all_wk,
    all_wv,
    all_wcv,
    all_wcg,
    own_taps,
    own_conv_gain,
    own_memory_gain,
    own_input_gates,
    own_forget_gates,
    own_input_offsets,
    own_forget_offsets,
    own_memory_out,
    own_conv_out,
    slots,
    tokens,
    wq,
    wk,
    wv,
    wcv,
    wcg,
    shifts,
    lines,
    weights,
    product,
    taps,
    conv_gain,
    memory_gain,
    gate_weights,
    offsets,
    gate_rows,
    level_before,
    level_here,
    keys,
    values,
    queries,
    weight_near,
    weight_far,
    memory_done,
    squares_done,
    squares_in,
    extended,
    conv,
    sums_done,
    sums_in,
    conv_done,
    memory_in,
    conv_in,
    memory_out,
    conv_out,
    partial,
    load_sem,
    send_sem,
    token_sem,
    y_sem,
    weight_sem,
    own_sem,
    offset_sem,
    level_sem,
    pair_sem,
    query_sem,
    halo_sem,
    sums_sem,
    squares_sem,
    memory_sem,
    conv_sem,
    out_sem,
    slot_sem,
):
    f32, bf16 = jnp.float32, jnp.bfloat16
    me, tp = lax.axis_index("sp"), lax.axis_index("tp")
    layers = count // 2
    z, x, y, core = me // 2, lax.rem(me, 2), tp // 2, lax.rem(tp, 2)
    side, odd = z // 2, lax.rem(z, 2)
    length, features = tokens.shape
    depth, head_dim = wq.shape[0], wq.shape[1] // 2
    channels = wcv.shape[1] // 2
    rows = 4 * length
    span = rows // 2
    near, far = core == side, core != side
    first, second = x == 0, x == 1
    middle = jnp.logical_or(z == 1, z == 2)
    ends = jnp.logical_not(middle)
    peer = (me, y * 2 + 1 - core)
    below, above = (me - 2, tp), (me + 2, tp)
    x_side = (z * 2 + 1 - x, tp)
    y_side = (me, (1 - y) * 2 + core)
    has_below, has_above = z > 0, z + 1 < layers
    sends = Sends(send_sem)

    barrier = pltpu.get_barrier_semaphore()
    devices = count * columns
    rank = me * columns + tp
    for step in range(1, devices):
        other = lax.rem(rank + step, devices)
        pl.semaphore_signal(
            barrier,
            inc=1,
            device_id=(other // columns, lax.rem(other, columns)),
            device_id_type=MESH,
        )

    def block(i, j):
        return lines.at[
            pl.ds(pl.multiple_of(i * length, length), length),
            pl.ds(pl.multiple_of(j * features, features), features),
        ]

    def blocks(number):
        return lines.at[: number * length // columns, :]

    place = odd * 2 + x
    own_part = x * 2 + core
    loads = []
    for source, target, *conditions in (
        (all_tokens, tokens),
        (all_tokens, block(place, tp), near),
        (all_wq, wq),
        (all_wk, wk),
        (all_wv, wv),
        (all_wcv, wcv),
        (all_wcg, wcg),
        (own_input_offsets, shifts.at[0]),
        (own_forget_offsets, shifts.at[1]),
        (own_taps, taps, far),
        (own_conv_gain, conv_gain, far),
        (own_memory_gain, memory_gain, far),
        (own_input_gates, gate_weights.at[0], far),
        (own_forget_gates, gate_weights.at[1], far),
        (own_memory_out, memory_out.at[own_part]),
        (own_conv_out, conv_out.at[own_part]),
    ):
        copy = pltpu.make_async_copy(source, target, load_sem.at[len(loads)])
        loads.append((copy, conditions))
        when(conditions, copy.start)

    def loaded(first_load, last_load):
        for copy, conditions in loads[first_load:last_load]:
            when(conditions, copy.wait)

    loaded(0, 2)
    pl.semaphore_wait(barrier, devices - 1)

    goal = y * 2 + side
    mine, mine_sem = block(place, tp), token_sem.at[place, core]
    z_leaving = sends.shared(
        (blocks(1), ends), (blocks(4), middle, near), (blocks(6), middle, far)
    )
    x_leaving = sends.shared((blocks(3), near), (blocks(5), far))
    y_leaving = sends.shared((blocks(7), near), (blocks(9), far))
    sends.start(tokens, mine, mine_sem, (me - 2, goal), has_below, leaving=z_leaving)
    sends.start(tokens, mine, mine_sem, (me + 2, goal), has_above, leaving=z_leaving)
    sends.start(tokens, mine, mine_sem, (z * 2 + 1 - x, goal), leaving=x_leaving)
    sends.start(tokens, mine, y_sem.at[0], (me, (1 - y) * 2 + side), leaving=y_leaving)
    sends.start(tokens, mine, mine_sem, peer, far)

    def piece(unit, i):
        return weights.at[
            pl.ds(pl.multiple_of(i * depth, depth), depth),
            unit * head_dim : (unit + 1) * head_dim,
        ]

    def shares(k, x_goal):
        whole = pl.ds(pl.multiple_of(k * head_dim, head_dim), head_dim)
        part = pl.ds(pl.multiple_of(k * channels, channels), channels)
        if x_goal == 0:
            return (
                (wk.at[:, whole], 0, 0, head_dim),
                (wv.at[:, whole], 1, head_dim, head_dim),
            )
        return (
            (wq.at[:, whole], 0, 0, head_dim),
            (wcv.at[:, part], 1, head_dim, channels),
            (wcg.at[:, part], 1, head_dim + channels, channels),
        )

    own_rows = pl.ds(pl.multiple_of(me * depth, depth), depth)
    z_first = (1 - core) * 2
    share = weights.at[:depth, :]

    def send_weights(k, cross, leaving, *conditions, to_peer=False):
        for x_goal in range(2):
            chosen = conditions + ((x != x_goal) if cross else (x == x_goal),)
            for source, unit, start, size in shares(k, x_goal):
                device = peer if to_peer else ((z_first + k) * 2 + x_goal, y * 2 + unit)
                target = weights.at[own_rows, start : start + size]
                sends.start(
                    source, target, weight_sem.at[unit, me], device, *chosen, leaving=leaving
                )

    loaded(2, len(loads))
    mate_leaving, other_leaving = sends.shared((share,)), sends.shared((share,))
    send_weights(odd, False, other_leaving, far, to_peer=True)
    send_weights(1 - odd, False, mate_leaving, far)
    for x_goal in range(2):

        def keep():
            for source, _, start, size in shares(odd, x_goal):
                weights[own_rows, start : start + size] = source[...]

        when((far, x == x_goal), keep)

    own_arrays = (taps, conv_gain, memory_gain, gate_weights)
    for index, array in enumerate(own_arrays):
        sends.start(array, array, own_sem.at[index], peer, far)
    leaving = sends.shared((offsets.at[:2],))
    for k in range(2):
        device = ((z_first + k) * 2, y * 2 + side)
        sends.start(shifts, offsets.at[place], offset_sem.at[0], device, leaving=leaving)

    half_rows = memory_out.shape[1] // 2
    out_width = memory_out.shape[2]
    three_pieces = weights.at[: 3 * half_rows * out_width // (2 * head_dim), :]

    def out_piece(part, number):
        if number == 1:
            return conv_out.at[part]
        start = half_rows * (number // 2)
        return memory_out.at[part, start : start + half_rows, :]

    out_leaving = [sends.shared((three_pieces,)) for _ in range(2)]

    def send_out(number, *conditions):
        spot = out_piece(own_part, number)
        for device, leaving in zip((x_side, peer), out_leaving):
            sends.start(spot, spot, out_sem.at[own_part], device, *conditions, leaving=leaving)

    k_near = jnp.where(near, odd, 1 - core)
    groups = []
    for k in (k_near, 1 - k_near):
        source = core * 2 + k
        groups.append((source, k * 2 + x, k * 2 + 1 - x))
    for source, i, _ in groups:
        away, up = source != z, source < z
        onward = (jnp.where(up, z + 1, z - 1) * 2 + x, tp)
        for j in range(2):
            spot, sem = block(i, y * 2 + j), token_sem.at[i, j]
            arrived(spot, sem, jnp.logical_or(away, j != core))
            sends.start(spot, spot, sem, onward, away, middle, leaving=z_leaving)
            sends.start(spot, spot, sem, x_side, away, leaving=x_leaving)
            sends.start(spot, spot, y_sem.at[0], y_side, away, leaving=y_leaving)
    cross_leaving = [sends.shared((share,)) for _ in range(2)]
    send_weights(side, False, mate_leaving, near, middle)
    send_weights(odd, True, cross_leaving[1], far)
    send_weights(1 - odd, True, cross_leaving[0], far, ends)
    for _, _, i in groups:
        for j in range(2):
            spot, sem = block(i, y * 2 + j), token_sem.at[i, j]
            arrived(spot, sem)
            sends.start(spot, spot, y_sem.at[0], y_side, leaving=y_leaving)

    send_weights(side, False, mate_leaving, near, ends)
    last = jnp.logical_and(middle, first)
    send_weights(1 - side, False, other_leaving, near, jnp.logical_not(last))
    k_cross = jnp.where(near, 1 - side, 1 - odd)
    send_weights(k_cross, True, cross_leaving[0], jnp.logical_or(near, middle))
    send_weights(side, True, cross_leaving[1], near)
    send_weights(1 - side, False, other_leaving, near, last)
    for number in range(2):
        send_out(number, near)

    arrived(blocks(8), y_sem.at[0])
    for index, array in enumerate(own_arrays):
        arrived(array, own_sem.at[index], near)
    arrived(offsets, offset_sem.at[0], first)

    @pl.when(first)
    def _():
        gate_rows[...] = jnp.zeros_like(gate_rows)
        gate_rows[0:2, :] = gate_weights[0].astype(f32)
        gate_rows[2:4, :] = gate_weights[1].astype(f32)
        gates = lax.dot_general(
            lines[...], gate_rows[...].astype(bf16), NT, preferred_element_type=f32
        ).T
        shift = [jnp.concatenate([offsets[i, kind] for i in range(4)], 1) for kind in range(2)]
        gate_in = pick(odd, gates[0:1] + shift[0][0:1], gates[1:2] + shift[0][1:2])
        forget = pick(odd, gates[2:3] + shift[1][0:1], gates[3:4] + shift[1][1:2])
        forget_log = jnp.minimum(forget, 0.0) - jnp.log1p(jnp.exp(-jnp.abs(forget)))
        coarse = jnp.round(forget_log * 8.0) * 0.125
        within = prefix_sums(stacked((coarse, forget_log - coarse), rows))
        which = lax.broadcasted_iota(jnp.int32, (ROW_TILE, rows), 0)
        level_here[...] = jnp.where(which == 2, gate_in, within)

    first_core, second_core = core == 0, core == 1
    sends.start(level_here, level_before, level_sem.at[0], peer, first, first_core)

    @pl.when(jnp.logical_and(first, first_core))
    def _():
        level_before[...] = jnp.zeros_like(level_before)
        keys[:rows, :] = jnp.zeros_like(keys[:rows, :])
        values[:rows, :] = jnp.zeros_like(values[:rows, :])

    scale = head_dim ** (-0.5)
    reach = (rows + span, 2 * rows)
    stores = (weight_near, weight_far)

    def position_weights():
        before = level_before[...]
        which = lax.broadcasted_iota(jnp.int32, (ROW_TILE, rows), 0)
        here = level_here[...] + jnp.where(which < 2, before[:, rows - 1 :], 0.0)
        from_rows = jnp.concatenate([before, here], axis=1)
        to_columns = as_columns(here)
        tile = 64
        for start in range(0, rows, tile):
            index = start // span
            width = reach[index]
            to = to_columns[start : start + tile]
            log_weight = (
                (to[:, 0:1] - from_rows[0:1, :width])
                + (to[:, 1:2] - from_rows[1:2, :width])
                + from_rows[2:3, :width]
            )
            at = lax.broadcasted_iota(jnp.int32, (tile, width), 1)
            until = lax.broadcasted_iota(jnp.int32, (tile, width), 0) + (start + rows)
            seen = jnp.logical_and(at <= until, at >= rows * (1 - core))
            log_weight = jnp.where(seen, log_weight, -jnp.inf)
            weight = jnp.exp(log_weight - jnp.max(log_weight, axis=1, keepdims=True)) * scale
            stores[index][start - index * span : start - index * span + tile, :] = weight

    forward_leaving = sends.shared((weights.at[: 7 * depth // 2, :],))

    def own_unit(i):
        for unit in range(2):
            spot, sem = piece(unit, i), weight_sem.at[unit, i]
            arrived(spot, sem, core == unit)
            sends.start(spot, spot, sem, peer, core == unit, leaving=forward_leaving)

    def other_unit(i):
        for unit in range(2):
            arrived(piece(unit, i), weight_sem.at[unit, i], core != unit)

    def multiply(start, size):
        part = pl.ds(pl.multiple_of(start, size), size)
        return jnp.dot(lines[:, part], weights[part, :], preferred_element_type=f32)

    z_mate = side * 2 + 1 - odd
    z_far = (jnp.where(side == 0, 3, 0), jnp.where(side == 0, 2, 1))
    own_unit(z_mate * 2 + x)
    own_unit(z_far[0] * 2 + x)
    arrived(level_before, level_sem.at[0], first, second_core)
    when((first,), position_weights)
    for i in (z * 2 + 1 - x, z_mate * 2 + 1 - x):
        own_unit(i)
    for i in (z_mate * 2 + x, z * 2 + 1 - x, z_mate * 2 + 1 - x):
        other_unit(i)
    for unit in range(2):
        arrived(piece(unit, me), weight_sem.at[unit, me], near)
    half = count // 2 * depth
    product[...] = multiply(side * half, half)
    own_unit(z_far[0] * 2 + 1 - x)
    own_unit(z_far[1] * 2 + x)
    own_unit(z_far[1] * 2 + 1 - x)
    for pair in z_far:
        other_unit(pair * 2)
        other_unit(pair * 2 + 1)
        product[...] += multiply(pair * 2 * depth, 2 * depth)

    for number in range(2):
        send_out(number, first, far)
    send_out(2, first)

    @pl.when(second)
    def _():
        queries[...] = product[:, :head_dim].astype(bf16)

    leaving = sends.shared((queries, second))
    for number in range(4):
        part = queries.at[number * length : (number + 1) * length, :]
        sends.start(part, part, query_sem.at[number], x_side, second, leaving=leaving)

    @pl.when(first)
    def _():
        keys[rows:, :] = product[:, :head_dim].astype(bf16)
        values[rows:, :] = product[:, head_dim:].astype(bf16)

    leaving = sends.shared((keys, first, first_core))
    for array in (keys, values):
        sends.start(
            array.at[rows:, :],
            array.at[:rows, :],
            pair_sem.at[0],
            peer,
            first,
            first_core,
            leaving=leaving,
        )

    halo = extended.shape[0] - rows

    @pl.when(second)
    def _():
        gated = product[:, head_dim : head_dim + channels] * jax.nn.sigmoid(
            product[:, head_dim + channels :]
        )
        extended[halo:, :] = gated.astype(bf16).astype(f32)

    sends.start(
        extended.at[rows:, :], extended.at[:halo, :], halo_sem.at[0], peer, second, first_core
    )

    @pl.when(jnp.logical_and(second, first_core))
    def _():
        extended[:halo, :] = jnp.zeros((halo, channels), f32)

    arrived(extended.at[:halo, :], halo_sem.at[0], second, second_core)
    source_index = y * layers + z

    @pl.when(second)
    def _():
        number = taps.shape[0]
        kernel = taps[...].astype(f32)
        kernel = pick(odd, kernel[:, :channels], kernel[:, channels:])
        for start in range(0, rows, length):
            base = start + halo - (number - 1)
            total = extended[base : base + length, :] * kernel[0:1]
            for index in range(1, number):
                total = total + (
                    extended[base + index : base + index + length, :] * kernel[index : index + 1]
                )
            conv[start : start + length, :] = total
        all_rows = conv[...]
        both = as_rows(
            (
                jnp.sum(all_rows, axis=1, keepdims=True),
                jnp.sum(all_rows * all_rows, axis=1, keepdims=True),
            )
        )
        sums_done[...] = jnp.concatenate(
            [both[:2, start : start + LANES] for start in range(0, rows, LANES)], axis=0
        )
        sums_in[source_index] = sums_done[...]

    sources = [(z_other, y_other) for z_other in range(layers) for y_other in range(2)]
    others = sums_in.at[: count - 1]
    leaving = sends.shared((others, second))
    for z_other, y_other in sources:
        away = jnp.logical_or(z != z_other, y != y_other)
        device = (z_other * 2 + 1, y_other * 2 + core)
        sends.start(
            sums_done,
            sums_in.at[source_index],
            sums_sem.at[0],
            device,
            second,
            away,
            leaving=leaving,
        )
    arrived(others, sums_sem.at[0], second)

    @pl.when(second)
    def _():
        total = sums_in[0]
        for index in range(1, 2 * layers):
            total = total + sums_in[index]
        total = total * (1.0 / (2 * layers * channels))
        total = jnp.concatenate([total[at : at + 2] for at in range(0, ROW_TILE, 2)], axis=1)
        mean = total[0:1]
        inverse = lax.rsqrt(total[1:2] - mean * mean + EPS)
        across = as_columns(stacked((mean, inverse), rows))
        gain = conv_gain[...]
        gain = pick(odd, gain[:, :channels], gain[:, channels:])
        normed = (conv[...] - across[:, 0:1]) * across[:, 1:2] * gain
        conv_done[...] = (normed * jax.nn.sigmoid(normed)).astype(bf16)

    piece_rows = span * (head_dim + channels) // (2 * head_dim)

    def so_many(number):
        return weights.at[: number * piece_rows, :]

    up_leaving = sends.shared(*((so_many(at + 1), z == at) for at in range(layers - 1)))
    down_leaving = sends.shared(*((so_many(layers - at), z == at) for at in range(1, layers)))
    given_leaving = sends.shared((memory_in.at[0], first), (conv_in.at[0], second))

    def spread(done, inside, semaphores, home, number):
        here, index = x == home, number // 2
        source = done.at[number * length : (number + 1) * length, :]
        part = slice(index * length, (index + 1) * length)
        target, sem = inside.at[z, part, :], semaphores.at[z, index]
        if number % 2 != home:
            sends.start(source, target, sem, x_side, here, leaving=given_leaving)
            return
        sends.start(source, target, sem, below, here, has_below, leaving=down_leaving)
        sends.start(source, target, sem, above, here, has_above, leaving=up_leaving)

        @pl.when(here)
        def _():
            inside[z, part, :] = source[...]

    for number in range(4):
        spread(conv_done, conv_in, conv_sem, 1, number)
    for number in range(2):
        send_out(number, second, far)
    send_out(2, second)

    for array in (keys,):
        arrived(array, pair_sem.at[0], first, second_core)
    for number in range(4):
        start, index, inner = number * length, number // 2, number % 2
        arrived(queries.at[start : start + length, :], query_sem.at[number], first)

        @pl.when(first)
        def _():
            width = reach[index]
            gain = memory_gain[...]
            gain = pick(odd, gain[:, :head_dim], gain[:, head_dim:])
            scores = lax.dot_general(
                queries[start : start + length, :],
                keys[:width, :],
                NT,
                preferred_element_type=f32,
            )
            scores = scores * stores[index][inner * length : (inner + 1) * length, :]
            numer = jnp.dot(scores.astype(bf16), values[:width, :], preferred_element_type=f32)
            denom = jnp.sum(scores, axis=1, keepdims=True)
            cell = numer / jnp.maximum(jnp.abs(denom), 1.0)
            memory_done[start : start + length, :] = (cell * gain).astype(bf16)
            square = as_rows((jnp.sum(cell * cell, axis=1, keepdims=True),))
            squares_done[index, inner] = square[0:1]

        spread(memory_done, memory_in, memory_sem, 0, number)

    @pl.when(first)
    def _():
        for index in range(2):
            squares_in[index * count + source_index] = squares_done[index, 0]

    for index in range(2):
        squares_leaving = sends.shared((squares_in.at[: 2 * count - 1], first))
        for z_other, y_other in sources:
            for x_other in range(2):
                away = jnp.logical_or(
                    jnp.logical_or(z != z_other, y != y_other), x != x_other
                )
                sends.start(
                    squares_done.at[index, x_other],
                    squares_in.at[index * count + source_index],
                    squares_sem.at[index],
                    (z_other * 2 + x_other, y_other * 2 + core),
                    first,
                    away,
                    leaving=squares_leaving,
                )

    order = line_order(z, layers)
    across = (1 - x) * 2 + core
    across_leaving = sends.shared((three_pieces,))

    def pass_on(distance, kind, index, *conditions):
        inside, semaphores, home = kind
        part = slice(index * length, (index + 1) * length)
        if distance == 0:
            away = x != home
            spot, sem = inside.at[z, part, :], semaphores.at[z, index]
            arrived(spot, sem, away, *conditions)
            for device, further, leaving in (
                (below, has_below, down_leaving),
                (above, has_above, up_leaving),
            ):
                sends.start(spot, spot, sem, device, away, further, *conditions, leaving=leaving)
            return
        down, up = order[2 * distance - 2 : 2 * distance]
        for (source, there, onward, further), leaving in ((down, up_leaving), (up, down_leaving)):
            spot, sem = inside.at[source, part, :], semaphores.at[source, index]
            arrived(spot, sem, there, *conditions)
            device = (onward * 2 + x, tp)
            sends.start(spot, spot, sem, device, there, further, *conditions, leaving=leaving)

    def share_out(*conditions):
        arrived(three_pieces, out_sem.at[across], *conditions)
        for spot in (memory_out.at[across], conv_out.at[across]):
            sends.start(spot, spot, out_sem.at[across], peer, *conditions, leaving=across_leaving)

    convs, memories = (conv_in, conv_sem, 1), (memory_in, memory_sem, 0)
    pass_on(0, convs, 0, first)
    pass_on(0, convs, 1, first)
    for distance in range(1, layers):
        for kind in (memories, convs):
            for index in range(2):
                if distance + 1 < layers or index == 0:
                    pass_on(distance, kind, index, first)
        if distance == layers - 2:
            share_out(first)
    for distance in range(1, layers + 2):
        if distance < layers:
            pass_on(distance, convs, 0, second)
            pass_on(distance, convs, 1, second)
        if 0 <= distance - 2 < layers - 1:
            pass_on(distance - 2, memories, 1, second)
        if 0 <= distance - 1 < layers:
            pass_on(distance - 1, memories, 0, second)
        if distance == layers - 1:
            share_out(second)
    entries = layers * 2 * head_dim
    for index in range(2):
        part = slice(index * length, (index + 1) * length)
        if index == 1:
            pass_on(layers - 1, memories, 1)
            pass_on(layers - 1, convs, 1, first)
        at = index * count
        arrived(squares_in.at[at : at + count - 1], squares_sem.at[index], first)
        arrived(squares_in.at[at : at + count], squares_sem.at[index], second)
        if index == 0:
            for group in range(2):
                arrived(three_pieces, out_sem.at[group * 2 + 1 - core])
        total = squares_in[at]
        for slot in range(1, 2 * layers):
            total = total + squares_in[at + slot]
        row_scale = stacked((lax.rsqrt(total * (1.0 / entries) + EPS),), length)
        row_scale = as_columns(row_scale)[:, 0:1]
        for group in range(2):
            from_memory, from_conv = None, None
            for head in range(layers):
                where = group * 2 + 1 - head // 2
                inner = head % 2
                memory_term = jnp.dot(
                    memory_in[head, part, :],
                    memory_out[where, inner * head_dim : (inner + 1) * head_dim, :],
                    preferred_element_type=f32,
                )
                conv_term = jnp.dot(
                    conv_in[head, part, :],
                    conv_out[where, inner * channels : (inner + 1) * channels, :],
                    preferred_element_type=f32,
                )
                from_memory = memory_term if head == 0 else from_memory + memory_term
                from_conv = conv_term if head == 0 else from_conv + conv_term
            width = from_memory.shape[1]
            partial[index, :, group * width : (group + 1) * width] = (
                from_conv + row_scale * from_memory
            ).astype(bf16)
        device = ((core * 2 + index) * 2 + x, z)
        away = jnp.logical_or(core * 2 + index != z, tp != z)
        sends.start(partial.at[index], slots.at[y], slot_sem.at[y], device, away)

        @pl.when(jnp.logical_not(away))
        def _():
            slots[y] = partial[index]

    for y_other in range(2):
        own = jnp.logical_and(tp == z, jnp.logical_and(y == y_other, core == side))
        arrived(slots.at[y_other], slot_sem.at[y_other], jnp.logical_not(own))
    sends.finish()


def layer(arrays):
    count, columns = lax.axis_size("sp"), lax.axis_size("tp")
    (
        tokens,
        conv_value_weight,
        conv_gate_weight,
        conv_kernel,
        conv_norm_gain,
        query_weight,
        key_weight,
        value_weight,
        input_gate_weight,
        forget_gate_weight,
        input_offset,
        forget_offset,
        memory_norm_gain,
        conv_out_weight,
        memory_out_weight,
    ) = arrays
    length, features = tokens.shape
    depth, head_dim = query_weight.shape[0], query_weight.shape[1] // 2
    channels = conv_value_weight.shape[1] // 2
    wide = features * columns
    rows = length * count // 2
    span = rows // 2
    layers = count // 2
    halo = -(-(conv_kernel.shape[0] - 1) // ROW_TILE) * ROW_TILE
    width = memory_out_weight.shape[1]
    f32, bf16 = jnp.float32, jnp.bfloat16
    DMA = pltpu.SemaphoreType.DMA
    V = pltpu.VMEM
    return pl.pallas_call(
        lambda *refs: layer_kernel(count, columns, *refs),
        out_shape=jax.ShapeDtypeStruct((2, length, features), bf16),
        in_specs=[pl.BlockSpec(memory_space=pltpu.HBM)] * 15,
        out_specs=IN_VMEM,
        scratch_shapes=[
            V(tokens.shape, bf16),
            V(query_weight.shape, bf16),
            V(key_weight.shape, bf16),
            V(value_weight.shape, bf16),
            V(conv_value_weight.shape, bf16),
            V(conv_gate_weight.shape, bf16),
            V((2, 2, length), f32),
            V((rows, wide), bf16),
            V((wide, 2 * head_dim), bf16),
            V((rows, 2 * head_dim), f32),
            V(conv_kernel.shape, bf16),
            V((1, 2 * channels), f32),
            V((1, 2 * head_dim), f32),
            V((2, 2, wide), bf16),
            V((4, 2, 2, length), f32),
            V((LANES, wide), f32),
            V((ROW_TILE, rows), f32),
            V((ROW_TILE, rows), f32),
            V((2 * rows, head_dim), bf16),
            V((2 * rows, head_dim), bf16),
            V((rows, head_dim), bf16),
            V((span, rows + span), f32),
            V((span, 2 * rows), f32),
            V((rows, head_dim), bf16),
            V((2, 2, 1, length), f32),
            V((2 * count, 1, length), f32),
            V((halo + rows, channels), f32),
            V((rows, channels), f32),
            V((ROW_TILE, LANES), f32),
            V((count, ROW_TILE, LANES), f32),
            V((rows, channels), bf16),
            V((layers, span, head_dim), bf16),
            V((layers, span, channels), bf16),
            V((4, 2 * head_dim, width), bf16),
            V((4, 2 * channels, width), bf16),
            V((2, length, features), bf16),
            DMA((16,)),
            DMA((SENDS,)),
            DMA((4, 2)),
            DMA((1,)),
            DMA((2, count)),
            DMA((4,)),
            DMA((1,)),
            DMA((1,)),
            DMA((1,)),
            DMA((4,)),
            DMA((1,)),
            DMA((1,)),
            DMA((2,)),
            DMA((layers, 2)),
            DMA((layers, 2)),
            DMA((4,)),
            DMA((2,)),
        ],
        compiler_params=pltpu.CompilerParams(
            collective_id=0, has_side_effects=True, vmem_limit_bytes=40 * 2**20
        ),
    )(
        *(
            pltpu.with_memory_space_constraint(array, pltpu.HBM)
            for array in (
                tokens,
                query_weight,
                key_weight,
                value_weight,
                conv_value_weight,
                conv_gate_weight,
                conv_kernel,
                conv_norm_gain.reshape(1, -1),
                memory_norm_gain.reshape(1, -1),
                input_gate_weight.T,
                forget_gate_weight.T,
                input_offset.T,
                forget_offset.T,
                memory_out_weight,
                conv_out_weight,
            )
        )
    )


def on_device_by_column(*arrays):
    slots = layer(arrays)
    return jnp.sum(slots.astype(jnp.float32), axis=0).astype(jnp.bfloat16)


def splits_by_column(mesh, tokens, query_weight, conv_value_weight, conv_kernel, input_gate_weight):
    count, columns = mesh.shape["sp"], mesh.shape["tp"]
    heads = input_gate_weight.shape[1]
    head_dim = query_weight.shape[1] // heads
    length = tokens.shape[0] // count
    return (
        count == 8
        and columns == 4
        and heads == count
        and length == LANES
        and tokens.size * 2 <= 4 * 2**20
        and conv_value_weight.shape[1] * 2 == head_dim * heads
        and head_dim == 256
        and conv_kernel.shape[0] - 1 <= length
    )


def solution(mesh):
    in_specs = (
        P("sp", "tp"),
        P("sp", "tp"),
        P("sp", "tp"),
        P(None, "tp"),
        P("tp"),
        P("sp", "tp"),
        P("sp", "tp"),
        P("sp", "tp"),
        P(None, "tp"),
        P(None, "tp"),
        P("sp", "tp"),
        P("sp", "tp"),
        P("tp"),
        P("tp", "sp"),
        P("tp", "sp"),
    )
    out_specs = P("sp", "tp")

    def run(*arrays):
        by_column = splits_by_column(
            mesh, arrays[0], arrays[5], arrays[1], arrays[3], arrays[8]
        )
        on_device = on_device_by_column if by_column else on_device_by_position
        return jax.shard_map(
            on_device, mesh=mesh, in_specs=in_specs, out_specs=out_specs, check_vma=False
        )(*arrays)

    return run
```

```python
import jax
import jax.numpy as jnp
from jax import lax
from jax.experimental import pallas as pl
from jax.experimental.pallas import tpu as pltpu
from jax.sharding import PartitionSpec as P

BLOCK = 64


EPS = 1e-06
LOWEST_LEVEL = -1e30


def shifted_2(value, axis, steps):
    count = lax.axis_size(axis)
    leading, last = (max(0, -steps), min(count, count - steps))
    return lax.ppermute(value, axis, [(source, source + steps) for source in range(leading, last)])


def carried_in(shard, axis, join, neutral):
    place = lax.axis_index(axis)
    gathered = jax.tree.map(
        lambda a, kind: lax.all_gather(a.astype(kind), axis),
        shard,
        (jnp.bfloat16, jnp.bfloat16, jnp.bfloat16, jnp.bfloat16),
    )
    state = jax.tree.map(lambda a, e: jnp.zeros_like(a) + jnp.asarray(e, a.dtype), shard, neutral)

    def one(step, state):
        return join(
            state,
            jax.tree.map(
                lambda a, own: lax.dynamic_index_in_dim(a, step, 0, False).astype(own.dtype),
                gathered,
                shard,
            ),
        )

    return lax.fori_loop(0, place, one, state)


def block_step(carry, inputs):
    state, normal, level = carry
    query, key, value, gate_in, forget_log = inputs
    length = gate_in.shape[-1]
    scale = query.shape[-1] ** (-0.5)
    causal = jnp.tril(jnp.ones((length, length), dtype=bool))
    within = jnp.cumsum(forget_log, axis=-1)
    log_weight = within[:, :, None] - within[:, None, :] + gate_in[:, None, :]
    log_weight = jnp.where(causal, log_weight, -jnp.inf)
    carried = within + level[:, None]
    top = jnp.maximum(carried, jnp.max(log_weight, axis=-1))
    weight = jnp.exp(log_weight - top[:, :, None])
    carried_weight = jnp.exp(carried - top) * scale
    scores = jnp.einsum("htd,hsd->hts", query, key, preferred_element_type=jnp.float32) * (
        scale * weight
    )
    numer = jnp.einsum(
        "hts,hse->hte", scores.astype(jnp.bfloat16), value, preferred_element_type=jnp.float32
    )
    numer = numer + carried_weight[:, :, None] * jnp.einsum(
        "hed,htd->hte", state.astype(jnp.bfloat16), query, preferred_element_type=jnp.float32
    )
    denom = jnp.sum(scores, axis=-1) + carried_weight * jnp.einsum(
        "hd,htd->ht", normal.astype(jnp.bfloat16), query, preferred_element_type=jnp.float32
    )
    result = numer / jnp.maximum(jnp.abs(denom), 1.0)[:, :, None]
    last = within[:, -1]
    end_log = last[:, None] - within + gate_in
    new_level = jnp.maximum(last + level, jnp.max(end_log, axis=-1))
    keep = jnp.exp(last + level - new_level)
    fresh = jnp.exp(end_log - new_level[:, None])
    scaled_key = (fresh[:, :, None] * key).astype(jnp.bfloat16)
    new_state = keep[:, None, None] * state + jnp.einsum(
        "hse,hsd->hed", value, scaled_key, preferred_element_type=jnp.float32
    )
    new_normal = keep[:, None] * normal + jnp.sum(scaled_key.astype(jnp.float32), axis=1)
    return ((new_state, new_normal, new_level), result)


def depthwise(extended, kernel):
    taps = kernel.shape[0]
    length = extended.shape[0] - taps + 1
    total = extended[0:length] * kernel[0]
    for index in range(1, taps):
        total = total + extended[index : index + length] * kernel[index]
    return total


def merge_states(first, second):
    first_state, first_normal, first_level, first_total = first
    second_state, second_normal, second_level, second_total = second
    shifted = first_level + second_total
    level = jnp.maximum(shifted, second_level)
    older = jnp.exp(shifted - level)
    newer = jnp.exp(second_level - level)
    state = older[:, None, None] * first_state + newer[:, None, None] * second_state
    normal = older[:, None] * first_normal + newer[:, None] * second_normal
    return (state, normal, level, first_total + second_total)


def on_device_by_position(
    tokens,
    conv_value_weight,
    conv_gate_weight,
    conv_kernel,
    conv_norm_gain,
    query_weight,
    key_weight,
    value_weight,
    input_gate_weight,
    forget_gate_weight,
    input_offset,
    forget_offset,
    memory_norm_gain,
    conv_out_weight,
    memory_out_weight,
):
    length = tokens.shape[0]
    heads_here = input_gate_weight.shape[1]
    whole = lax.all_gather(tokens, "tp", axis=1, tiled=True)
    pieces = (
        lax.all_gather(conv_value_weight, "sp", axis=0, tiled=True),
        lax.all_gather(conv_gate_weight, "sp", axis=0, tiled=True),
        lax.all_gather(query_weight, "sp", axis=0, tiled=True),
        lax.all_gather(key_weight, "sp", axis=0, tiled=True),
        lax.all_gather(value_weight, "sp", axis=0, tiled=True),
    )
    folded = tuple((jnp.dot(whole, piece, preferred_element_type=jnp.float32) for piece in pieces))
    conv_value, conv_gate, query_flat, key_flat, value_flat = folded
    gate_pre = jnp.dot(whole, input_gate_weight, preferred_element_type=jnp.float32)
    forget_pre = jnp.dot(whole, forget_gate_weight, preferred_element_type=jnp.float32)
    glu = (conv_value * jax.nn.sigmoid(conv_gate)).astype(jnp.bfloat16)
    taps = conv_kernel.shape[0]
    head_dim = query_flat.shape[1] // heads_here

    def to_heads(flat):
        return flat.astype(jnp.bfloat16).reshape(length, heads_here, head_dim).transpose(1, 0, 2)

    query = to_heads(query_flat)
    key = to_heads(key_flat)
    value = to_heads(value_flat)
    gate_in = (gate_pre + input_offset).T
    forget_log = jax.nn.log_sigmoid(forget_pre + forget_offset).T
    within = jnp.cumsum(forget_log, axis=1)
    total = within[:, -1]
    end_log = total[:, None] - within + gate_in
    local_level = jnp.max(end_log, axis=1)
    fresh = jnp.exp(end_log - local_level[:, None])
    scaled_key = (fresh[:, :, None] * key).astype(jnp.bfloat16)
    local_state = jnp.einsum("hse,hsd->hed", value, scaled_key, preferred_element_type=jnp.float32)
    local_normal = jnp.sum(scaled_key.astype(jnp.float32), axis=1)
    blank_state = (
        jnp.zeros_like(local_state),
        jnp.zeros_like(local_normal),
        jnp.full_like(local_level, LOWEST_LEVEL),
        jnp.zeros_like(total),
    )
    prior = shifted_2(glu[length - (taps - 1) :], "sp", 1)
    incoming = carried_in(
        (local_state, local_normal, local_level, total), "sp", merge_states, blank_state
    )
    extended = jnp.concatenate([prior, glu], axis=0).astype(jnp.float32)
    conv = depthwise(extended, conv_kernel.astype(jnp.float32))
    blocks = length // BLOCK

    def split(array):
        return jnp.moveaxis(array.reshape((heads_here, blocks, BLOCK) + array.shape[2:]), 1, 0)

    _, hidden = lax.scan(
        block_step,
        tuple(incoming[:3]),
        (split(query), split(key), split(value), split(gate_in), split(forget_log)),
    )
    hidden = jnp.moveaxis(hidden, 0, 1).reshape(heads_here, length, head_dim)
    hidden_squares = jnp.sum(hidden * hidden, axis=(0, 2))
    channel_sum, channel_squares, memory_squares = lax.psum(
        (jnp.sum(conv, axis=1), jnp.sum(conv * conv, axis=1), hidden_squares), "tp"
    )
    channels = conv.shape[1] * lax.axis_size("tp")
    mean = (channel_sum / channels)[:, None]
    variance = (channel_squares / channels)[:, None] - mean * mean
    conv_branch = jax.nn.silu((conv - mean) * lax.rsqrt(variance + EPS) * conv_norm_gain).astype(
        jnp.bfloat16
    )
    entries = heads_here * head_dim * lax.axis_size("tp")
    memory_scale = lax.rsqrt(memory_squares / entries + EPS)
    hidden = hidden * memory_scale[None, :, None]
    hidden = hidden * memory_norm_gain.reshape(heads_here, 1, head_dim)
    memory_branch = (
        hidden.transpose(1, 0, 2).reshape(length, heads_here * head_dim).astype(jnp.bfloat16)
    )
    conv_columns, memory_columns = (
        lax.all_gather(conv_out_weight, "sp", axis=1, tiled=True),
        lax.all_gather(memory_out_weight, "sp", axis=1, tiled=True),
    )
    contract = (((0,), (1,)), ((), ()))
    summed = lax.psum_scatter(
        (
            lax.dot_general(conv_columns, conv_branch, contract, preferred_element_type=jnp.float32)
            + lax.dot_general(
                memory_columns, memory_branch, contract, preferred_element_type=jnp.float32
            )
        ).astype(jnp.bfloat16),
        "tp",
        scatter_dimension=0,
        tiled=True,
    ).astype(jnp.float32)
    return summed.T.astype(jnp.bfloat16)


MESH = pl.DeviceIdType.MESH
IN_VMEM = pl.BlockSpec(memory_space=pltpu.VMEM)
SENDS = 30
ROW_TILE = 8
LANES = 128
NT = (((1,), (1,)), ((), ()))


def when(conditions, action):
    if not conditions:
        action()
        return
    every = conditions[0]
    for condition in conditions[1:]:
        every = jnp.logical_and(every, condition)
    pl.when(every)(action)


class Sends:
    def __init__(self, semaphores):
        self.semaphores = semaphores
        self.waits = []
        self.used = 0

    def shared(self, *waits):
        semaphore = self.semaphores.at[self.used]
        self.used += 1
        for whole, *conditions in waits:
            self.waits.append((whole, semaphore, conditions))
        return semaphore

    def start(self, source, target, arrival, device, *conditions, leaving=None):
        if leaving is None:
            leaving = self.shared((source, *conditions))
        copy = pltpu.make_async_remote_copy(
            src_ref=source,
            dst_ref=target,
            send_sem=leaving,
            recv_sem=arrival,
            device_id=device,
            device_id_type=MESH,
        )
        when(conditions, copy.start)

    def finish(self):
        for whole, semaphore, conditions in self.waits:
            when(conditions, waiting(whole, semaphore).wait_send)


def waiting(block, semaphore):
    return pltpu.make_async_remote_copy(
        src_ref=block,
        dst_ref=block,
        send_sem=semaphore,
        recv_sem=semaphore,
        device_id=(lax.axis_index("sp"), lax.axis_index("tp")),
        device_id_type=MESH,
    )


def arrived(block, semaphore, *conditions):
    copy = waiting(block, semaphore)
    when(conditions, copy.wait_recv)


def line_order(here, count):
    order = []
    for distance in range(1, count):
        order.append((here - distance, here >= distance, here + 1, here + 1 < count))
        order.append((here + distance, here + distance < count, here - 1, here > 0))
    return order


def pick(index, first, second):
    return jnp.where(jnp.full(first.shape, index, jnp.int32) == 1, second, first)


def stacked(rows, length):
    place = lax.broadcasted_iota(jnp.int32, (ROW_TILE, length), 0)
    result = jnp.zeros((ROW_TILE, length), jnp.float32)
    for index, row in enumerate(rows):
        result = jnp.where(place == index, row, result)
    return result


def as_columns(rows):
    length = rows.shape[1]
    rest = jnp.zeros((LANES - ROW_TILE, length), jnp.float32)
    return jnp.concatenate([rows, rest], axis=0).T


def as_rows(columns):
    length = columns[0].shape[0]
    place = lax.broadcasted_iota(jnp.int32, (length, LANES), 1)
    result = jnp.zeros((length, LANES), jnp.float32)
    for index, column in enumerate(columns):
        result = jnp.where(place == index, column, result)
    return result.T[:ROW_TILE]


def prefix_sums(rows):
    before = lax.broadcasted_iota(jnp.int32, (LANES, LANES), 0)
    after = lax.broadcasted_iota(jnp.int32, (LANES, LANES), 1)
    upper = (before <= after).astype(jnp.float32)
    carry = jnp.zeros((ROW_TILE, 1), jnp.float32)
    parts = []
    for start in range(0, rows.shape[1], LANES):
        part = carry + jnp.dot(
            rows[:, start : start + LANES],
            upper,
            precision=lax.Precision.HIGHEST,
            preferred_element_type=jnp.float32,
        )
        carry = part[:, LANES - 1 :]
        parts.append(part)
    return jnp.concatenate(parts, axis=1)


def layer_kernel(
    count,
    columns,
    all_tokens,
    all_wq,
    all_wk,
    all_wv,
    all_wcv,
    all_wcg,
    own_taps,
    own_conv_gain,
    own_memory_gain,
    own_input_gates,
    own_forget_gates,
    own_input_offsets,
    own_forget_offsets,
    own_memory_out,
    own_conv_out,
    slots,
    tokens,
    wq,
    wk,
    wv,
    wcv,
    wcg,
    shifts,
    lines,
    weights,
    product,
    taps,
    conv_gain,
    memory_gain,
    gate_weights,
    offsets,
    gate_rows,
    level_before,
    level_here,
    keys,
    values,
    queries,
    weight_near,
    weight_far,
    memory_done,
    squares_done,
    squares_in,
    extended,
    conv,
    sums_done,
    sums_in,
    conv_done,
    memory_in,
    conv_in,
    memory_out,
    conv_out,
    partial,
    load_sem,
    send_sem,
    token_sem,
    y_sem,
    weight_sem,
    own_sem,
    offset_sem,
    level_sem,
    pair_sem,
    query_sem,
    halo_sem,
    sums_sem,
    squares_sem,
    memory_sem,
    conv_sem,
    out_sem,
    slot_sem,
):
    f32, bf16 = jnp.float32, jnp.bfloat16
    me, tp = lax.axis_index("sp"), lax.axis_index("tp")
    layers = count // 2
    z, x, y, core = me // 2, lax.rem(me, 2), tp // 2, lax.rem(tp, 2)
    side, odd = z // 2, lax.rem(z, 2)
    length, features = tokens.shape
    depth, head_dim = wq.shape[0], wq.shape[1] // 2
    channels = wcv.shape[1] // 2
    rows = 4 * length
    span = rows // 2
    near, far = core == side, core != side
    first, second = x == 0, x == 1
    middle = jnp.logical_or(z == 1, z == 2)
    ends = jnp.logical_not(middle)
    peer = (me, y * 2 + 1 - core)
    below, above = (me - 2, tp), (me + 2, tp)
    x_side = (z * 2 + 1 - x, tp)
    y_side = (me, (1 - y) * 2 + core)
    has_below, has_above = z > 0, z + 1 < layers
    sends = Sends(send_sem)

    barrier = pltpu.get_barrier_semaphore()
    devices = count * columns
    rank = me * columns + tp
    for step in range(1, devices):
        other = lax.rem(rank + step, devices)
        pl.semaphore_signal(
            barrier,
            inc=1,
            device_id=(other // columns, lax.rem(other, columns)),
            device_id_type=MESH,
        )

    def block(i, j):
        return lines.at[
            pl.ds(pl.multiple_of(i * length, length), length),
            pl.ds(pl.multiple_of(j * features, features), features),
        ]

    def blocks(number):
        return lines.at[: number * length // columns, :]

    place = odd * 2 + x
    own_part = x * 2 + core
    loads = []
    for source, target, *conditions in (
        (all_tokens, tokens),
        (all_tokens, block(place, tp), near),
        (all_wq, wq),
        (all_wk, wk),
        (all_wv, wv),
        (all_wcv, wcv),
        (all_wcg, wcg),
        (own_input_offsets, shifts.at[0]),
        (own_forget_offsets, shifts.at[1]),
        (own_taps, taps, far),
        (own_conv_gain, conv_gain, far),
        (own_memory_gain, memory_gain, far),
        (own_input_gates, gate_weights.at[0], far),
        (own_forget_gates, gate_weights.at[1], far),
        (own_memory_out, memory_out.at[own_part]),
        (own_conv_out, conv_out.at[own_part]),
    ):
        copy = pltpu.make_async_copy(source, target, load_sem.at[len(loads)])
        loads.append((copy, conditions))
        when(conditions, copy.start)

    def loaded(first_load, last_load):
        for copy, conditions in loads[first_load:last_load]:
            when(conditions, copy.wait)

    loaded(0, 2)
    pl.semaphore_wait(barrier, devices - 1)

    goal = y * 2 + side
    mine, mine_sem = block(place, tp), token_sem.at[place, core]
    z_leaving = sends.shared(
        (blocks(1), ends), (blocks(4), middle, near), (blocks(6), middle, far)
    )
    x_leaving = sends.shared((blocks(3), near), (blocks(5), far))
    y_leaving = sends.shared((blocks(7), near), (blocks(9), far))
    sends.start(tokens, mine, mine_sem, (me - 2, goal), has_below, leaving=z_leaving)
    sends.start(tokens, mine, mine_sem, (me + 2, goal), has_above, leaving=z_leaving)
    sends.start(tokens, mine, mine_sem, (z * 2 + 1 - x, goal), leaving=x_leaving)
    sends.start(tokens, mine, y_sem.at[0], (me, (1 - y) * 2 + side), leaving=y_leaving)
    sends.start(tokens, mine, mine_sem, peer, far)

    def piece(unit, i):
        return weights.at[
            pl.ds(pl.multiple_of(i * depth, depth), depth),
            unit * head_dim : (unit + 1) * head_dim,
        ]

    def shares(k, x_goal):
        whole = pl.ds(pl.multiple_of(k * head_dim, head_dim), head_dim)
        part = pl.ds(pl.multiple_of(k * channels, channels), channels)
        if x_goal == 0:
            return (
                (wk.at[:, whole], 0, 0, head_dim),
                (wv.at[:, whole], 1, head_dim, head_dim),
            )
        return (
            (wq.at[:, whole], 0, 0, head_dim),
            (wcv.at[:, part], 1, head_dim, channels),
            (wcg.at[:, part], 1, head_dim + channels, channels),
        )

    own_rows = pl.ds(pl.multiple_of(me * depth, depth), depth)
    z_first = (1 - core) * 2
    share = weights.at[:depth, :]

    def send_weights(k, cross, leaving, *conditions, to_peer=False):
        for x_goal in range(2):
            chosen = conditions + ((x != x_goal) if cross else (x == x_goal),)
            for source, unit, start, size in shares(k, x_goal):
                device = peer if to_peer else ((z_first + k) * 2 + x_goal, y * 2 + unit)
                target = weights.at[own_rows, start : start + size]
                sends.start(
                    source, target, weight_sem.at[unit, me], device, *chosen, leaving=leaving
                )

    loaded(2, len(loads))
    mate_leaving, other_leaving = sends.shared((share,)), sends.shared((share,))
    send_weights(odd, False, other_leaving, far, to_peer=True)
    send_weights(1 - odd, False, mate_leaving, far)
    for x_goal in range(2):

        def keep():
            for source, _, start, size in shares(odd, x_goal):
                weights[own_rows, start : start + size] = source[...]

        when((far, x == x_goal), keep)

    own_arrays = (taps, conv_gain, memory_gain, gate_weights)
    for index, array in enumerate(own_arrays):
        sends.start(array, array, own_sem.at[index], peer, far)
    leaving = sends.shared((offsets.at[:2],))
    for k in range(2):
        device = ((z_first + k) * 2, y * 2 + side)
        sends.start(shifts, offsets.at[place], offset_sem.at[0], device, leaving=leaving)

    half_rows = memory_out.shape[1] // 2
    out_width = memory_out.shape[2]
    three_pieces = weights.at[: 3 * half_rows * out_width // (2 * head_dim), :]

    def out_piece(part, number):
        if number == 1:
            return conv_out.at[part]
        start = half_rows * (number // 2)
        return memory_out.at[part, start : start + half_rows, :]

    out_leaving = [sends.shared((three_pieces,)) for _ in range(2)]

    def send_out(number, *conditions):
        spot = out_piece(own_part, number)
        for device, leaving in zip((x_side, peer), out_leaving):
            sends.start(spot, spot, out_sem.at[own_part], device, *conditions, leaving=leaving)

    k_near = jnp.where(near, odd, 1 - core)
    groups = []
    for k in (k_near, 1 - k_near):
        source = core * 2 + k
        groups.append((source, k * 2 + x, k * 2 + 1 - x))
    for source, i, _ in groups:
        away, up = source != z, source < z
        onward = (jnp.where(up, z + 1, z - 1) * 2 + x, tp)
        for j in range(2):
            spot, sem = block(i, y * 2 + j), token_sem.at[i, j]
            arrived(spot, sem, jnp.logical_or(away, j != core))
            sends.start(spot, spot, sem, onward, away, middle, leaving=z_leaving)
            sends.start(spot, spot, sem, x_side, away, leaving=x_leaving)
            sends.start(spot, spot, y_sem.at[0], y_side, away, leaving=y_leaving)
    cross_leaving = [sends.shared((share,)) for _ in range(2)]
    send_weights(side, False, mate_leaving, near, middle)
    send_weights(odd, True, cross_leaving[1], far)
    send_weights(1 - odd, True, cross_leaving[0], far, ends)
    for _, _, i in groups:
        for j in range(2):
            spot, sem = block(i, y * 2 + j), token_sem.at[i, j]
            arrived(spot, sem)
            sends.start(spot, spot, y_sem.at[0], y_side, leaving=y_leaving)

    send_weights(side, False, mate_leaving, near, ends)
    last = jnp.logical_and(middle, first)
    send_weights(1 - side, False, other_leaving, near, jnp.logical_not(last))
    k_cross = jnp.where(near, 1 - side, 1 - odd)
    send_weights(k_cross, True, cross_leaving[0], jnp.logical_or(near, middle))
    send_weights(side, True, cross_leaving[1], near)
    send_weights(1 - side, False, other_leaving, near, last)
    for number in range(2):
        send_out(number, near, second)

    arrived(blocks(8), y_sem.at[0])
    for index, array in enumerate(own_arrays):
        arrived(array, own_sem.at[index], near)
    arrived(offsets, offset_sem.at[0], first)

    @pl.when(first)
    def _():
        gate_rows[...] = jnp.zeros_like(gate_rows)
        gate_rows[0:2, :] = gate_weights[0].astype(f32)
        gate_rows[2:4, :] = gate_weights[1].astype(f32)
        gates = lax.dot_general(
            lines[...], gate_rows[...].astype(bf16), NT, preferred_element_type=f32
        ).T
        shift = [jnp.concatenate([offsets[i, kind] for i in range(4)], 1) for kind in range(2)]
        gate_in = pick(odd, gates[0:1] + shift[0][0:1], gates[1:2] + shift[0][1:2])
        forget = pick(odd, gates[2:3] + shift[1][0:1], gates[3:4] + shift[1][1:2])
        forget_log = jnp.minimum(forget, 0.0) - jnp.log1p(jnp.exp(-jnp.abs(forget)))
        coarse = jnp.round(forget_log * 8.0) * 0.125
        within = prefix_sums(stacked((coarse, forget_log - coarse), rows))
        which = lax.broadcasted_iota(jnp.int32, (ROW_TILE, rows), 0)
        level_here[...] = jnp.where(which == 2, gate_in, within)

    first_core, second_core = core == 0, core == 1
    sends.start(level_here, level_before, level_sem.at[0], peer, first, first_core)

    @pl.when(jnp.logical_and(first, first_core))
    def _():
        level_before[...] = jnp.zeros_like(level_before)
        keys[:rows, :] = jnp.zeros_like(keys[:rows, :])
        values[:rows, :] = jnp.zeros_like(values[:rows, :])

    scale = head_dim ** (-0.5)
    reach = (rows + span, 2 * rows)
    stores = (weight_near, weight_far)

    def position_weights():
        before = level_before[...]
        which = lax.broadcasted_iota(jnp.int32, (ROW_TILE, rows), 0)
        here = level_here[...] + jnp.where(which < 2, before[:, rows - 1 :], 0.0)
        from_rows = jnp.concatenate([before, here], axis=1)
        to_columns = as_columns(here)
        tile = 64
        for start in range(0, rows, tile):
            index = start // span
            width = reach[index]
            to = to_columns[start : start + tile]
            log_weight = (
                (to[:, 0:1] - from_rows[0:1, :width])
                + (to[:, 1:2] - from_rows[1:2, :width])
                + from_rows[2:3, :width]
            )
            at = lax.broadcasted_iota(jnp.int32, (tile, width), 1)
            until = lax.broadcasted_iota(jnp.int32, (tile, width), 0) + (start + rows)
            seen = jnp.logical_and(at <= until, at >= rows * (1 - core))
            log_weight = jnp.where(seen, log_weight, -jnp.inf)
            weight = jnp.exp(log_weight - jnp.max(log_weight, axis=1, keepdims=True)) * scale
            stores[index][start - index * span : start - index * span + tile, :] = weight

    forward_leaving = sends.shared((weights.at[: 7 * depth // 2, :],))

    def own_unit(i):
        for unit in range(2):
            spot, sem = piece(unit, i), weight_sem.at[unit, i]
            arrived(spot, sem, core == unit)
            sends.start(spot, spot, sem, peer, core == unit, leaving=forward_leaving)

    def other_unit(i):
        for unit in range(2):
            arrived(piece(unit, i), weight_sem.at[unit, i], core != unit)

    def multiply(start, size):
        part = pl.ds(pl.multiple_of(start, size), size)
        return jnp.dot(lines[:, part], weights[part, :], preferred_element_type=f32)

    z_mate = side * 2 + 1 - odd
    z_far = (jnp.where(side == 0, 3, 0), jnp.where(side == 0, 2, 1))
    own_unit(z_mate * 2 + x)
    own_unit(z_far[0] * 2 + x)
    arrived(level_before, level_sem.at[0], first, second_core)
    when((first,), position_weights)
    for i in (z * 2 + 1 - x, z_mate * 2 + 1 - x):
        own_unit(i)
    for i in (z_mate * 2 + x, z * 2 + 1 - x, z_mate * 2 + 1 - x):
        other_unit(i)
    for unit in range(2):
        arrived(piece(unit, me), weight_sem.at[unit, me], near)
    half = count // 2 * depth
    product[...] = multiply(side * half, half)
    own_unit(z_far[0] * 2 + 1 - x)
    own_unit(z_far[1] * 2 + x)
    own_unit(z_far[1] * 2 + 1 - x)
    for pair in z_far:
        other_unit(pair * 2)
        other_unit(pair * 2 + 1)
        product[...] += multiply(pair * 2 * depth, 2 * depth)

    for number in range(2):
        send_out(number, first, near)

    @pl.when(second)
    def _():
        queries[...] = product[:, :head_dim].astype(bf16)

    leaving = sends.shared((queries, second))
    for number in range(4):
        part = queries.at[number * length : (number + 1) * length, :]
        sends.start(part, part, query_sem.at[number], x_side, second, leaving=leaving)

    @pl.when(first)
    def _():
        keys[rows:, :] = product[:, :head_dim].astype(bf16)
        values[rows:, :] = product[:, head_dim:].astype(bf16)

    leaving = sends.shared((keys, first, first_core))
    for array in (keys, values):
        sends.start(
            array.at[rows:, :],
            array.at[:rows, :],
            pair_sem.at[0],
            peer,
            first,
            first_core,
            leaving=leaving,
        )

    halo = extended.shape[0] - rows

    @pl.when(second)
    def _():
        gated = product[:, head_dim : head_dim + channels] * jax.nn.sigmoid(
            product[:, head_dim + channels :]
        )
        extended[halo:, :] = gated.astype(bf16).astype(f32)

    sends.start(
        extended.at[rows:, :], extended.at[:halo, :], halo_sem.at[0], peer, second, first_core
    )

    @pl.when(jnp.logical_and(second, first_core))
    def _():
        extended[:halo, :] = jnp.zeros((halo, channels), f32)

    arrived(extended.at[:halo, :], halo_sem.at[0], second, second_core)
    source_index = y * layers + z

    @pl.when(second)
    def _():
        number = taps.shape[0]
        kernel = taps[...].astype(f32)
        kernel = pick(odd, kernel[:, :channels], kernel[:, channels:])
        for start in range(0, rows, length):
            base = start + halo - (number - 1)
            total = extended[base : base + length, :] * kernel[0:1]
            for index in range(1, number):
                total = total + (
                    extended[base + index : base + index + length, :] * kernel[index : index + 1]
                )
            conv[start : start + length, :] = total
        all_rows = conv[...]
        both = as_rows(
            (
                jnp.sum(all_rows, axis=1, keepdims=True),
                jnp.sum(all_rows * all_rows, axis=1, keepdims=True),
            )
        )
        sums_done[...] = jnp.concatenate(
            [both[:2, start : start + LANES] for start in range(0, rows, LANES)], axis=0
        )
        sums_in[source_index] = sums_done[...]

    sources = [(z_other, y_other) for z_other in range(layers) for y_other in range(2)]
    others = sums_in.at[: count - 1]
    leaving = sends.shared((others, second))
    for z_other, y_other in sources:
        away = jnp.logical_or(z != z_other, y != y_other)
        device = (z_other * 2 + 1, y_other * 2 + core)
        sends.start(
            sums_done,
            sums_in.at[source_index],
            sums_sem.at[0],
            device,
            second,
            away,
            leaving=leaving,
        )
    arrived(others, sums_sem.at[0], second)

    @pl.when(second)
    def _():
        total = sums_in[0]
        for index in range(1, 2 * layers):
            total = total + sums_in[index]
        total = total * (1.0 / (2 * layers * channels))
        total = jnp.concatenate([total[at : at + 2] for at in range(0, ROW_TILE, 2)], axis=1)
        mean = total[0:1]
        inverse = lax.rsqrt(total[1:2] - mean * mean + EPS)
        across = as_columns(stacked((mean, inverse), rows))
        gain = conv_gain[...]
        gain = pick(odd, gain[:, :channels], gain[:, channels:])
        normed = (conv[...] - across[:, 0:1]) * across[:, 1:2] * gain
        conv_done[...] = (normed * jax.nn.sigmoid(normed)).astype(bf16)

    piece_rows = span * (head_dim + channels) // (2 * head_dim)

    def so_many(number):
        return weights.at[: number * piece_rows, :]

    up_leaving = sends.shared(*((so_many(at + 1), z == at) for at in range(layers - 1)))
    down_leaving = sends.shared(*((so_many(layers - at), z == at) for at in range(1, layers)))
    given_leaving = sends.shared((memory_in.at[0], first), (conv_in.at[0], second))

    def spread(done, inside, semaphores, home, number):
        here, index = x == home, number // 2
        source = done.at[number * length : (number + 1) * length, :]
        part = slice(index * length, (index + 1) * length)
        target, sem = inside.at[z, part, :], semaphores.at[z, index]
        if number % 2 != home:
            sends.start(source, target, sem, x_side, here, leaving=given_leaving)
            return
        sends.start(source, target, sem, below, here, has_below, leaving=down_leaving)
        sends.start(source, target, sem, above, here, has_above, leaving=up_leaving)

        @pl.when(here)
        def _():
            inside[z, part, :] = source[...]

    for number in range(4):
        spread(conv_done, conv_in, conv_sem, 1, number)
    for number in range(2):
        send_out(number, second, far)
    send_out(2, second)

    for array in (keys,):
        arrived(array, pair_sem.at[0], first, second_core)
    for number in range(4):
        start, index, inner = number * length, number // 2, number % 2
        arrived(queries.at[start : start + length, :], query_sem.at[number], first)

        @pl.when(first)
        def _():
            width = reach[index]
            gain = memory_gain[...]
            gain = pick(odd, gain[:, :head_dim], gain[:, head_dim:])
            scores = lax.dot_general(
                queries[start : start + length, :],
                keys[:width, :],
                NT,
                preferred_element_type=f32,
            )
            scores = scores * stores[index][inner * length : (inner + 1) * length, :]
            numer = jnp.dot(scores.astype(bf16), values[:width, :], preferred_element_type=f32)
            denom = jnp.sum(scores, axis=1, keepdims=True)
            cell = numer / jnp.maximum(jnp.abs(denom), 1.0)
            memory_done[start : start + length, :] = (cell * gain).astype(bf16)
            square = as_rows((jnp.sum(cell * cell, axis=1, keepdims=True),))
            squares_done[index, inner] = square[0:1]

        spread(memory_done, memory_in, memory_sem, 0, number)
    for number in range(2):
        send_out(number, first, far)
    send_out(2, first)

    @pl.when(first)
    def _():
        for index in range(2):
            squares_in[index * count + source_index] = squares_done[index, 0]

    for index in range(2):
        squares_leaving = sends.shared((squares_in.at[: 2 * count - 1], first))
        for z_other, y_other in sources:
            for x_other in range(2):
                away = jnp.logical_or(
                    jnp.logical_or(z != z_other, y != y_other), x != x_other
                )
                sends.start(
                    squares_done.at[index, x_other],
                    squares_in.at[index * count + source_index],
                    squares_sem.at[index],
                    (z_other * 2 + x_other, y_other * 2 + core),
                    first,
                    away,
                    leaving=squares_leaving,
                )

    order = line_order(z, layers)
    across = (1 - x) * 2 + core
    across_leaving = sends.shared((three_pieces,))

    def pass_on(distance, kind, index, *conditions):
        inside, semaphores, home = kind
        part = slice(index * length, (index + 1) * length)
        if distance == 0:
            away = x != home
            spot, sem = inside.at[z, part, :], semaphores.at[z, index]
            arrived(spot, sem, away, *conditions)
            for device, further, leaving in (
                (below, has_below, down_leaving),
                (above, has_above, up_leaving),
            ):
                sends.start(spot, spot, sem, device, away, further, *conditions, leaving=leaving)
            return
        down, up = order[2 * distance - 2 : 2 * distance]
        for (source, there, onward, further), leaving in ((down, up_leaving), (up, down_leaving)):
            spot, sem = inside.at[source, part, :], semaphores.at[source, index]
            arrived(spot, sem, there, *conditions)
            device = (onward * 2 + x, tp)
            sends.start(spot, spot, sem, device, there, further, *conditions, leaving=leaving)

    def share_out(*conditions):
        arrived(three_pieces, out_sem.at[across], *conditions)
        for spot in (memory_out.at[across], conv_out.at[across]):
            sends.start(spot, spot, out_sem.at[across], peer, *conditions, leaving=across_leaving)

    convs, memories = (conv_in, conv_sem, 1), (memory_in, memory_sem, 0)
    pass_on(0, convs, 0, first)
    pass_on(0, convs, 1, first)
    for distance in range(1, layers):
        for kind in (memories, convs):
            for index in range(2):
                if distance + 1 < layers or index == 0:
                    pass_on(distance, kind, index, first)
        if distance == layers - 2:
            share_out(first)
    for distance in range(1, layers + 2):
        if distance < layers:
            pass_on(distance, convs, 0, second)
            pass_on(distance, convs, 1, second)
        if 0 <= distance - 2 < layers - 1:
            pass_on(distance - 2, memories, 1, second)
        if 0 <= distance - 1 < layers:
            pass_on(distance - 1, memories, 0, second)
        if distance == layers - 1:
            share_out(second)
    entries = layers * 2 * head_dim
    for index in range(2):
        part = slice(index * length, (index + 1) * length)
        if index == 1:
            pass_on(layers - 1, memories, 1)
            pass_on(layers - 1, convs, 1, first)
        at = index * count
        arrived(squares_in.at[at : at + count - 1], squares_sem.at[index], first)
        arrived(squares_in.at[at : at + count], squares_sem.at[index], second)
        if index == 0:
            for group in range(2):
                arrived(three_pieces, out_sem.at[group * 2 + 1 - core])
        total = squares_in[at]
        for slot in range(1, 2 * layers):
            total = total + squares_in[at + slot]
        row_scale = stacked((lax.rsqrt(total * (1.0 / entries) + EPS),), length)
        row_scale = as_columns(row_scale)[:, 0:1]
        for group in range(2):
            from_memory, from_conv = None, None
            for head in range(layers):
                where = group * 2 + 1 - head // 2
                inner = head % 2
                memory_term = jnp.dot(
                    memory_in[head, part, :],
                    memory_out[where, inner * head_dim : (inner + 1) * head_dim, :],
                    preferred_element_type=f32,
                )
                conv_term = jnp.dot(
                    conv_in[head, part, :],
                    conv_out[where, inner * channels : (inner + 1) * channels, :],
                    preferred_element_type=f32,
                )
                from_memory = memory_term if head == 0 else from_memory + memory_term
                from_conv = conv_term if head == 0 else from_conv + conv_term
            width = from_memory.shape[1]
            partial[index, :, group * width : (group + 1) * width] = (
                from_conv + row_scale * from_memory
            ).astype(bf16)
        device = ((core * 2 + index) * 2 + x, z)
        away = jnp.logical_or(core * 2 + index != z, tp != z)
        sends.start(partial.at[index], slots.at[y], slot_sem.at[y], device, away)

        @pl.when(jnp.logical_not(away))
        def _():
            slots[y] = partial[index]

    for y_other in range(2):
        own = jnp.logical_and(tp == z, jnp.logical_and(y == y_other, core == side))
        arrived(slots.at[y_other], slot_sem.at[y_other], jnp.logical_not(own))
    sends.finish()


def layer(arrays):
    count, columns = lax.axis_size("sp"), lax.axis_size("tp")
    (
        tokens,
        conv_value_weight,
        conv_gate_weight,
        conv_kernel,
        conv_norm_gain,
        query_weight,
        key_weight,
        value_weight,
        input_gate_weight,
        forget_gate_weight,
        input_offset,
        forget_offset,
        memory_norm_gain,
        conv_out_weight,
        memory_out_weight,
    ) = arrays
    length, features = tokens.shape
    depth, head_dim = query_weight.shape[0], query_weight.shape[1] // 2
    channels = conv_value_weight.shape[1] // 2
    wide = features * columns
    rows = length * count // 2
    span = rows // 2
    layers = count // 2
    halo = -(-(conv_kernel.shape[0] - 1) // ROW_TILE) * ROW_TILE
    width = memory_out_weight.shape[1]
    f32, bf16 = jnp.float32, jnp.bfloat16
    DMA = pltpu.SemaphoreType.DMA
    V = pltpu.VMEM
    return pl.pallas_call(
        lambda *refs: layer_kernel(count, columns, *refs),
        out_shape=jax.ShapeDtypeStruct((2, length, features), bf16),
        in_specs=[pl.BlockSpec(memory_space=pltpu.HBM)] * 15,
        out_specs=IN_VMEM,
        scratch_shapes=[
            V(tokens.shape, bf16),
            V(query_weight.shape, bf16),
            V(key_weight.shape, bf16),
            V(value_weight.shape, bf16),
            V(conv_value_weight.shape, bf16),
            V(conv_gate_weight.shape, bf16),
            V((2, 2, length), f32),
            V((rows, wide), bf16),
            V((wide, 2 * head_dim), bf16),
            V((rows, 2 * head_dim), f32),
            V(conv_kernel.shape, bf16),
            V((1, 2 * channels), f32),
            V((1, 2 * head_dim), f32),
            V((2, 2, wide), bf16),
            V((4, 2, 2, length), f32),
            V((LANES, wide), f32),
            V((ROW_TILE, rows), f32),
            V((ROW_TILE, rows), f32),
            V((2 * rows, head_dim), bf16),
            V((2 * rows, head_dim), bf16),
            V((rows, head_dim), bf16),
            V((span, rows + span), f32),
            V((span, 2 * rows), f32),
            V((rows, head_dim), bf16),
            V((2, 2, 1, length), f32),
            V((2 * count, 1, length), f32),
            V((halo + rows, channels), f32),
            V((rows, channels), f32),
            V((ROW_TILE, LANES), f32),
            V((count, ROW_TILE, LANES), f32),
            V((rows, channels), bf16),
            V((layers, span, head_dim), bf16),
            V((layers, span, channels), bf16),
            V((4, 2 * head_dim, width), bf16),
            V((4, 2 * channels, width), bf16),
            V((2, length, features), bf16),
            DMA((16,)),
            DMA((SENDS,)),
            DMA((4, 2)),
            DMA((1,)),
            DMA((2, count)),
            DMA((4,)),
            DMA((1,)),
            DMA((1,)),
            DMA((1,)),
            DMA((4,)),
            DMA((1,)),
            DMA((1,)),
            DMA((2,)),
            DMA((layers, 2)),
            DMA((layers, 2)),
            DMA((4,)),
            DMA((2,)),
        ],
        compiler_params=pltpu.CompilerParams(
            collective_id=0, has_side_effects=True, vmem_limit_bytes=40 * 2**20
        ),
    )(
        *(
            pltpu.with_memory_space_constraint(array, pltpu.HBM)
            for array in (
                tokens,
                query_weight,
                key_weight,
                value_weight,
                conv_value_weight,
                conv_gate_weight,
                conv_kernel,
                conv_norm_gain.reshape(1, -1),
                memory_norm_gain.reshape(1, -1),
                input_gate_weight.T,
                forget_gate_weight.T,
                input_offset.T,
                forget_offset.T,
                memory_out_weight,
                conv_out_weight,
            )
        )
    )


def on_device_by_column(*arrays):
    slots = layer(arrays)
    return jnp.sum(slots.astype(jnp.float32), axis=0).astype(jnp.bfloat16)


def splits_by_column(mesh, tokens, query_weight, conv_value_weight, conv_kernel, input_gate_weight):
    count, columns = mesh.shape["sp"], mesh.shape["tp"]
    heads = input_gate_weight.shape[1]
    head_dim = query_weight.shape[1] // heads
    length = tokens.shape[0] // count
    return (
        count == 8
        and columns == 4
        and heads == count
        and length == LANES
        and tokens.size * 2 <= 4 * 2**20
        and conv_value_weight.shape[1] * 2 == head_dim * heads
        and head_dim == 256
        and conv_kernel.shape[0] - 1 <= length
    )


def solution(mesh):
    in_specs = (
        P("sp", "tp"),
        P("sp", "tp"),
        P("sp", "tp"),
        P(None, "tp"),
        P("tp"),
        P("sp", "tp"),
        P("sp", "tp"),
        P("sp", "tp"),
        P(None, "tp"),
        P(None, "tp"),
        P("sp", "tp"),
        P("sp", "tp"),
        P("tp"),
        P("tp", "sp"),
        P("tp", "sp"),
    )
    out_specs = P("sp", "tp")

    def run(*arrays):
        by_column = splits_by_column(
            mesh, arrays[0], arrays[5], arrays[1], arrays[3], arrays[8]
        )
        on_device = on_device_by_column if by_column else on_device_by_position
        return jax.shard_map(
            on_device, mesh=mesh, in_specs=in_specs, out_specs=out_specs, check_vma=False
        )(*arrays)

    return run
```

```python
import jax
import jax.numpy as jnp
from jax import lax
from jax.experimental import pallas as pl
from jax.experimental.pallas import tpu as pltpu
from jax.sharding import PartitionSpec as P

BLOCK = 64


EPS = 1e-06
LOWEST_LEVEL = -1e30


def shifted_2(value, axis, steps):
    count = lax.axis_size(axis)
    leading, last = (max(0, -steps), min(count, count - steps))
    return lax.ppermute(value, axis, [(source, source + steps) for source in range(leading, last)])


def carried_in(shard, axis, join, neutral):
    place = lax.axis_index(axis)
    gathered = jax.tree.map(
        lambda a, kind: lax.all_gather(a.astype(kind), axis),
        shard,
        (jnp.bfloat16, jnp.bfloat16, jnp.bfloat16, jnp.bfloat16),
    )
    state = jax.tree.map(lambda a, e: jnp.zeros_like(a) + jnp.asarray(e, a.dtype), shard, neutral)

    def one(step, state):
        return join(
            state,
            jax.tree.map(
                lambda a, own: lax.dynamic_index_in_dim(a, step, 0, False).astype(own.dtype),
                gathered,
                shard,
            ),
        )

    return lax.fori_loop(0, place, one, state)


def block_step(carry, inputs):
    state, normal, level = carry
    query, key, value, gate_in, forget_log = inputs
    length = gate_in.shape[-1]
    scale = query.shape[-1] ** (-0.5)
    causal = jnp.tril(jnp.ones((length, length), dtype=bool))
    within = jnp.cumsum(forget_log, axis=-1)
    log_weight = within[:, :, None] - within[:, None, :] + gate_in[:, None, :]
    log_weight = jnp.where(causal, log_weight, -jnp.inf)
    carried = within + level[:, None]
    top = jnp.maximum(carried, jnp.max(log_weight, axis=-1))
    weight = jnp.exp(log_weight - top[:, :, None])
    carried_weight = jnp.exp(carried - top) * scale
    scores = jnp.einsum("htd,hsd->hts", query, key, preferred_element_type=jnp.float32) * (
        scale * weight
    )
    numer = jnp.einsum(
        "hts,hse->hte", scores.astype(jnp.bfloat16), value, preferred_element_type=jnp.float32
    )
    numer = numer + carried_weight[:, :, None] * jnp.einsum(
        "hed,htd->hte", state.astype(jnp.bfloat16), query, preferred_element_type=jnp.float32
    )
    denom = jnp.sum(scores, axis=-1) + carried_weight * jnp.einsum(
        "hd,htd->ht", normal.astype(jnp.bfloat16), query, preferred_element_type=jnp.float32
    )
    result = numer / jnp.maximum(jnp.abs(denom), 1.0)[:, :, None]
    last = within[:, -1]
    end_log = last[:, None] - within + gate_in
    new_level = jnp.maximum(last + level, jnp.max(end_log, axis=-1))
    keep = jnp.exp(last + level - new_level)
    fresh = jnp.exp(end_log - new_level[:, None])
    scaled_key = (fresh[:, :, None] * key).astype(jnp.bfloat16)
    new_state = keep[:, None, None] * state + jnp.einsum(
        "hse,hsd->hed", value, scaled_key, preferred_element_type=jnp.float32
    )
    new_normal = keep[:, None] * normal + jnp.sum(scaled_key.astype(jnp.float32), axis=1)
    return ((new_state, new_normal, new_level), result)


def depthwise(extended, kernel):
    taps = kernel.shape[0]
    length = extended.shape[0] - taps + 1
    total = extended[0:length] * kernel[0]
    for index in range(1, taps):
        total = total + extended[index : index + length] * kernel[index]
    return total


def merge_states(first, second):
    first_state, first_normal, first_level, first_total = first
    second_state, second_normal, second_level, second_total = second
    shifted = first_level + second_total
    level = jnp.maximum(shifted, second_level)
    older = jnp.exp(shifted - level)
    newer = jnp.exp(second_level - level)
    state = older[:, None, None] * first_state + newer[:, None, None] * second_state
    normal = older[:, None] * first_normal + newer[:, None] * second_normal
    return (state, normal, level, first_total + second_total)


def on_device_by_position(
    tokens,
    conv_value_weight,
    conv_gate_weight,
    conv_kernel,
    conv_norm_gain,
    query_weight,
    key_weight,
    value_weight,
    input_gate_weight,
    forget_gate_weight,
    input_offset,
    forget_offset,
    memory_norm_gain,
    conv_out_weight,
    memory_out_weight,
):
    length = tokens.shape[0]
    heads_here = input_gate_weight.shape[1]
    whole = lax.all_gather(tokens, "tp", axis=1, tiled=True)
    pieces = (
        lax.all_gather(conv_value_weight, "sp", axis=0, tiled=True),
        lax.all_gather(conv_gate_weight, "sp", axis=0, tiled=True),
        lax.all_gather(query_weight, "sp", axis=0, tiled=True),
        lax.all_gather(key_weight, "sp", axis=0, tiled=True),
        lax.all_gather(value_weight, "sp", axis=0, tiled=True),
    )
    folded = tuple((jnp.dot(whole, piece, preferred_element_type=jnp.float32) for piece in pieces))
    conv_value, conv_gate, query_flat, key_flat, value_flat = folded
    gate_pre = jnp.dot(whole, input_gate_weight, preferred_element_type=jnp.float32)
    forget_pre = jnp.dot(whole, forget_gate_weight, preferred_element_type=jnp.float32)
    glu = (conv_value * jax.nn.sigmoid(conv_gate)).astype(jnp.bfloat16)
    taps = conv_kernel.shape[0]
    head_dim = query_flat.shape[1] // heads_here

    def to_heads(flat):
        return flat.astype(jnp.bfloat16).reshape(length, heads_here, head_dim).transpose(1, 0, 2)

    query = to_heads(query_flat)
    key = to_heads(key_flat)
    value = to_heads(value_flat)
    gate_in = (gate_pre + input_offset).T
    forget_log = jax.nn.log_sigmoid(forget_pre + forget_offset).T
    within = jnp.cumsum(forget_log, axis=1)
    total = within[:, -1]
    end_log = total[:, None] - within + gate_in
    local_level = jnp.max(end_log, axis=1)
    fresh = jnp.exp(end_log - local_level[:, None])
    scaled_key = (fresh[:, :, None] * key).astype(jnp.bfloat16)
    local_state = jnp.einsum("hse,hsd->hed", value, scaled_key, preferred_element_type=jnp.float32)
    local_normal = jnp.sum(scaled_key.astype(jnp.float32), axis=1)
    blank_state = (
        jnp.zeros_like(local_state),
        jnp.zeros_like(local_normal),
        jnp.full_like(local_level, LOWEST_LEVEL),
        jnp.zeros_like(total),
    )
    prior = shifted_2(glu[length - (taps - 1) :], "sp", 1)
    incoming = carried_in(
        (local_state, local_normal, local_level, total), "sp", merge_states, blank_state
    )
    extended = jnp.concatenate([prior, glu], axis=0).astype(jnp.float32)
    conv = depthwise(extended, conv_kernel.astype(jnp.float32))
    blocks = length // BLOCK

    def split(array):
        return jnp.moveaxis(array.reshape((heads_here, blocks, BLOCK) + array.shape[2:]), 1, 0)

    _, hidden = lax.scan(
        block_step,
        tuple(incoming[:3]),
        (split(query), split(key), split(value), split(gate_in), split(forget_log)),
    )
    hidden = jnp.moveaxis(hidden, 0, 1).reshape(heads_here, length, head_dim)
    hidden_squares = jnp.sum(hidden * hidden, axis=(0, 2))
    channel_sum, channel_squares, memory_squares = lax.psum(
        (jnp.sum(conv, axis=1), jnp.sum(conv * conv, axis=1), hidden_squares), "tp"
    )
    channels = conv.shape[1] * lax.axis_size("tp")
    mean = (channel_sum / channels)[:, None]
    variance = (channel_squares / channels)[:, None] - mean * mean
    conv_branch = jax.nn.silu((conv - mean) * lax.rsqrt(variance + EPS) * conv_norm_gain).astype(
        jnp.bfloat16
    )
    entries = heads_here * head_dim * lax.axis_size("tp")
    memory_scale = lax.rsqrt(memory_squares / entries + EPS)
    hidden = hidden * memory_scale[None, :, None]
    hidden = hidden * memory_norm_gain.reshape(heads_here, 1, head_dim)
    memory_branch = (
        hidden.transpose(1, 0, 2).reshape(length, heads_here * head_dim).astype(jnp.bfloat16)
    )
    conv_columns, memory_columns = (
        lax.all_gather(conv_out_weight, "sp", axis=1, tiled=True),
        lax.all_gather(memory_out_weight, "sp", axis=1, tiled=True),
    )
    contract = (((0,), (1,)), ((), ()))
    summed = lax.psum_scatter(
        (
            lax.dot_general(conv_columns, conv_branch, contract, preferred_element_type=jnp.float32)
            + lax.dot_general(
                memory_columns, memory_branch, contract, preferred_element_type=jnp.float32
            )
        ).astype(jnp.bfloat16),
        "tp",
        scatter_dimension=0,
        tiled=True,
    ).astype(jnp.float32)
    return summed.T.astype(jnp.bfloat16)


MESH = pl.DeviceIdType.MESH
IN_VMEM = pl.BlockSpec(memory_space=pltpu.VMEM)
SENDS = 30
ROW_TILE = 8
LANES = 128
NT = (((1,), (1,)), ((), ()))


def when(conditions, action):
    if not conditions:
        action()
        return
    every = conditions[0]
    for condition in conditions[1:]:
        every = jnp.logical_and(every, condition)
    pl.when(every)(action)


class Sends:
    def __init__(self, semaphores):
        self.semaphores = semaphores
        self.waits = []
        self.used = 0

    def shared(self, *waits):
        semaphore = self.semaphores.at[self.used]
        self.used += 1
        for whole, *conditions in waits:
            self.waits.append((whole, semaphore, conditions))
        return semaphore

    def start(self, source, target, arrival, device, *conditions, leaving=None):
        if leaving is None:
            leaving = self.shared((source, *conditions))
        copy = pltpu.make_async_remote_copy(
            src_ref=source,
            dst_ref=target,
            send_sem=leaving,
            recv_sem=arrival,
            device_id=device,
            device_id_type=MESH,
        )
        when(conditions, copy.start)

    def finish(self):
        for whole, semaphore, conditions in self.waits:
            when(conditions, waiting(whole, semaphore).wait_send)


def waiting(block, semaphore):
    return pltpu.make_async_remote_copy(
        src_ref=block,
        dst_ref=block,
        send_sem=semaphore,
        recv_sem=semaphore,
        device_id=(lax.axis_index("sp"), lax.axis_index("tp")),
        device_id_type=MESH,
    )


def arrived(block, semaphore, *conditions):
    copy = waiting(block, semaphore)
    when(conditions, copy.wait_recv)


def line_order(here, count):
    order = []
    for distance in range(1, count):
        order.append((here - distance, here >= distance, here + 1, here + 1 < count))
        order.append((here + distance, here + distance < count, here - 1, here > 0))
    return order


def pick(index, first, second):
    return jnp.where(jnp.full(first.shape, index, jnp.int32) == 1, second, first)


def stacked(rows, length):
    place = lax.broadcasted_iota(jnp.int32, (ROW_TILE, length), 0)
    result = jnp.zeros((ROW_TILE, length), jnp.float32)
    for index, row in enumerate(rows):
        result = jnp.where(place == index, row, result)
    return result


def as_columns(rows):
    length = rows.shape[1]
    rest = jnp.zeros((LANES - ROW_TILE, length), jnp.float32)
    return jnp.concatenate([rows, rest], axis=0).T


def as_rows(columns):
    length = columns[0].shape[0]
    place = lax.broadcasted_iota(jnp.int32, (length, LANES), 1)
    result = jnp.zeros((length, LANES), jnp.float32)
    for index, column in enumerate(columns):
        result = jnp.where(place == index, column, result)
    return result.T[:ROW_TILE]


def prefix_sums(rows):
    before = lax.broadcasted_iota(jnp.int32, (LANES, LANES), 0)
    after = lax.broadcasted_iota(jnp.int32, (LANES, LANES), 1)
    upper = (before <= after).astype(jnp.float32)
    carry = jnp.zeros((ROW_TILE, 1), jnp.float32)
    parts = []
    for start in range(0, rows.shape[1], LANES):
        part = carry + jnp.dot(
            rows[:, start : start + LANES],
            upper,
            precision=lax.Precision.HIGHEST,
            preferred_element_type=jnp.float32,
        )
        carry = part[:, LANES - 1 :]
        parts.append(part)
    return jnp.concatenate(parts, axis=1)


def layer_kernel(
    count,
    columns,
    all_tokens,
    all_wq,
    all_wk,
    all_wv,
    all_wcv,
    all_wcg,
    own_taps,
    own_conv_gain,
    own_memory_gain,
    own_input_gates,
    own_forget_gates,
    own_input_offsets,
    own_forget_offsets,
    own_memory_out,
    own_conv_out,
    slots,
    tokens,
    wq,
    wk,
    wv,
    wcv,
    wcg,
    shifts,
    lines,
    weights,
    product,
    taps,
    conv_gain,
    memory_gain,
    gate_weights,
    offsets,
    gate_rows,
    level_before,
    level_here,
    keys,
    values,
    queries,
    weight_near,
    weight_far,
    memory_done,
    squares_done,
    squares_in,
    extended,
    conv,
    sums_done,
    sums_in,
    conv_done,
    memory_in,
    conv_in,
    memory_out,
    conv_out,
    partial,
    load_sem,
    send_sem,
    token_sem,
    y_sem,
    weight_sem,
    own_sem,
    offset_sem,
    level_sem,
    pair_sem,
    query_sem,
    halo_sem,
    sums_sem,
    squares_sem,
    memory_sem,
    conv_sem,
    out_sem,
    slot_sem,
):
    f32, bf16 = jnp.float32, jnp.bfloat16
    me, tp = lax.axis_index("sp"), lax.axis_index("tp")
    layers = count // 2
    z, x, y, core = me // 2, lax.rem(me, 2), tp // 2, lax.rem(tp, 2)
    side, odd = z // 2, lax.rem(z, 2)
    length, features = tokens.shape
    depth, head_dim = wq.shape[0], wq.shape[1] // 2
    channels = wcv.shape[1] // 2
    rows = 4 * length
    span = rows // 2
    near, far = core == side, core != side
    first, second = x == 0, x == 1
    middle = jnp.logical_or(z == 1, z == 2)
    ends = jnp.logical_not(middle)
    peer = (me, y * 2 + 1 - core)
    below, above = (me - 2, tp), (me + 2, tp)
    x_side = (z * 2 + 1 - x, tp)
    y_side = (me, (1 - y) * 2 + core)
    has_below, has_above = z > 0, z + 1 < layers
    sends = Sends(send_sem)

    barrier = pltpu.get_barrier_semaphore()
    devices = count * columns
    rank = me * columns + tp
    for step in range(1, devices):
        other = lax.rem(rank + step, devices)
        pl.semaphore_signal(
            barrier,
            inc=1,
            device_id=(other // columns, lax.rem(other, columns)),
            device_id_type=MESH,
        )

    def block(i, j):
        return lines.at[
            pl.ds(pl.multiple_of(i * length, length), length),
            pl.ds(pl.multiple_of(j * features, features), features),
        ]

    def blocks(number):
        return lines.at[: number * length // columns, :]

    place = odd * 2 + x
    own_part = x * 2 + core
    loads = []
    for source, target, *conditions in (
        (all_tokens, tokens),
        (all_tokens, block(place, tp), near),
        (all_wq, wq),
        (all_wk, wk),
        (all_wv, wv),
        (all_wcv, wcv),
        (all_wcg, wcg),
        (own_input_offsets, shifts.at[0]),
        (own_forget_offsets, shifts.at[1]),
        (own_taps, taps, far),
        (own_conv_gain, conv_gain, far),
        (own_memory_gain, memory_gain, far),
        (own_input_gates, gate_weights.at[0], far),
        (own_forget_gates, gate_weights.at[1], far),
        (own_memory_out, memory_out.at[own_part]),
        (own_conv_out, conv_out.at[own_part]),
    ):
        copy = pltpu.make_async_copy(source, target, load_sem.at[len(loads)])
        loads.append((copy, conditions))
        when(conditions, copy.start)

    def loaded(first_load, last_load):
        for copy, conditions in loads[first_load:last_load]:
            when(conditions, copy.wait)

    loaded(0, 2)
    pl.semaphore_wait(barrier, devices - 1)

    goal = y * 2 + side
    mine, mine_sem = block(place, tp), token_sem.at[place, core]
    z_leaving = sends.shared(
        (blocks(1), ends), (blocks(4), middle, near), (blocks(6), middle, far)
    )
    x_leaving = sends.shared((blocks(3), near), (blocks(5), far))
    y_leaving = sends.shared((blocks(7), near), (blocks(9), far))
    sends.start(tokens, mine, mine_sem, (me - 2, goal), has_below, leaving=z_leaving)
    sends.start(tokens, mine, mine_sem, (me + 2, goal), has_above, leaving=z_leaving)
    sends.start(tokens, mine, mine_sem, (z * 2 + 1 - x, goal), leaving=x_leaving)
    sends.start(tokens, mine, y_sem.at[0], (me, (1 - y) * 2 + side), leaving=y_leaving)
    sends.start(tokens, mine, mine_sem, peer, far)

    def piece(unit, i):
        return weights.at[
            pl.ds(pl.multiple_of(i * depth, depth), depth),
            unit * head_dim : (unit + 1) * head_dim,
        ]

    def shares(k, x_goal):
        whole = pl.ds(pl.multiple_of(k * head_dim, head_dim), head_dim)
        part = pl.ds(pl.multiple_of(k * channels, channels), channels)
        if x_goal == 0:
            return (
                (wk.at[:, whole], 0, 0, head_dim),
                (wv.at[:, whole], 1, head_dim, head_dim),
            )
        return (
            (wq.at[:, whole], 0, 0, head_dim),
            (wcv.at[:, part], 1, head_dim, channels),
            (wcg.at[:, part], 1, head_dim + channels, channels),
        )

    own_rows = pl.ds(pl.multiple_of(me * depth, depth), depth)
    z_first = (1 - core) * 2
    share = weights.at[:depth, :]

    def send_weights(k, cross, leaving, *conditions, to_peer=False):
        for x_goal in range(2):
            chosen = conditions + ((x != x_goal) if cross else (x == x_goal),)
            for source, unit, start, size in shares(k, x_goal):
                device = peer if to_peer else ((z_first + k) * 2 + x_goal, y * 2 + unit)
                target = weights.at[own_rows, start : start + size]
                sends.start(
                    source, target, weight_sem.at[unit, me], device, *chosen, leaving=leaving
                )

    loaded(2, len(loads))
    mate_leaving, other_leaving = sends.shared((share,)), sends.shared((share,))
    send_weights(odd, False, other_leaving, far, to_peer=True)
    send_weights(1 - odd, False, mate_leaving, far)
    for x_goal in range(2):

        def keep():
            for source, _, start, size in shares(odd, x_goal):
                weights[own_rows, start : start + size] = source[...]

        when((far, x == x_goal), keep)

    own_arrays = (taps, conv_gain, memory_gain, gate_weights)
    for index, array in enumerate(own_arrays):
        sends.start(array, array, own_sem.at[index], peer, far)
    leaving = sends.shared((offsets.at[:2],))
    for k in range(2):
        device = ((z_first + k) * 2, y * 2 + side)
        sends.start(shifts, offsets.at[place], offset_sem.at[0], device, leaving=leaving)

    half_rows = memory_out.shape[1] // 2
    out_width = memory_out.shape[2]
    three_pieces = weights.at[: 3 * half_rows * out_width // (2 * head_dim), :]

    def out_piece(part, number):
        if number == 1:
            return conv_out.at[part]
        start = half_rows * (number // 2)
        return memory_out.at[part, start : start + half_rows, :]

    out_leaving = [sends.shared((three_pieces,)) for _ in range(2)]

    def send_out(number, *conditions):
        spot = out_piece(own_part, number)
        for device, leaving in zip((x_side, peer), out_leaving):
            sends.start(spot, spot, out_sem.at[own_part], device, *conditions, leaving=leaving)

    k_near = jnp.where(near, odd, 1 - core)
    groups = []
    for k in (k_near, 1 - k_near):
        source = core * 2 + k
        groups.append((source, k * 2 + x, k * 2 + 1 - x))
    for source, i, _ in groups:
        away, up = source != z, source < z
        onward = (jnp.where(up, z + 1, z - 1) * 2 + x, tp)
        for j in range(2):
            spot, sem = block(i, y * 2 + j), token_sem.at[i, j]
            arrived(spot, sem, jnp.logical_or(away, j != core))
            sends.start(spot, spot, sem, onward, away, middle, leaving=z_leaving)
            sends.start(spot, spot, sem, x_side, away, leaving=x_leaving)
            sends.start(spot, spot, y_sem.at[0], y_side, away, leaving=y_leaving)
    cross_leaving = [sends.shared((share,)) for _ in range(2)]
    send_weights(side, False, mate_leaving, near, middle)
    send_weights(odd, True, cross_leaving[1], far)
    send_weights(1 - odd, True, cross_leaving[0], far, ends)
    for _, _, i in groups:
        for j in range(2):
            spot, sem = block(i, y * 2 + j), token_sem.at[i, j]
            arrived(spot, sem)
            sends.start(spot, spot, y_sem.at[0], y_side, leaving=y_leaving)

    send_weights(side, False, mate_leaving, near, ends)
    last = jnp.logical_and(middle, first)
    send_weights(1 - side, False, other_leaving, near, jnp.logical_not(last))
    k_cross = jnp.where(near, 1 - side, 1 - odd)
    send_weights(k_cross, True, cross_leaving[0], jnp.logical_or(near, middle))
    send_weights(side, True, cross_leaving[1], near)
    send_weights(1 - side, False, other_leaving, near, last)
    for number in range(2):
        send_out(number, near, second)

    arrived(blocks(8), y_sem.at[0])
    for index, array in enumerate(own_arrays):
        arrived(array, own_sem.at[index], near)
    arrived(offsets, offset_sem.at[0], first)

    @pl.when(first)
    def _():
        gate_rows[...] = jnp.zeros_like(gate_rows)
        gate_rows[0:2, :] = gate_weights[0].astype(f32)
        gate_rows[2:4, :] = gate_weights[1].astype(f32)
        gates = lax.dot_general(
            lines[...], gate_rows[...].astype(bf16), NT, preferred_element_type=f32
        ).T
        shift = [jnp.concatenate([offsets[i, kind] for i in range(4)], 1) for kind in range(2)]
        gate_in = pick(odd, gates[0:1] + shift[0][0:1], gates[1:2] + shift[0][1:2])
        forget = pick(odd, gates[2:3] + shift[1][0:1], gates[3:4] + shift[1][1:2])
        forget_log = jnp.minimum(forget, 0.0) - jnp.log1p(jnp.exp(-jnp.abs(forget)))
        coarse = jnp.round(forget_log * 8.0) * 0.125
        within = prefix_sums(stacked((coarse, forget_log - coarse), rows))
        which = lax.broadcasted_iota(jnp.int32, (ROW_TILE, rows), 0)
        level_here[...] = jnp.where(which == 2, gate_in, within)

    first_core, second_core = core == 0, core == 1
    sends.start(level_here, level_before, level_sem.at[0], peer, first, first_core)

    @pl.when(jnp.logical_and(first, first_core))
    def _():
        level_before[...] = jnp.zeros_like(level_before)
        keys[:rows, :] = jnp.zeros_like(keys[:rows, :])
        values[:rows, :] = jnp.zeros_like(values[:rows, :])

    scale = head_dim ** (-0.5)
    reach = (rows + span, 2 * rows)
    stores = (weight_near, weight_far)

    def position_weights():
        before = level_before[...]
        which = lax.broadcasted_iota(jnp.int32, (ROW_TILE, rows), 0)
        here = level_here[...] + jnp.where(which < 2, before[:, rows - 1 :], 0.0)
        from_rows = jnp.concatenate([before, here], axis=1)
        to_columns = as_columns(here)
        tile = 64
        for start in range(0, rows, tile):
            index = start // span
            width = reach[index]
            to = to_columns[start : start + tile]
            log_weight = (
                (to[:, 0:1] - from_rows[0:1, :width])
                + (to[:, 1:2] - from_rows[1:2, :width])
                + from_rows[2:3, :width]
            )
            at = lax.broadcasted_iota(jnp.int32, (tile, width), 1)
            until = lax.broadcasted_iota(jnp.int32, (tile, width), 0) + (start + rows)
            seen = jnp.logical_and(at <= until, at >= rows * (1 - core))
            log_weight = jnp.where(seen, log_weight, -jnp.inf)
            weight = jnp.exp(log_weight - jnp.max(log_weight, axis=1, keepdims=True)) * scale
            stores[index][start - index * span : start - index * span + tile, :] = weight

    forward_leaving = sends.shared((weights.at[: 7 * depth // 2, :],))

    def own_unit(i):
        for unit in range(2):
            spot, sem = piece(unit, i), weight_sem.at[unit, i]
            arrived(spot, sem, core == unit)
            sends.start(spot, spot, sem, peer, core == unit, leaving=forward_leaving)

    def other_unit(i):
        for unit in range(2):
            arrived(piece(unit, i), weight_sem.at[unit, i], core != unit)

    def multiply(start, size):
        part = pl.ds(pl.multiple_of(start, size), size)
        return jnp.dot(lines[:, part], weights[part, :], preferred_element_type=f32)

    z_mate = side * 2 + 1 - odd
    z_far = (jnp.where(side == 0, 3, 0), jnp.where(side == 0, 2, 1))
    own_unit(z_mate * 2 + x)
    own_unit(z_far[0] * 2 + x)
    arrived(level_before, level_sem.at[0], first, second_core)
    when((first,), position_weights)
    for i in (z * 2 + 1 - x, z_mate * 2 + 1 - x):
        own_unit(i)
    for i in (z_mate * 2 + x, z * 2 + 1 - x, z_mate * 2 + 1 - x):
        other_unit(i)
    for unit in range(2):
        arrived(piece(unit, me), weight_sem.at[unit, me], near)
    half = count // 2 * depth
    product[...] = multiply(side * half, half)
    own_unit(z_far[0] * 2 + 1 - x)
    own_unit(z_far[1] * 2 + x)
    own_unit(z_far[1] * 2 + 1 - x)
    for pair in z_far:
        other_unit(pair * 2)
        other_unit(pair * 2 + 1)
        product[...] += multiply(pair * 2 * depth, 2 * depth)

    for number in range(2):
        send_out(number, first, near)

    @pl.when(second)
    def _():
        queries[...] = product[:, :head_dim].astype(bf16)

    leaving = sends.shared((queries, second))
    for number in (0, 1, 3, 2):
        part = queries.at[number * length : (number + 1) * length, :]
        sends.start(part, part, query_sem.at[number], x_side, second, leaving=leaving)

    @pl.when(first)
    def _():
        keys[rows:, :] = product[:, :head_dim].astype(bf16)
        values[rows:, :] = product[:, head_dim:].astype(bf16)

    leaving = sends.shared((keys, first, first_core))
    for array in (keys, values):
        sends.start(
            array.at[rows:, :],
            array.at[:rows, :],
            pair_sem.at[0],
            peer,
            first,
            first_core,
            leaving=leaving,
        )

    halo = extended.shape[0] - rows

    @pl.when(second)
    def _():
        gated = product[:, head_dim : head_dim + channels] * jax.nn.sigmoid(
            product[:, head_dim + channels :]
        )
        extended[halo:, :] = gated.astype(bf16).astype(f32)

    sends.start(
        extended.at[rows:, :], extended.at[:halo, :], halo_sem.at[0], peer, second, first_core
    )

    @pl.when(jnp.logical_and(second, first_core))
    def _():
        extended[:halo, :] = jnp.zeros((halo, channels), f32)

    arrived(extended.at[:halo, :], halo_sem.at[0], second, second_core)
    source_index = y * layers + z

    @pl.when(second)
    def _():
        number = taps.shape[0]
        kernel = taps[...].astype(f32)
        kernel = pick(odd, kernel[:, :channels], kernel[:, channels:])
        for start in range(0, rows, length):
            base = start + halo - (number - 1)
            total = extended[base : base + length, :] * kernel[0:1]
            for index in range(1, number):
                total = total + (
                    extended[base + index : base + index + length, :] * kernel[index : index + 1]
                )
            conv[start : start + length, :] = total
        all_rows = conv[...]
        both = as_rows(
            (
                jnp.sum(all_rows, axis=1, keepdims=True),
                jnp.sum(all_rows * all_rows, axis=1, keepdims=True),
            )
        )
        sums_done[...] = jnp.concatenate(
            [both[:2, start : start + LANES] for start in range(0, rows, LANES)], axis=0
        )
        sums_in[source_index] = sums_done[...]

    sources = [(z_other, y_other) for z_other in range(layers) for y_other in range(2)]
    others = sums_in.at[: count - 1]
    leaving = sends.shared((others, second))
    for z_other, y_other in sources:
        away = jnp.logical_or(z != z_other, y != y_other)
        device = (z_other * 2 + 1, y_other * 2 + core)
        sends.start(
            sums_done,
            sums_in.at[source_index],
            sums_sem.at[0],
            device,
            second,
            away,
            leaving=leaving,
        )
    arrived(others, sums_sem.at[0], second)

    @pl.when(second)
    def _():
        total = sums_in[0]
        for index in range(1, 2 * layers):
            total = total + sums_in[index]
        total = total * (1.0 / (2 * layers * channels))
        total = jnp.concatenate([total[at : at + 2] for at in range(0, ROW_TILE, 2)], axis=1)
        mean = total[0:1]
        inverse = lax.rsqrt(total[1:2] - mean * mean + EPS)
        across = as_columns(stacked((mean, inverse), rows))
        gain = conv_gain[...]
        gain = pick(odd, gain[:, :channels], gain[:, channels:])
        normed = (conv[...] - across[:, 0:1]) * across[:, 1:2] * gain
        conv_done[...] = (normed * jax.nn.sigmoid(normed)).astype(bf16)

    piece_rows = span * (head_dim + channels) // (2 * head_dim)

    def so_many(number):
        return weights.at[: number * piece_rows, :]

    up_leaving = sends.shared(*((so_many(at + 1), z == at) for at in range(layers - 1)))
    down_leaving = sends.shared(*((so_many(layers - at), z == at) for at in range(1, layers)))
    given_leaving = sends.shared((memory_in.at[0], first), (conv_in.at[0], second))

    def spread(done, inside, semaphores, home, number):
        here, index = x == home, number // 2
        source = done.at[number * length : (number + 1) * length, :]
        part = slice(index * length, (index + 1) * length)
        target, sem = inside.at[z, part, :], semaphores.at[z, index]
        if number % 2 != home:
            sends.start(source, target, sem, x_side, here, leaving=given_leaving)
            return
        sends.start(source, target, sem, below, here, has_below, leaving=down_leaving)
        sends.start(source, target, sem, above, here, has_above, leaving=up_leaving)

        @pl.when(here)
        def _():
            inside[z, part, :] = source[...]

    for number in range(4):
        spread(conv_done, conv_in, conv_sem, 1, number)
    for number in range(2):
        send_out(number, second, far)
    send_out(2, second)

    for array in (keys,):
        arrived(array, pair_sem.at[0], first, second_core)
    for number in (0, 1, 3, 2):
        start, index, inner = number * length, number // 2, number % 2
        arrived(queries.at[start : start + length, :], query_sem.at[number], first)

        @pl.when(first)
        def _():
            width = reach[index]
            gain = memory_gain[...]
            gain = pick(odd, gain[:, :head_dim], gain[:, head_dim:])
            scores = lax.dot_general(
                queries[start : start + length, :],
                keys[:width, :],
                NT,
                preferred_element_type=f32,
            )
            scores = scores * stores[index][inner * length : (inner + 1) * length, :]
            numer = jnp.dot(scores.astype(bf16), values[:width, :], preferred_element_type=f32)
            denom = jnp.sum(scores, axis=1, keepdims=True)
            cell = numer / jnp.maximum(jnp.abs(denom), 1.0)
            memory_done[start : start + length, :] = (cell * gain).astype(bf16)
            square = as_rows((jnp.sum(cell * cell, axis=1, keepdims=True),))
            squares_done[index, inner] = square[0:1]

        spread(memory_done, memory_in, memory_sem, 0, number)
    for number in range(2):
        send_out(number, first, far)
    send_out(2, first)

    @pl.when(first)
    def _():
        for index in range(2):
            squares_in[index * count + source_index] = squares_done[index, 0]

    for index in range(2):
        squares_leaving = sends.shared((squares_in.at[: 2 * count - 1], first))
        for z_other, y_other in sources:
            for x_other in range(2):
                away = jnp.logical_or(
                    jnp.logical_or(z != z_other, y != y_other), x != x_other
                )
                sends.start(
                    squares_done.at[index, x_other],
                    squares_in.at[index * count + source_index],
                    squares_sem.at[index],
                    (z_other * 2 + x_other, y_other * 2 + core),
                    first,
                    away,
                    leaving=squares_leaving,
                )

    order = line_order(z, layers)
    across = (1 - x) * 2 + core
    across_leaving = sends.shared((three_pieces,))

    def pass_on(distance, kind, index, *conditions):
        inside, semaphores, home = kind
        part = slice(index * length, (index + 1) * length)
        if distance == 0:
            away = x != home
            spot, sem = inside.at[z, part, :], semaphores.at[z, index]
            arrived(spot, sem, away, *conditions)
            for device, further, leaving in (
                (below, has_below, down_leaving),
                (above, has_above, up_leaving),
            ):
                sends.start(spot, spot, sem, device, away, further, *conditions, leaving=leaving)
            return
        down, up = order[2 * distance - 2 : 2 * distance]
        for (source, there, onward, further), leaving in ((down, up_leaving), (up, down_leaving)):
            spot, sem = inside.at[source, part, :], semaphores.at[source, index]
            arrived(spot, sem, there, *conditions)
            device = (onward * 2 + x, tp)
            sends.start(spot, spot, sem, device, there, further, *conditions, leaving=leaving)

    def share_out(*conditions):
        arrived(three_pieces, out_sem.at[across], *conditions)
        for spot in (memory_out.at[across], conv_out.at[across]):
            sends.start(spot, spot, out_sem.at[across], peer, *conditions, leaving=across_leaving)

    convs, memories = (conv_in, conv_sem, 1), (memory_in, memory_sem, 0)
    pass_on(0, convs, 0, first)
    pass_on(0, convs, 1, first)
    for distance in range(1, layers):
        for kind in (memories, convs):
            for index in range(2):
                if distance + 1 < layers or index == 0:
                    pass_on(distance, kind, index, first)
        if distance == layers - 2:
            share_out(first)
    for distance in range(1, layers + 2):
        if distance < layers:
            pass_on(distance, convs, 0, second)
            pass_on(distance, convs, 1, second)
        if 0 <= distance - 2 < layers - 1:
            pass_on(distance - 2, memories, 1, second)
        if 0 <= distance - 1 < layers:
            pass_on(distance - 1, memories, 0, second)
        if distance == layers - 1:
            share_out(second)
    entries = layers * 2 * head_dim
    for index in range(2):
        part = slice(index * length, (index + 1) * length)
        if index == 1:
            pass_on(layers - 1, memories, 1)
            pass_on(layers - 1, convs, 1, first)
        at = index * count
        arrived(squares_in.at[at : at + count - 1], squares_sem.at[index], first)
        arrived(squares_in.at[at : at + count], squares_sem.at[index], second)
        if index == 0:
            for group in range(2):
                arrived(three_pieces, out_sem.at[group * 2 + 1 - core])
        total = squares_in[at]
        for slot in range(1, 2 * layers):
            total = total + squares_in[at + slot]
        row_scale = stacked((lax.rsqrt(total * (1.0 / entries) + EPS),), length)
        row_scale = as_columns(row_scale)[:, 0:1]
        for group in range(2):
            from_memory, from_conv = None, None
            for head in range(layers):
                where = group * 2 + 1 - head // 2
                inner = head % 2
                memory_term = jnp.dot(
                    memory_in[head, part, :],
                    memory_out[where, inner * head_dim : (inner + 1) * head_dim, :],
                    preferred_element_type=f32,
                )
                conv_term = jnp.dot(
                    conv_in[head, part, :],
                    conv_out[where, inner * channels : (inner + 1) * channels, :],
                    preferred_element_type=f32,
                )
                from_memory = memory_term if head == 0 else from_memory + memory_term
                from_conv = conv_term if head == 0 else from_conv + conv_term
            width = from_memory.shape[1]
            partial[index, :, group * width : (group + 1) * width] = (
                from_conv + row_scale * from_memory
            ).astype(bf16)
        device = ((core * 2 + index) * 2 + x, z)
        away = jnp.logical_or(core * 2 + index != z, tp != z)
        sends.start(partial.at[index], slots.at[y], slot_sem.at[y], device, away)

        @pl.when(jnp.logical_not(away))
        def _():
            slots[y] = partial[index]

    for y_other in range(2):
        own = jnp.logical_and(tp == z, jnp.logical_and(y == y_other, core == side))
        arrived(slots.at[y_other], slot_sem.at[y_other], jnp.logical_not(own))
    sends.finish()


def layer(arrays):
    count, columns = lax.axis_size("sp"), lax.axis_size("tp")
    (
        tokens,
        conv_value_weight,
        conv_gate_weight,
        conv_kernel,
        conv_norm_gain,
        query_weight,
        key_weight,
        value_weight,
        input_gate_weight,
        forget_gate_weight,
        input_offset,
        forget_offset,
        memory_norm_gain,
        conv_out_weight,
        memory_out_weight,
    ) = arrays
    length, features = tokens.shape
    depth, head_dim = query_weight.shape[0], query_weight.shape[1] // 2
    channels = conv_value_weight.shape[1] // 2
    wide = features * columns
    rows = length * count // 2
    span = rows // 2
    layers = count // 2
    halo = -(-(conv_kernel.shape[0] - 1) // ROW_TILE) * ROW_TILE
    width = memory_out_weight.shape[1]
    f32, bf16 = jnp.float32, jnp.bfloat16
    DMA = pltpu.SemaphoreType.DMA
    V = pltpu.VMEM
    return pl.pallas_call(
        lambda *refs: layer_kernel(count, columns, *refs),
        out_shape=jax.ShapeDtypeStruct((2, length, features), bf16),
        in_specs=[pl.BlockSpec(memory_space=pltpu.HBM)] * 15,
        out_specs=IN_VMEM,
        scratch_shapes=[
            V(tokens.shape, bf16),
            V(query_weight.shape, bf16),
            V(key_weight.shape, bf16),
            V(value_weight.shape, bf16),
            V(conv_value_weight.shape, bf16),
            V(conv_gate_weight.shape, bf16),
            V((2, 2, length), f32),
            V((rows, wide), bf16),
            V((wide, 2 * head_dim), bf16),
            V((rows, 2 * head_dim), f32),
            V(conv_kernel.shape, bf16),
            V((1, 2 * channels), f32),
            V((1, 2 * head_dim), f32),
            V((2, 2, wide), bf16),
            V((4, 2, 2, length), f32),
            V((LANES, wide), f32),
            V((ROW_TILE, rows), f32),
            V((ROW_TILE, rows), f32),
            V((2 * rows, head_dim), bf16),
            V((2 * rows, head_dim), bf16),
            V((rows, head_dim), bf16),
            V((span, rows + span), f32),
            V((span, 2 * rows), f32),
            V((rows, head_dim), bf16),
            V((2, 2, 1, length), f32),
            V((2 * count, 1, length), f32),
            V((halo + rows, channels), f32),
            V((rows, channels), f32),
            V((ROW_TILE, LANES), f32),
            V((count, ROW_TILE, LANES), f32),
            V((rows, channels), bf16),
            V((layers, span, head_dim), bf16),
            V((layers, span, channels), bf16),
            V((4, 2 * head_dim, width), bf16),
            V((4, 2 * channels, width), bf16),
            V((2, length, features), bf16),
            DMA((16,)),
            DMA((SENDS,)),
            DMA((4, 2)),
            DMA((1,)),
            DMA((2, count)),
            DMA((4,)),
            DMA((1,)),
            DMA((1,)),
            DMA((1,)),
            DMA((4,)),
            DMA((1,)),
            DMA((1,)),
            DMA((2,)),
            DMA((layers, 2)),
            DMA((layers, 2)),
            DMA((4,)),
            DMA((2,)),
        ],
        compiler_params=pltpu.CompilerParams(
            collective_id=0, has_side_effects=True, vmem_limit_bytes=40 * 2**20
        ),
    )(
        *(
            pltpu.with_memory_space_constraint(array, pltpu.HBM)
            for array in (
                tokens,
                query_weight,
                key_weight,
                value_weight,
                conv_value_weight,
                conv_gate_weight,
                conv_kernel,
                conv_norm_gain.reshape(1, -1),
                memory_norm_gain.reshape(1, -1),
                input_gate_weight.T,
                forget_gate_weight.T,
                input_offset.T,
                forget_offset.T,
                memory_out_weight,
                conv_out_weight,
            )
        )
    )


def on_device_by_column(*arrays):
    slots = layer(arrays)
    return jnp.sum(slots.astype(jnp.float32), axis=0).astype(jnp.bfloat16)


def splits_by_column(mesh, tokens, query_weight, conv_value_weight, conv_kernel, input_gate_weight):
    count, columns = mesh.shape["sp"], mesh.shape["tp"]
    heads = input_gate_weight.shape[1]
    head_dim = query_weight.shape[1] // heads
    length = tokens.shape[0] // count
    return (
        count == 8
        and columns == 4
        and heads == count
        and length == LANES
        and tokens.size * 2 <= 4 * 2**20
        and conv_value_weight.shape[1] * 2 == head_dim * heads
        and head_dim == 256
        and conv_kernel.shape[0] - 1 <= length
    )


def solution(mesh):
    in_specs = (
        P("sp", "tp"),
        P("sp", "tp"),
        P("sp", "tp"),
        P(None, "tp"),
        P("tp"),
        P("sp", "tp"),
        P("sp", "tp"),
        P("sp", "tp"),
        P(None, "tp"),
        P(None, "tp"),
        P("sp", "tp"),
        P("sp", "tp"),
        P("tp"),
        P("tp", "sp"),
        P("tp", "sp"),
    )
    out_specs = P("sp", "tp")

    def run(*arrays):
        by_column = splits_by_column(
            mesh, arrays[0], arrays[5], arrays[1], arrays[3], arrays[8]
        )
        on_device = on_device_by_column if by_column else on_device_by_position
        return jax.shard_map(
            on_device, mesh=mesh, in_specs=in_specs, out_specs=out_specs, check_vma=False
        )(*arrays)

    return run
```

```python
import jax
import jax.numpy as jnp
from jax import lax
from jax.experimental import pallas as pl
from jax.experimental.pallas import tpu as pltpu
from jax.sharding import PartitionSpec as P

BLOCK = 64


EPS = 1e-06
LOWEST_LEVEL = -1e30


def shifted_2(value, axis, steps):
    count = lax.axis_size(axis)
    leading, last = (max(0, -steps), min(count, count - steps))
    return lax.ppermute(value, axis, [(source, source + steps) for source in range(leading, last)])


def carried_in(shard, axis, join, neutral):
    place = lax.axis_index(axis)
    gathered = jax.tree.map(
        lambda a, kind: lax.all_gather(a.astype(kind), axis),
        shard,
        (jnp.bfloat16, jnp.bfloat16, jnp.bfloat16, jnp.bfloat16),
    )
    state = jax.tree.map(lambda a, e: jnp.zeros_like(a) + jnp.asarray(e, a.dtype), shard, neutral)

    def one(step, state):
        return join(
            state,
            jax.tree.map(
                lambda a, own: lax.dynamic_index_in_dim(a, step, 0, False).astype(own.dtype),
                gathered,
                shard,
            ),
        )

    return lax.fori_loop(0, place, one, state)


def block_step(carry, inputs):
    state, normal, level = carry
    query, key, value, gate_in, forget_log = inputs
    length = gate_in.shape[-1]
    scale = query.shape[-1] ** (-0.5)
    causal = jnp.tril(jnp.ones((length, length), dtype=bool))
    within = jnp.cumsum(forget_log, axis=-1)
    log_weight = within[:, :, None] - within[:, None, :] + gate_in[:, None, :]
    log_weight = jnp.where(causal, log_weight, -jnp.inf)
    carried = within + level[:, None]
    top = jnp.maximum(carried, jnp.max(log_weight, axis=-1))
    weight = jnp.exp(log_weight - top[:, :, None])
    carried_weight = jnp.exp(carried - top) * scale
    scores = jnp.einsum("htd,hsd->hts", query, key, preferred_element_type=jnp.float32) * (
        scale * weight
    )
    numer = jnp.einsum(
        "hts,hse->hte", scores.astype(jnp.bfloat16), value, preferred_element_type=jnp.float32
    )
    numer = numer + carried_weight[:, :, None] * jnp.einsum(
        "hed,htd->hte", state.astype(jnp.bfloat16), query, preferred_element_type=jnp.float32
    )
    denom = jnp.sum(scores, axis=-1) + carried_weight * jnp.einsum(
        "hd,htd->ht", normal.astype(jnp.bfloat16), query, preferred_element_type=jnp.float32
    )
    result = numer / jnp.maximum(jnp.abs(denom), 1.0)[:, :, None]
    last = within[:, -1]
    end_log = last[:, None] - within + gate_in
    new_level = jnp.maximum(last + level, jnp.max(end_log, axis=-1))
    keep = jnp.exp(last + level - new_level)
    fresh = jnp.exp(end_log - new_level[:, None])
    scaled_key = (fresh[:, :, None] * key).astype(jnp.bfloat16)
    new_state = keep[:, None, None] * state + jnp.einsum(
        "hse,hsd->hed", value, scaled_key, preferred_element_type=jnp.float32
    )
    new_normal = keep[:, None] * normal + jnp.sum(scaled_key.astype(jnp.float32), axis=1)
    return ((new_state, new_normal, new_level), result)


def depthwise(extended, kernel):
    taps = kernel.shape[0]
    length = extended.shape[0] - taps + 1
    total = extended[0:length] * kernel[0]
    for index in range(1, taps):
        total = total + extended[index : index + length] * kernel[index]
    return total


def merge_states(first, second):
    first_state, first_normal, first_level, first_total = first
    second_state, second_normal, second_level, second_total = second
    shifted = first_level + second_total
    level = jnp.maximum(shifted, second_level)
    older = jnp.exp(shifted - level)
    newer = jnp.exp(second_level - level)
    state = older[:, None, None] * first_state + newer[:, None, None] * second_state
    normal = older[:, None] * first_normal + newer[:, None] * second_normal
    return (state, normal, level, first_total + second_total)


def on_device_by_position(
    tokens,
    conv_value_weight,
    conv_gate_weight,
    conv_kernel,
    conv_norm_gain,
    query_weight,
    key_weight,
    value_weight,
    input_gate_weight,
    forget_gate_weight,
    input_offset,
    forget_offset,
    memory_norm_gain,
    conv_out_weight,
    memory_out_weight,
):
    length = tokens.shape[0]
    heads_here = input_gate_weight.shape[1]
    whole = lax.all_gather(tokens, "tp", axis=1, tiled=True)
    pieces = (
        lax.all_gather(conv_value_weight, "sp", axis=0, tiled=True),
        lax.all_gather(conv_gate_weight, "sp", axis=0, tiled=True),
        lax.all_gather(query_weight, "sp", axis=0, tiled=True),
        lax.all_gather(key_weight, "sp", axis=0, tiled=True),
        lax.all_gather(value_weight, "sp", axis=0, tiled=True),
    )
    folded = tuple((jnp.dot(whole, piece, preferred_element_type=jnp.float32) for piece in pieces))
    conv_value, conv_gate, query_flat, key_flat, value_flat = folded
    gate_pre = jnp.dot(whole, input_gate_weight, preferred_element_type=jnp.float32)
    forget_pre = jnp.dot(whole, forget_gate_weight, preferred_element_type=jnp.float32)
    glu = (conv_value * jax.nn.sigmoid(conv_gate)).astype(jnp.bfloat16)
    taps = conv_kernel.shape[0]
    head_dim = query_flat.shape[1] // heads_here

    def to_heads(flat):
        return flat.astype(jnp.bfloat16).reshape(length, heads_here, head_dim).transpose(1, 0, 2)

    query = to_heads(query_flat)
    key = to_heads(key_flat)
    value = to_heads(value_flat)
    gate_in = (gate_pre + input_offset).T
    forget_log = jax.nn.log_sigmoid(forget_pre + forget_offset).T
    within = jnp.cumsum(forget_log, axis=1)
    total = within[:, -1]
    end_log = total[:, None] - within + gate_in
    local_level = jnp.max(end_log, axis=1)
    fresh = jnp.exp(end_log - local_level[:, None])
    scaled_key = (fresh[:, :, None] * key).astype(jnp.bfloat16)
    local_state = jnp.einsum("hse,hsd->hed", value, scaled_key, preferred_element_type=jnp.float32)
    local_normal = jnp.sum(scaled_key.astype(jnp.float32), axis=1)
    blank_state = (
        jnp.zeros_like(local_state),
        jnp.zeros_like(local_normal),
        jnp.full_like(local_level, LOWEST_LEVEL),
        jnp.zeros_like(total),
    )
    prior = shifted_2(glu[length - (taps - 1) :], "sp", 1)
    incoming = carried_in(
        (local_state, local_normal, local_level, total), "sp", merge_states, blank_state
    )
    extended = jnp.concatenate([prior, glu], axis=0).astype(jnp.float32)
    conv = depthwise(extended, conv_kernel.astype(jnp.float32))
    blocks = length // BLOCK

    def split(array):
        return jnp.moveaxis(array.reshape((heads_here, blocks, BLOCK) + array.shape[2:]), 1, 0)

    _, hidden = lax.scan(
        block_step,
        tuple(incoming[:3]),
        (split(query), split(key), split(value), split(gate_in), split(forget_log)),
    )
    hidden = jnp.moveaxis(hidden, 0, 1).reshape(heads_here, length, head_dim)
    hidden_squares = jnp.sum(hidden * hidden, axis=(0, 2))
    channel_sum, channel_squares, memory_squares = lax.psum(
        (jnp.sum(conv, axis=1), jnp.sum(conv * conv, axis=1), hidden_squares), "tp"
    )
    channels = conv.shape[1] * lax.axis_size("tp")
    mean = (channel_sum / channels)[:, None]
    variance = (channel_squares / channels)[:, None] - mean * mean
    conv_branch = jax.nn.silu((conv - mean) * lax.rsqrt(variance + EPS) * conv_norm_gain).astype(
        jnp.bfloat16
    )
    entries = heads_here * head_dim * lax.axis_size("tp")
    memory_scale = lax.rsqrt(memory_squares / entries + EPS)
    hidden = hidden * memory_scale[None, :, None]
    hidden = hidden * memory_norm_gain.reshape(heads_here, 1, head_dim)
    memory_branch = (
        hidden.transpose(1, 0, 2).reshape(length, heads_here * head_dim).astype(jnp.bfloat16)
    )
    conv_columns, memory_columns = (
        lax.all_gather(conv_out_weight, "sp", axis=1, tiled=True),
        lax.all_gather(memory_out_weight, "sp", axis=1, tiled=True),
    )
    contract = (((0,), (1,)), ((), ()))
    summed = lax.psum_scatter(
        (
            lax.dot_general(conv_columns, conv_branch, contract, preferred_element_type=jnp.float32)
            + lax.dot_general(
                memory_columns, memory_branch, contract, preferred_element_type=jnp.float32
            )
        ).astype(jnp.bfloat16),
        "tp",
        scatter_dimension=0,
        tiled=True,
    ).astype(jnp.float32)
    return summed.T.astype(jnp.bfloat16)


MESH = pl.DeviceIdType.MESH
IN_VMEM = pl.BlockSpec(memory_space=pltpu.VMEM)
SENDS = 30
ROW_TILE = 8
LANES = 128
NT = (((1,), (1,)), ((), ()))


def when(conditions, action):
    if not conditions:
        action()
        return
    every = conditions[0]
    for condition in conditions[1:]:
        every = jnp.logical_and(every, condition)
    pl.when(every)(action)


class Sends:
    def __init__(self, semaphores):
        self.semaphores = semaphores
        self.waits = []
        self.used = 0

    def shared(self, *waits):
        semaphore = self.semaphores.at[self.used]
        self.used += 1
        for whole, *conditions in waits:
            self.waits.append((whole, semaphore, conditions))
        return semaphore

    def start(self, source, target, arrival, device, *conditions, leaving=None):
        if leaving is None:
            leaving = self.shared((source, *conditions))
        copy = pltpu.make_async_remote_copy(
            src_ref=source,
            dst_ref=target,
            send_sem=leaving,
            recv_sem=arrival,
            device_id=device,
            device_id_type=MESH,
        )
        when(conditions, copy.start)

    def finish(self):
        for whole, semaphore, conditions in self.waits:
            when(conditions, waiting(whole, semaphore).wait_send)


def waiting(block, semaphore):
    return pltpu.make_async_remote_copy(
        src_ref=block,
        dst_ref=block,
        send_sem=semaphore,
        recv_sem=semaphore,
        device_id=(lax.axis_index("sp"), lax.axis_index("tp")),
        device_id_type=MESH,
    )


def arrived(block, semaphore, *conditions):
    copy = waiting(block, semaphore)
    when(conditions, copy.wait_recv)


def line_order(here, count):
    order = []
    for distance in range(1, count):
        order.append((here - distance, here >= distance, here + 1, here + 1 < count))
        order.append((here + distance, here + distance < count, here - 1, here > 0))
    return order


def pick(index, first, second):
    return jnp.where(jnp.full(first.shape, index, jnp.int32) == 1, second, first)


def stacked(rows, length):
    place = lax.broadcasted_iota(jnp.int32, (ROW_TILE, length), 0)
    result = jnp.zeros((ROW_TILE, length), jnp.float32)
    for index, row in enumerate(rows):
        result = jnp.where(place == index, row, result)
    return result


def as_columns(rows):
    length = rows.shape[1]
    rest = jnp.zeros((LANES - ROW_TILE, length), jnp.float32)
    return jnp.concatenate([rows, rest], axis=0).T


def as_rows(columns):
    length = columns[0].shape[0]
    place = lax.broadcasted_iota(jnp.int32, (length, LANES), 1)
    result = jnp.zeros((length, LANES), jnp.float32)
    for index, column in enumerate(columns):
        result = jnp.where(place == index, column, result)
    return result.T[:ROW_TILE]


def prefix_sums(rows):
    before = lax.broadcasted_iota(jnp.int32, (LANES, LANES), 0)
    after = lax.broadcasted_iota(jnp.int32, (LANES, LANES), 1)
    upper = (before <= after).astype(jnp.float32)
    carry = jnp.zeros((ROW_TILE, 1), jnp.float32)
    parts = []
    for start in range(0, rows.shape[1], LANES):
        part = carry + jnp.dot(
            rows[:, start : start + LANES],
            upper,
            precision=lax.Precision.HIGHEST,
            preferred_element_type=jnp.float32,
        )
        carry = part[:, LANES - 1 :]
        parts.append(part)
    return jnp.concatenate(parts, axis=1)


def layer_kernel(
    count,
    columns,
    all_tokens,
    all_wq,
    all_wk,
    all_wv,
    all_wcv,
    all_wcg,
    own_taps,
    own_conv_gain,
    own_memory_gain,
    own_input_gates,
    own_forget_gates,
    own_input_offsets,
    own_forget_offsets,
    own_memory_out,
    own_conv_out,
    slots,
    tokens,
    wq,
    wk,
    wv,
    wcv,
    wcg,
    shifts,
    lines,
    weights,
    product,
    taps,
    conv_gain,
    memory_gain,
    gate_weights,
    offsets,
    gate_rows,
    level_before,
    level_here,
    keys,
    values,
    queries,
    weight_near,
    weight_far,
    memory_done,
    squares_done,
    squares_in,
    extended,
    conv,
    sums_done,
    sums_in,
    conv_done,
    memory_in,
    conv_in,
    memory_out,
    conv_out,
    partial,
    load_sem,
    send_sem,
    token_sem,
    y_sem,
    weight_sem,
    own_sem,
    offset_sem,
    level_sem,
    pair_sem,
    query_sem,
    halo_sem,
    sums_sem,
    squares_sem,
    memory_sem,
    conv_sem,
    out_sem,
    slot_sem,
):
    f32, bf16 = jnp.float32, jnp.bfloat16
    me, tp = lax.axis_index("sp"), lax.axis_index("tp")
    layers = count // 2
    z, x, y, core = me // 2, lax.rem(me, 2), tp // 2, lax.rem(tp, 2)
    side, odd = z // 2, lax.rem(z, 2)
    length, features = tokens.shape
    depth, head_dim = wq.shape[0], wq.shape[1] // 2
    channels = wcv.shape[1] // 2
    rows = 4 * length
    span = rows // 2
    near, far = core == side, core != side
    first, second = x == 0, x == 1
    middle = jnp.logical_or(z == 1, z == 2)
    ends = jnp.logical_not(middle)
    peer = (me, y * 2 + 1 - core)
    below, above = (me - 2, tp), (me + 2, tp)
    x_side = (z * 2 + 1 - x, tp)
    y_side = (me, (1 - y) * 2 + core)
    has_below, has_above = z > 0, z + 1 < layers
    sends = Sends(send_sem)

    barrier = pltpu.get_barrier_semaphore()
    devices = count * columns
    rank = me * columns + tp
    for step in range(1, devices):
        other = lax.rem(rank + step, devices)
        pl.semaphore_signal(
            barrier,
            inc=1,
            device_id=(other // columns, lax.rem(other, columns)),
            device_id_type=MESH,
        )

    def block(i, j):
        return lines.at[
            pl.ds(pl.multiple_of(i * length, length), length),
            pl.ds(pl.multiple_of(j * features, features), features),
        ]

    def blocks(number):
        return lines.at[: number * length // columns, :]

    place = odd * 2 + x
    own_part = x * 2 + core
    loads = []
    for source, target, *conditions in (
        (all_tokens, tokens),
        (all_tokens, block(place, tp), near),
        (all_wq, wq),
        (all_wk, wk),
        (all_wv, wv),
        (all_wcv, wcv),
        (all_wcg, wcg),
        (own_input_offsets, shifts.at[0]),
        (own_forget_offsets, shifts.at[1]),
        (own_taps, taps, far),
        (own_conv_gain, conv_gain, far),
        (own_memory_gain, memory_gain, far),
        (own_input_gates, gate_weights.at[0], far),
        (own_forget_gates, gate_weights.at[1], far),
        (own_memory_out, memory_out.at[own_part]),
        (own_conv_out, conv_out.at[own_part]),
    ):
        copy = pltpu.make_async_copy(source, target, load_sem.at[len(loads)])
        loads.append((copy, conditions))
        when(conditions, copy.start)

    def loaded(first_load, last_load):
        for copy, conditions in loads[first_load:last_load]:
            when(conditions, copy.wait)

    loaded(0, 2)
    pl.semaphore_wait(barrier, devices - 1)

    goal = y * 2 + side
    mine, mine_sem = block(place, tp), token_sem.at[place, core]
    z_leaving = sends.shared(
        (blocks(1), ends), (blocks(4), middle, near), (blocks(6), middle, far)
    )
    x_leaving = sends.shared((blocks(3), near), (blocks(5), far))
    y_leaving = sends.shared((blocks(7), near), (blocks(9), far))
    sends.start(tokens, mine, mine_sem, (me - 2, goal), has_below, leaving=z_leaving)
    sends.start(tokens, mine, mine_sem, (me + 2, goal), has_above, leaving=z_leaving)
    sends.start(tokens, mine, mine_sem, (z * 2 + 1 - x, goal), leaving=x_leaving)
    sends.start(tokens, mine, y_sem.at[0], (me, (1 - y) * 2 + side), leaving=y_leaving)
    sends.start(tokens, mine, mine_sem, peer, far)

    def piece(unit, i):
        return weights.at[
            pl.ds(pl.multiple_of(i * depth, depth), depth),
            unit * head_dim : (unit + 1) * head_dim,
        ]

    def shares(k, x_goal):
        whole = pl.ds(pl.multiple_of(k * head_dim, head_dim), head_dim)
        part = pl.ds(pl.multiple_of(k * channels, channels), channels)
        if x_goal == 0:
            return (
                (wk.at[:, whole], 0, 0, head_dim),
                (wv.at[:, whole], 1, head_dim, head_dim),
            )
        return (
            (wq.at[:, whole], 0, 0, head_dim),
            (wcv.at[:, part], 1, head_dim, channels),
            (wcg.at[:, part], 1, head_dim + channels, channels),
        )

    own_rows = pl.ds(pl.multiple_of(me * depth, depth), depth)
    z_first = (1 - core) * 2
    share = weights.at[:depth, :]

    def send_weights(k, cross, leaving, *conditions, to_peer=False):
        for x_goal in range(2):
            chosen = conditions + ((x != x_goal) if cross else (x == x_goal),)
            for source, unit, start, size in shares(k, x_goal):
                device = peer if to_peer else ((z_first + k) * 2 + x_goal, y * 2 + unit)
                target = weights.at[own_rows, start : start + size]
                sends.start(
                    source, target, weight_sem.at[unit, me], device, *chosen, leaving=leaving
                )

    loaded(2, len(loads))
    mate_leaving, other_leaving = sends.shared((share,)), sends.shared((share,))
    send_weights(odd, False, other_leaving, far, to_peer=True)
    send_weights(1 - odd, False, mate_leaving, far)
    for x_goal in range(2):

        def keep():
            for source, _, start, size in shares(odd, x_goal):
                weights[own_rows, start : start + size] = source[...]

        when((far, x == x_goal), keep)

    own_arrays = (taps, conv_gain, memory_gain, gate_weights)
    for index, array in enumerate(own_arrays):
        sends.start(array, array, own_sem.at[index], peer, far)
    leaving = sends.shared((offsets.at[:2],))
    for k in range(2):
        device = ((z_first + k) * 2, y * 2 + side)
        sends.start(shifts, offsets.at[place], offset_sem.at[0], device, leaving=leaving)

    half_rows = memory_out.shape[1] // 2
    out_width = memory_out.shape[2]
    three_pieces = weights.at[: 3 * half_rows * out_width // (2 * head_dim), :]

    def out_piece(part, number):
        if number == 1:
            return conv_out.at[part]
        start = half_rows * (number // 2)
        return memory_out.at[part, start : start + half_rows, :]

    out_leaving = [sends.shared((three_pieces,)) for _ in range(2)]

    def send_out(number, *conditions):
        spot = out_piece(own_part, number)
        for device, leaving in zip((x_side, peer), out_leaving):
            sends.start(spot, spot, out_sem.at[own_part], device, *conditions, leaving=leaving)

    k_near = jnp.where(near, odd, 1 - core)
    groups = []
    for k in (k_near, 1 - k_near):
        source = core * 2 + k
        groups.append((source, k * 2 + x, k * 2 + 1 - x))
    for source, i, _ in groups:
        away, up = source != z, source < z
        onward = (jnp.where(up, z + 1, z - 1) * 2 + x, tp)
        for j in range(2):
            spot, sem = block(i, y * 2 + j), token_sem.at[i, j]
            arrived(spot, sem, jnp.logical_or(away, j != core))
            sends.start(spot, spot, sem, onward, away, middle, leaving=z_leaving)
            sends.start(spot, spot, sem, x_side, away, leaving=x_leaving)
            sends.start(spot, spot, y_sem.at[0], y_side, away, leaving=y_leaving)
    cross_leaving = [sends.shared((share,)) for _ in range(2)]
    send_weights(side, False, mate_leaving, near, middle)
    send_weights(odd, True, cross_leaving[1], far)
    send_weights(1 - odd, True, cross_leaving[0], far, ends)
    for _, _, i in groups:
        for j in range(2):
            spot, sem = block(i, y * 2 + j), token_sem.at[i, j]
            arrived(spot, sem)
            sends.start(spot, spot, y_sem.at[0], y_side, leaving=y_leaving)

    send_weights(side, False, mate_leaving, near, ends)
    last = jnp.logical_and(middle, first)
    send_weights(1 - side, False, other_leaving, near, jnp.logical_not(last))
    k_cross = jnp.where(near, 1 - side, 1 - odd)
    send_weights(k_cross, True, cross_leaving[0], jnp.logical_or(near, middle))
    send_weights(side, True, cross_leaving[1], near)
    send_weights(1 - side, False, other_leaving, near, last)
    for number in range(2):
        send_out(number, near, second)

    arrived(blocks(8), y_sem.at[0])
    for index, array in enumerate(own_arrays):
        arrived(array, own_sem.at[index], near)
    arrived(offsets, offset_sem.at[0], first)

    @pl.when(first)
    def _():
        gate_rows[...] = jnp.zeros_like(gate_rows)
        gate_rows[0:2, :] = gate_weights[0].astype(f32)
        gate_rows[2:4, :] = gate_weights[1].astype(f32)
        gates = lax.dot_general(
            lines[...], gate_rows[...].astype(bf16), NT, preferred_element_type=f32
        ).T
        shift = [jnp.concatenate([offsets[i, kind] for i in range(4)], 1) for kind in range(2)]
        gate_in = pick(odd, gates[0:1] + shift[0][0:1], gates[1:2] + shift[0][1:2])
        forget = pick(odd, gates[2:3] + shift[1][0:1], gates[3:4] + shift[1][1:2])
        forget_log = jnp.minimum(forget, 0.0) - jnp.log1p(jnp.exp(-jnp.abs(forget)))
        coarse = jnp.round(forget_log * 8.0) * 0.125
        within = prefix_sums(stacked((coarse, forget_log - coarse), rows))
        which = lax.broadcasted_iota(jnp.int32, (ROW_TILE, rows), 0)
        level_here[...] = jnp.where(which == 2, gate_in, within)

    first_core, second_core = core == 0, core == 1
    sends.start(level_here, level_before, level_sem.at[0], peer, first, first_core)

    @pl.when(jnp.logical_and(first, first_core))
    def _():
        level_before[...] = jnp.zeros_like(level_before)
        keys[:rows, :] = jnp.zeros_like(keys[:rows, :])
        values[:rows, :] = jnp.zeros_like(values[:rows, :])

    scale = head_dim ** (-0.5)
    reach = (rows + span, 2 * rows)
    stores = (weight_near, weight_far)

    def position_weights():
        before = level_before[...]
        which = lax.broadcasted_iota(jnp.int32, (ROW_TILE, rows), 0)
        here = level_here[...] + jnp.where(which < 2, before[:, rows - 1 :], 0.0)
        from_rows = jnp.concatenate([before, here], axis=1)
        to_columns = as_columns(here)
        tile = 64
        for start in range(0, rows, tile):
            index = start // span
            width = reach[index]
            to = to_columns[start : start + tile]
            log_weight = (
                (to[:, 0:1] - from_rows[0:1, :width])
                + (to[:, 1:2] - from_rows[1:2, :width])
                + from_rows[2:3, :width]
            )
            at = lax.broadcasted_iota(jnp.int32, (tile, width), 1)
            until = lax.broadcasted_iota(jnp.int32, (tile, width), 0) + (start + rows)
            seen = jnp.logical_and(at <= until, at >= rows * (1 - core))
            log_weight = jnp.where(seen, log_weight, -jnp.inf)
            weight = jnp.exp(log_weight - jnp.max(log_weight, axis=1, keepdims=True)) * scale
            stores[index][start - index * span : start - index * span + tile, :] = weight

    forward_leaving = sends.shared((weights.at[: 7 * depth // 2, :],))

    def own_unit(i):
        for unit in range(2):
            spot, sem = piece(unit, i), weight_sem.at[unit, i]
            arrived(spot, sem, core == unit)
            sends.start(spot, spot, sem, peer, core == unit, leaving=forward_leaving)

    def other_unit(i):
        for unit in range(2):
            arrived(piece(unit, i), weight_sem.at[unit, i], core != unit)

    def multiply(start, size):
        part = pl.ds(pl.multiple_of(start, size), size)
        return jnp.dot(lines[:, part], weights[part, :], preferred_element_type=f32)

    z_mate = side * 2 + 1 - odd
    z_far = (jnp.where(side == 0, 3, 0), jnp.where(side == 0, 2, 1))
    own_unit(z_mate * 2 + x)
    own_unit(z_far[0] * 2 + x)
    arrived(level_before, level_sem.at[0], first, second_core)
    when((first,), position_weights)
    for i in (z * 2 + 1 - x, z_mate * 2 + 1 - x):
        own_unit(i)
    for i in (z_mate * 2 + x, z * 2 + 1 - x, z_mate * 2 + 1 - x):
        other_unit(i)
    for unit in range(2):
        arrived(piece(unit, me), weight_sem.at[unit, me], near)
    half = count // 2 * depth
    product[...] = multiply(side * half, half)
    own_unit(z_far[0] * 2 + 1 - x)
    own_unit(z_far[1] * 2 + x)
    own_unit(z_far[1] * 2 + 1 - x)
    for pair in z_far:
        other_unit(pair * 2)
        other_unit(pair * 2 + 1)
        product[...] += multiply(pair * 2 * depth, 2 * depth)

    for number in range(2):
        send_out(number, first, near)

    @pl.when(second)
    def _():
        queries[...] = product[:, :head_dim].astype(bf16)

    leaving = sends.shared((queries, second))
    for number in (0, 1, 3, 2):
        part = queries.at[number * length : (number + 1) * length, :]
        sends.start(part, part, query_sem.at[number], x_side, second, leaving=leaving)

    @pl.when(first)
    def _():
        keys[rows:, :] = product[:, :head_dim].astype(bf16)
        values[rows:, :] = product[:, head_dim:].astype(bf16)

    leaving = sends.shared((keys, first, first_core))
    for array in (keys, values):
        sends.start(
            array.at[rows:, :],
            array.at[:rows, :],
            pair_sem.at[0],
            peer,
            first,
            first_core,
            leaving=leaving,
        )

    halo = extended.shape[0] - rows

    @pl.when(second)
    def _():
        gated = product[:, head_dim : head_dim + channels] * jax.nn.sigmoid(
            product[:, head_dim + channels :]
        )
        extended[halo:, :] = gated.astype(bf16).astype(f32)

    sends.start(
        extended.at[rows:, :], extended.at[:halo, :], halo_sem.at[0], peer, second, first_core
    )

    @pl.when(jnp.logical_and(second, first_core))
    def _():
        extended[:halo, :] = jnp.zeros((halo, channels), f32)

    arrived(extended.at[:halo, :], halo_sem.at[0], second, second_core)
    source_index = y * layers + z

    @pl.when(second)
    def _():
        number = taps.shape[0]
        kernel = taps[...].astype(f32)
        kernel = pick(odd, kernel[:, :channels], kernel[:, channels:])
        for start in range(0, rows, length):
            base = start + halo - (number - 1)
            total = extended[base : base + length, :] * kernel[0:1]
            for index in range(1, number):
                total = total + (
                    extended[base + index : base + index + length, :] * kernel[index : index + 1]
                )
            conv[start : start + length, :] = total
        all_rows = conv[...]
        both = as_rows(
            (
                jnp.sum(all_rows, axis=1, keepdims=True),
                jnp.sum(all_rows * all_rows, axis=1, keepdims=True),
            )
        )
        sums_done[...] = jnp.concatenate(
            [both[:2, start : start + LANES] for start in range(0, rows, LANES)], axis=0
        )
        sums_in[source_index] = sums_done[...]

    sources = [(z_other, y_other) for z_other in range(layers) for y_other in range(2)]
    others = sums_in.at[: count - 1]
    leaving = sends.shared((others, second))
    for z_other, y_other in sources:
        away = jnp.logical_or(z != z_other, y != y_other)
        device = (z_other * 2 + 1, y_other * 2 + core)
        sends.start(
            sums_done,
            sums_in.at[source_index],
            sums_sem.at[0],
            device,
            second,
            away,
            leaving=leaving,
        )
    arrived(others, sums_sem.at[0], second)

    @pl.when(second)
    def _():
        total = sums_in[0]
        for index in range(1, 2 * layers):
            total = total + sums_in[index]
        total = total * (1.0 / (2 * layers * channels))
        total = jnp.concatenate([total[at : at + 2] for at in range(0, ROW_TILE, 2)], axis=1)
        mean = total[0:1]
        inverse = lax.rsqrt(total[1:2] - mean * mean + EPS)
        across = as_columns(stacked((mean, inverse), rows))
        gain = conv_gain[...]
        gain = pick(odd, gain[:, :channels], gain[:, channels:])
        normed = (conv[...] - across[:, 0:1]) * across[:, 1:2] * gain
        conv_done[...] = (normed * jax.nn.sigmoid(normed)).astype(bf16)

    piece_rows = span * (head_dim + channels) // (2 * head_dim)

    def so_many(number):
        return weights.at[: number * piece_rows, :]

    up_leaving = sends.shared(*((so_many(at + 1), z == at) for at in range(layers - 1)))
    down_leaving = sends.shared(*((so_many(layers - at), z == at) for at in range(1, layers)))
    given_leaving = sends.shared((memory_in.at[0], first), (conv_in.at[0], second))

    def spread(done, inside, semaphores, home, number):
        here, index = x == home, number // 2
        source = done.at[number * length : (number + 1) * length, :]
        part = slice(index * length, (index + 1) * length)
        target, sem = inside.at[z, part, :], semaphores.at[z, index]
        if number % 2 != home:
            sends.start(source, target, sem, x_side, here, leaving=given_leaving)
            return
        sends.start(source, target, sem, below, here, has_below, leaving=down_leaving)
        sends.start(source, target, sem, above, here, has_above, leaving=up_leaving)

        @pl.when(here)
        def _():
            inside[z, part, :] = source[...]

    for number in range(4):
        spread(conv_done, conv_in, conv_sem, 1, number)
    for number in range(2):
        send_out(number, second, far)
    send_out(2, second)

    for array in (keys,):
        arrived(array, pair_sem.at[0], first, second_core)
    for number in (0, 1, 3, 2):
        start, index, inner = number * length, number // 2, number % 2
        arrived(queries.at[start : start + length, :], query_sem.at[number], first)

        @pl.when(first)
        def _():
            width = reach[index]
            gain = memory_gain[...]
            gain = pick(odd, gain[:, :head_dim], gain[:, head_dim:])
            scores = lax.dot_general(
                queries[start : start + length, :],
                keys[:width, :],
                NT,
                preferred_element_type=f32,
            )
            scores = scores * stores[index][inner * length : (inner + 1) * length, :]
            numer = jnp.dot(scores.astype(bf16), values[:width, :], preferred_element_type=f32)
            denom = jnp.sum(scores, axis=1, keepdims=True)
            cell = numer / jnp.maximum(jnp.abs(denom), 1.0)
            memory_done[start : start + length, :] = (cell * gain).astype(bf16)
            square = as_rows((jnp.sum(cell * cell, axis=1, keepdims=True),))
            squares_done[index, inner] = square[0:1]

        spread(memory_done, memory_in, memory_sem, 0, number)
    for number in range(2):
        send_out(number, first, far)
    send_out(2, first)

    @pl.when(first)
    def _():
        for index in range(2):
            squares_in[index * count + source_index] = squares_done[index, 0]

    order = line_order(z, layers)
    across = (1 - x) * 2 + core
    across_leaving = sends.shared((three_pieces,))

    def pass_on(distance, kind, index, *conditions):
        inside, semaphores, home = kind
        part = slice(index * length, (index + 1) * length)
        if distance == 0:
            away = x != home
            spot, sem = inside.at[z, part, :], semaphores.at[z, index]
            arrived(spot, sem, away, *conditions)
            for device, further, leaving in (
                (below, has_below, down_leaving),
                (above, has_above, up_leaving),
            ):
                sends.start(spot, spot, sem, device, away, further, *conditions, leaving=leaving)
            return
        down, up = order[2 * distance - 2 : 2 * distance]
        for (source, there, onward, further), leaving in ((down, up_leaving), (up, down_leaving)):
            spot, sem = inside.at[source, part, :], semaphores.at[source, index]
            arrived(spot, sem, there, *conditions)
            device = (onward * 2 + x, tp)
            sends.start(spot, spot, sem, device, there, further, *conditions, leaving=leaving)

    def share_out(*conditions):
        arrived(three_pieces, out_sem.at[across], *conditions)
        for spot in (memory_out.at[across], conv_out.at[across]):
            sends.start(spot, spot, out_sem.at[across], peer, *conditions, leaving=across_leaving)

    convs, memories = (conv_in, conv_sem, 1), (memory_in, memory_sem, 0)
    pass_on(0, convs, 0, first)
    pass_on(0, convs, 1, first)
    for index in range(2):
        squares_leaving = sends.shared((squares_in.at[: 2 * count - 1], first))
        for z_other, y_other in sources:
            for x_other in range(2):
                away = jnp.logical_or(
                    jnp.logical_or(z != z_other, y != y_other), x != x_other
                )
                sends.start(
                    squares_done.at[index, x_other],
                    squares_in.at[index * count + source_index],
                    squares_sem.at[index],
                    (z_other * 2 + x_other, y_other * 2 + core),
                    first,
                    away,
                    leaving=squares_leaving,
                )

    for distance in range(1, layers):
        for kind in (memories, convs):
            for index in range(2):
                if distance + 1 < layers or index == 0:
                    pass_on(distance, kind, index, first)
        if distance == layers - 2:
            share_out(first)
    for distance in range(1, layers + 2):
        if distance < layers:
            pass_on(distance, convs, 0, second)
            pass_on(distance, convs, 1, second)
        if 0 <= distance - 2 < layers - 1:
            pass_on(distance - 2, memories, 1, second)
        if 0 <= distance - 1 < layers:
            pass_on(distance - 1, memories, 0, second)
        if distance == layers - 1:
            share_out(second)
    entries = layers * 2 * head_dim
    for index in range(2):
        part = slice(index * length, (index + 1) * length)
        if index == 1:
            pass_on(layers - 1, memories, 1)
            pass_on(layers - 1, convs, 1, first)
        at = index * count
        arrived(squares_in.at[at : at + count - 1], squares_sem.at[index], first)
        arrived(squares_in.at[at : at + count], squares_sem.at[index], second)
        if index == 0:
            for group in range(2):
                arrived(three_pieces, out_sem.at[group * 2 + 1 - core])
        total = squares_in[at]
        for slot in range(1, 2 * layers):
            total = total + squares_in[at + slot]
        row_scale = stacked((lax.rsqrt(total * (1.0 / entries) + EPS),), length)
        row_scale = as_columns(row_scale)[:, 0:1]
        for group in range(2):
            from_memory, from_conv = None, None
            for head in range(layers):
                where = group * 2 + 1 - head // 2
                inner = head % 2
                memory_term = jnp.dot(
                    memory_in[head, part, :],
                    memory_out[where, inner * head_dim : (inner + 1) * head_dim, :],
                    preferred_element_type=f32,
                )
                conv_term = jnp.dot(
                    conv_in[head, part, :],
                    conv_out[where, inner * channels : (inner + 1) * channels, :],
                    preferred_element_type=f32,
                )
                from_memory = memory_term if head == 0 else from_memory + memory_term
                from_conv = conv_term if head == 0 else from_conv + conv_term
            width = from_memory.shape[1]
            partial[index, :, group * width : (group + 1) * width] = (
                from_conv + row_scale * from_memory
            ).astype(bf16)
        device = ((core * 2 + index) * 2 + x, z)
        away = jnp.logical_or(core * 2 + index != z, tp != z)
        sends.start(partial.at[index], slots.at[y], slot_sem.at[y], device, away)

        @pl.when(jnp.logical_not(away))
        def _():
            slots[y] = partial[index]

    for y_other in range(2):
        own = jnp.logical_and(tp == z, jnp.logical_and(y == y_other, core == side))
        arrived(slots.at[y_other], slot_sem.at[y_other], jnp.logical_not(own))
    sends.finish()


def layer(arrays):
    count, columns = lax.axis_size("sp"), lax.axis_size("tp")
    (
        tokens,
        conv_value_weight,
        conv_gate_weight,
        conv_kernel,
        conv_norm_gain,
        query_weight,
        key_weight,
        value_weight,
        input_gate_weight,
        forget_gate_weight,
        input_offset,
        forget_offset,
        memory_norm_gain,
        conv_out_weight,
        memory_out_weight,
    ) = arrays
    length, features = tokens.shape
    depth, head_dim = query_weight.shape[0], query_weight.shape[1] // 2
    channels = conv_value_weight.shape[1] // 2
    wide = features * columns
    rows = length * count // 2
    span = rows // 2
    layers = count // 2
    halo = -(-(conv_kernel.shape[0] - 1) // ROW_TILE) * ROW_TILE
    width = memory_out_weight.shape[1]
    f32, bf16 = jnp.float32, jnp.bfloat16
    DMA = pltpu.SemaphoreType.DMA
    V = pltpu.VMEM
    return pl.pallas_call(
        lambda *refs: layer_kernel(count, columns, *refs),
        out_shape=jax.ShapeDtypeStruct((2, length, features), bf16),
        in_specs=[pl.BlockSpec(memory_space=pltpu.HBM)] * 15,
        out_specs=IN_VMEM,
        scratch_shapes=[
            V(tokens.shape, bf16),
            V(query_weight.shape, bf16),
            V(key_weight.shape, bf16),
            V(value_weight.shape, bf16),
            V(conv_value_weight.shape, bf16),
            V(conv_gate_weight.shape, bf16),
            V((2, 2, length), f32),
            V((rows, wide), bf16),
            V((wide, 2 * head_dim), bf16),
            V((rows, 2 * head_dim), f32),
            V(conv_kernel.shape, bf16),
            V((1, 2 * channels), f32),
            V((1, 2 * head_dim), f32),
            V((2, 2, wide), bf16),
            V((4, 2, 2, length), f32),
            V((LANES, wide), f32),
            V((ROW_TILE, rows), f32),
            V((ROW_TILE, rows), f32),
            V((2 * rows, head_dim), bf16),
            V((2 * rows, head_dim), bf16),
            V((rows, head_dim), bf16),
            V((span, rows + span), f32),
            V((span, 2 * rows), f32),
            V((rows, head_dim), bf16),
            V((2, 2, 1, length), f32),
            V((2 * count, 1, length), f32),
            V((halo + rows, channels), f32),
            V((rows, channels), f32),
            V((ROW_TILE, LANES), f32),
            V((count, ROW_TILE, LANES), f32),
            V((rows, channels), bf16),
            V((layers, span, head_dim), bf16),
            V((layers, span, channels), bf16),
            V((4, 2 * head_dim, width), bf16),
            V((4, 2 * channels, width), bf16),
            V((2, length, features), bf16),
            DMA((16,)),
            DMA((SENDS,)),
            DMA((4, 2)),
            DMA((1,)),
            DMA((2, count)),
            DMA((4,)),
            DMA((1,)),
            DMA((1,)),
            DMA((1,)),
            DMA((4,)),
            DMA((1,)),
            DMA((1,)),
            DMA((2,)),
            DMA((layers, 2)),
            DMA((layers, 2)),
            DMA((4,)),
            DMA((2,)),
        ],
        compiler_params=pltpu.CompilerParams(
            collective_id=0, has_side_effects=True, vmem_limit_bytes=40 * 2**20
        ),
    )(
        *(
            pltpu.with_memory_space_constraint(array, pltpu.HBM)
            for array in (
                tokens,
                query_weight,
                key_weight,
                value_weight,
                conv_value_weight,
                conv_gate_weight,
                conv_kernel,
                conv_norm_gain.reshape(1, -1),
                memory_norm_gain.reshape(1, -1),
                input_gate_weight.T,
                forget_gate_weight.T,
                input_offset.T,
                forget_offset.T,
                memory_out_weight,
                conv_out_weight,
            )
        )
    )


def on_device_by_column(*arrays):
    slots = layer(arrays)
    return jnp.sum(slots.astype(jnp.float32), axis=0).astype(jnp.bfloat16)


def splits_by_column(mesh, tokens, query_weight, conv_value_weight, conv_kernel, input_gate_weight):
    count, columns = mesh.shape["sp"], mesh.shape["tp"]
    heads = input_gate_weight.shape[1]
    head_dim = query_weight.shape[1] // heads
    length = tokens.shape[0] // count
    return (
        count == 8
        and columns == 4
        and heads == count
        and length == LANES
        and tokens.size * 2 <= 4 * 2**20
        and conv_value_weight.shape[1] * 2 == head_dim * heads
        and head_dim == 256
        and conv_kernel.shape[0] - 1 <= length
    )


def solution(mesh):
    in_specs = (
        P("sp", "tp"),
        P("sp", "tp"),
        P("sp", "tp"),
        P(None, "tp"),
        P("tp"),
        P("sp", "tp"),
        P("sp", "tp"),
        P("sp", "tp"),
        P(None, "tp"),
        P(None, "tp"),
        P("sp", "tp"),
        P("sp", "tp"),
        P("tp"),
        P("tp", "sp"),
        P("tp", "sp"),
    )
    out_specs = P("sp", "tp")

    def run(*arrays):
        by_column = splits_by_column(
            mesh, arrays[0], arrays[5], arrays[1], arrays[3], arrays[8]
        )
        on_device = on_device_by_column if by_column else on_device_by_position
        return jax.shard_map(
            on_device, mesh=mesh, in_specs=in_specs, out_specs=out_specs, check_vma=False
        )(*arrays)

    return run
```
